512 devices in a mesh: sp: 16 (over z), fs: 4 (over y), tp: 8 (over x, core).
Axes of the slice: x: 4, y: 4, z: 16, core: 2. Of those that a mesh axis runs over, the one named last changes fastest.
Arguments:
- layer_entering_vectors: bfloat16 [4, 4096, 2048], P('fs', ('sp', 'tp')), may hold values from -6 to 6
- entering_rms_coefficients: float32 [2048], replicated, may hold values from 0.1 to 1.9
- question_projection: bfloat16 [2048, 1536], P('fs', 'tp'), may hold values from -0.125 to 0.125
- compressing_projection: bfloat16 [2048, 256], P('fs'), may hold values from -0.125 to 0.125
- spinning_address_projection: bfloat16 [2048, 32], P('fs'), may hold values from -0.125 to 0.125
- compact_rms_coefficients: float32 [256], replicated, may hold values from 0.1 to 1.9
- compact_to_plain_address: bfloat16 [256, 1024], P(None, 'tp'), may hold values from -0.375 to 0.375
- compact_to_content: bfloat16 [256, 1024], P(None, 'tp'), may hold values from -0.375 to 0.375
- question_rms_coefficients: float32 [96], replicated, may hold values from 0.7 to 6
- address_rms_coefficients: float32 [96], replicated, may hold values from 0.7 to 6
- acceptance_projection: bfloat16 [2048, 1024], P('fs', 'tp'), may hold values from -0.125 to 0.125
- state_address_projection: bfloat16 [2048, 1024], P('fs', 'tp'), may hold values from -0.125 to 0.125
- state_content_projection: bfloat16 [2048, 1024], P('fs', 'tp'), may hold values from -0.125 to 0.125
- fading_first_lowrank: bfloat16 [2048, 128], replicated, may hold values from -0.125 to 0.125
- fading_second_lowrank: bfloat16 [128, 1024], P(None, 'tp'), may hold values from -0.375 to 0.375
- fading_channel_bias: float32 [1024], P('tp'), may hold values from -20 to -2
- fading_speed_multiplier: float32 [4, 16, 4096], P('fs', 'tp', 'sp'), may hold values from 0.5 to 2, as said below
- fading_extra_exponent: float32 [4, 16, 4096], P('fs', 'tp', 'sp'), may hold values from -0.7 to 0
- adaptation_first_lowrank: bfloat16 [2048, 128], replicated, may hold values from -0.125 to 0.125
- adaptation_second_lowrank: bfloat16 [128, 1024], P(None, 'tp'), may hold values from -0.5 to 0.5
- adaptation_channel_bias: float32 [1024], P('tp'), may hold values from -12 to -1
- present_token_coefficients: float32 [16, 64], P('tp'), may hold values from -1.5 to 1.5
- branch_rms_coefficients: float32 [1024], P('tp'), may hold values from 0.1 to 1.9
- softmax_merge_projection: bfloat16 [1024, 2048], P('tp', 'fs'), may hold values from -0.1875 to 0.1875
- state_merge_projection: bfloat16 [1024, 2048], P('tp', 'fs'), may hold values from -0.1875 to 0.1875
Outputs:
- mixed: bfloat16 [4, 4096, 2048], P('fs', ('sp', 'tp'))
- log_total: float32 [4, 16, 4096], P('fs', 'tp', 'sp')
The draws below stay inside these ranges and needn't reach their ends.
Inputs may be any that keep to these rules, and one draw needn't show every extreme that they name: `fading_speed_multiplier`: constant over aligned blocks of 256 positions.
All inputs are finite; a program needn't handle non-finite values.
Results may differ from the reference program's by a relative error of at most 0.015.
Values may be sent and summed in bfloat16 or wider, within the bound.
No kernel may reach another device: no remote copies, remote signals or barrier semaphores. Data moves between devices by JAX's collectives and lax.ppermute only.
A program may use at most 64 MiB of HBM per device.

```python
import math
import jax
import jax.numpy as jnp
from jax import lax

D = 2048
MHEADS = 16
NOPE = 64
ROPE = 32
VHEAD = 64
KVLAT = 256
STATE_BRANCHES = 16
BRANCH_CHANNELS = 64
DLORA = 128
ALORA = 128
TOK_DEV = 256
SEQS = 4
TOKEN_SPAN = 4096
N_TP = 8


def draw_gain_common(key):
    return jax.random.uniform(key, (NOPE + ROPE,), jnp.float32, 0.7, 1.3)


def draw_question_rms_coefficients(key, part):
    return draw_gain_common(jax.random.fold_in(key, 11))


def draw_address_rms_coefficients(key, part):
    return draw_gain_common(jax.random.fold_in(key, 12))


def draw_fading_channel_bias(key, part):
    first, second = jax.random.split(jax.random.fold_in(key, 21))
    quick = jax.random.uniform(first, (STATE_BRANCHES,), jnp.float32) < 0.5
    slow_value = jnp.log(0.15 / TOKEN_SPAN) + 0.5
    centre = jnp.where(quick, -3.2, slow_value)
    jitter = jax.random.uniform(second, (STATE_BRANCHES, BRANCH_CHANNELS), jnp.float32, -0.5, 0.5)
    return (centre[:, None] + jitter).reshape(STATE_BRANCHES * BRANCH_CHANNELS)


def draw_adaptation_channel_bias(key, part):
    spread = jax.random.uniform(jax.random.fold_in(key, 31), (STATE_BRANCHES * BRANCH_CHANNELS,), jnp.float32, math.log(8.0), math.log(40.0))
    return spread - math.log(max(TOKEN_SPAN, 256) * 1.0)


def draw_fading_speed_multiplier(key, part):
    blocks = TOKEN_SPAN // TOK_DEV
    values = jnp.exp(jax.random.uniform(jax.random.fold_in(key, 41), (SEQS, STATE_BRANCHES, blocks), jnp.float32, math.log(0.5), math.log(2.0)))
    return jnp.repeat(values, TOK_DEV, axis=2)


def draw_fading_extra_exponent(key, part):
    first, second = jax.random.split(jax.random.fold_in(key, 51))
    stratum = TOKEN_SPAN // 3
    offsets = jax.random.randint(first, (SEQS, 3), 0, stratum, dtype=jnp.int32)
    places = offsets + stratum * jnp.arange(3, dtype=jnp.int32)[None, :]
    strength = jax.random.uniform(second, (SEQS, STATE_BRANCHES, 3), jnp.float32, 0.2, 0.5)
    where_hit = (jnp.arange(TOKEN_SPAN, dtype=jnp.int32)[None, None, None, :] == places[:, None, :, None]).astype(jnp.float32)
    return jnp.sum(jnp.log(1.0 - strength)[..., None] * where_hit, axis=2)


def block_scale(stream_key, shape, shards, smallest, top_value):
    def one(position, parts):
        draws = jax.random.uniform(jax.random.fold_in(jax.random.fold_in(stream_key, 6), position), (parts,), jnp.float32, smallest / len(shards), top_value / len(shards))
        return jnp.repeat(jnp.exp(draws), shape[position] // parts).reshape((-1,) + (1,) * (len(shape) - position - 1))

    loudness = one(*shards[0])
    for cut in shards[1:]:
        loudness = loudness * one(*cut)
    return loudness


def normal_values(key, extent, deviation, reach, pieces=(), held_as=jnp.bfloat16):
    level = block_scale(key, extent, pieces, -0.22, 0.18) if pieces else 1.0
    entries = jax.random.normal(key, extent, jnp.float32) * deviation * level
    return jnp.minimum(jnp.maximum(entries, -reach), reach).astype(held_as)


def setup_inputs(seed: int = 0) -> dict:
    key_list = jax.random.split(jax.random.key(seed), 26)
    return {
        "layer_entering_vectors": normal_values(key_list[0], (SEQS, TOKEN_SPAN, D), 1.0, 6.0, ((0, 4), (1, 128))),
        "entering_rms_coefficients": jnp.clip(1.0 + 0.18 * jax.random.normal(key_list[1], (D,), jnp.float32), 0.1, 1.9),
        "question_projection": normal_values(key_list[2], (D, MHEADS * (NOPE + ROPE)), D ** -0.5, 0.125, ((0, 4), (1, 8))),
        "compressing_projection": normal_values(key_list[3], (D, KVLAT), D ** -0.5, 0.125, ((0, 4),)),
        "spinning_address_projection": normal_values(key_list[4], (D, ROPE), D ** -0.5, 0.125, ((0, 4),)),
        "compact_rms_coefficients": jnp.clip(1.0 + 0.18 * jax.random.normal(key_list[5], (KVLAT,), jnp.float32), 0.1, 1.9),
        "compact_to_plain_address": normal_values(key_list[6], (KVLAT, MHEADS * NOPE), KVLAT ** -0.5, 0.375, ((1, 8),)),
        "compact_to_content": normal_values(key_list[7], (KVLAT, MHEADS * VHEAD), KVLAT ** -0.5, 0.375, ((1, 8),)),
        "question_rms_coefficients": draw_question_rms_coefficients(jax.random.fold_in(key_list[25], 71), 0),
        "address_rms_coefficients": draw_address_rms_coefficients(jax.random.fold_in(key_list[25], 71), 0),
        "acceptance_projection": normal_values(key_list[10], (D, STATE_BRANCHES * BRANCH_CHANNELS), D ** -0.5, 0.125, ((0, 4), (1, 8))),
        "state_address_projection": normal_values(key_list[11], (D, STATE_BRANCHES * BRANCH_CHANNELS), D ** -0.5, 0.125, ((0, 4), (1, 8))),
        "state_content_projection": normal_values(key_list[12], (D, STATE_BRANCHES * BRANCH_CHANNELS), D ** -0.5, 0.125, ((0, 4), (1, 8))),
        "fading_first_lowrank": normal_values(key_list[13], (D, DLORA), D ** -0.5, 0.125),
        "fading_second_lowrank": normal_values(key_list[14], (DLORA, STATE_BRANCHES * BRANCH_CHANNELS), (2 * DLORA) ** -0.5, 0.375, ((1, 8),)),
        "fading_channel_bias": draw_fading_channel_bias(jax.random.fold_in(key_list[25], 71), 0),
        "fading_speed_multiplier": draw_fading_speed_multiplier(jax.random.fold_in(key_list[25], 71), 0),
        "fading_extra_exponent": draw_fading_extra_exponent(jax.random.fold_in(key_list[25], 71), 0),
        "adaptation_first_lowrank": normal_values(key_list[18], (D, ALORA), D ** -0.5, 0.125),
        "adaptation_second_lowrank": normal_values(key_list[19], (ALORA, STATE_BRANCHES * BRANCH_CHANNELS), ALORA ** -0.5, 0.5, ((1, 8),)),
        "adaptation_channel_bias": draw_adaptation_channel_bias(jax.random.fold_in(key_list[25], 71), 0),
        "present_token_coefficients": normal_values(key_list[21], (STATE_BRANCHES, BRANCH_CHANNELS), 0.3, 1.5, ((0, 8),), jnp.float32),
        "branch_rms_coefficients": jnp.clip(1.0 + 0.18 * jax.random.normal(key_list[22], (STATE_BRANCHES * BRANCH_CHANNELS,), jnp.float32), 0.1, 1.9),
        "softmax_merge_projection": normal_values(key_list[23], (MHEADS * VHEAD, D), (MHEADS * VHEAD) ** -0.5, 0.1875, ((0, 8), (1, 4))),
        "state_merge_projection": normal_values(key_list[24], (STATE_BRANCHES * BRANCH_CHANNELS, D), (STATE_BRANCHES * BRANCH_CHANNELS) ** -0.5, 0.1875, ((0, 8), (1, 4))),
    }


norm_epsilon = 1e-06
group_epsilon = 0.00064
highest = lax.Precision.HIGHEST

def rms_rows(values, gain):
    floats = values.astype(jnp.float32)
    return floats * lax.rsqrt(lax.optimization_barrier(jnp.mean(floats * floats, axis=-1, keepdims=True)) + norm_epsilon) * gain

def rotate(values, positions):
    half = values.shape[-1] // 2
    inverse = 10000.0 ** (-jnp.arange(half, dtype=jnp.float32) / half)
    angle = positions.astype(jnp.float32)[:, None] * inverse[None, :]
    cosine = jnp.cos(angle)[:, None, :]
    sine = jnp.sin(angle)[:, None, :]
    first = values[..., :half]
    second = values[..., half:]
    return jnp.concatenate([first * cosine - second * sine, second * cosine + first * sine], axis=-1)

def finish(stacked, gain, positions):
    normed = rms_rows(stacked, gain)
    return jnp.concatenate([normed[..., :NOPE], rotate(normed[..., NOPE:], positions)], axis=-1).astype(jnp.bfloat16)

def matmul(left, right):
    return jnp.dot(left, right, preferred_element_type=jnp.float32)

def recur(state, inputs):
    decay_now, unit_now, learn_now, value_now, key_now, recept_now = inputs
    along = jnp.einsum('hvk,hk->hv', state, unit_now, precision=highest)
    state = state * decay_now[:, None, :] - along[:, :, None] * (unit_now * learn_now)[:, None, :] + value_now[:, :, None] * key_now[:, None, :]
    return (state, jnp.einsum('hvk,hk->hv', state, recept_now, precision=highest))

def solo_stream(entering_tokens_flat, entering_rms_coefficients, question_projection, compressing_projection, spinning_address_projection, compact_rms_coefficients, compact_to_plain_address, compact_to_content, question_rms_coefficients, address_rms_coefficients, acceptance_projection, state_address_projection, state_content_projection, fading_first_lowrank, fading_second_lowrank, fading_channel_bias, fading_speed_multiplier, fading_extra_exponent, adaptation_first_lowrank, adaptation_second_lowrank, adaptation_channel_bias, present_token_coefficients, branch_rms_coefficients, softmax_merge_projection, state_merge_projection):
    positions = jnp.arange(TOKEN_SPAN, dtype=jnp.int32)
    normed = rms_rows(entering_tokens_flat, entering_rms_coefficients).astype(jnp.bfloat16)
    query = matmul(normed, question_projection).astype(jnp.bfloat16).reshape(TOKEN_SPAN, MHEADS, NOPE + ROPE)
    latent = matmul(normed, compressing_projection).astype(jnp.bfloat16)
    rope_key = matmul(normed, spinning_address_projection).astype(jnp.bfloat16)
    latent_normed = rms_rows(latent, compact_rms_coefficients).astype(jnp.bfloat16)
    key_nope = matmul(latent_normed, compact_to_plain_address).astype(jnp.bfloat16).reshape(TOKEN_SPAN, MHEADS, NOPE)
    values_heads = matmul(latent_normed, compact_to_content).astype(jnp.bfloat16).reshape(TOKEN_SPAN, MHEADS, VHEAD)
    key_stack = jnp.concatenate([key_nope, jnp.broadcast_to(rope_key[:, None, :], (TOKEN_SPAN, MHEADS, ROPE))], axis=-1)
    query_ready = finish(query, question_rms_coefficients, positions)
    key_ready = finish(key_stack, address_rms_coefficients, positions)
    scale = (NOPE + ROPE) ** (-0.5)
    keys_wide = key_ready.astype(jnp.float32)
    values_wide = values_heads.astype(jnp.float32)

    def attend(block):
        start = block * TOK_DEV
        query_block = lax.dynamic_slice_in_dim(query_ready, start, TOK_DEV, 0).astype(jnp.float32)
        scores = jnp.einsum('qhd,khd->hqk', query_block, keys_wide) * scale
        allowed = positions[None, :] <= (start + jnp.arange(TOK_DEV, dtype=jnp.int32))[:, None]
        scores = jnp.where(allowed[None], scores, -jnp.inf)
        highest_score = lax.optimization_barrier(jnp.max(scores, axis=-1))
        weights = jnp.exp(scores - highest_score[..., None])
        total = lax.optimization_barrier(jnp.sum(weights, axis=-1))
        summed = jnp.einsum('hqk,khd->qhd', weights.astype(jnp.bfloat16).astype(jnp.float32), values_wide)
        attended = (summed / jnp.transpose(total)[:, :, None]).astype(jnp.bfloat16)
        return (attended, highest_score + jnp.log(total))
    blocks_out, blocks_log = lax.map(attend, jnp.arange(TOKEN_SPAN // TOK_DEV, dtype=jnp.int32))
    attended = blocks_out.reshape(TOKEN_SPAN, MHEADS * VHEAD)
    log_total = jnp.transpose(blocks_log, (1, 0, 2)).reshape(MHEADS, TOKEN_SPAN)

    def heads(values):
        return values.astype(jnp.float32).reshape(TOKEN_SPAN, STATE_BRANCHES, BRANCH_CHANNELS)
    acceptance_tokens_flat = heads(matmul(normed, acceptance_projection).astype(jnp.bfloat16))
    state_address = heads(matmul(normed, state_address_projection).astype(jnp.bfloat16))
    state_content = heads(matmul(normed, state_content_projection).astype(jnp.bfloat16))
    decay_low = jnp.tanh(matmul(normed, fading_first_lowrank).astype(jnp.bfloat16).astype(jnp.float32)).astype(jnp.bfloat16)
    rate_logarithm = -jax.nn.softplus(-(fading_channel_bias + matmul(decay_low, fading_second_lowrank))) - 0.5
    decay_factor = jnp.exp(-jnp.exp(rate_logarithm).reshape(TOKEN_SPAN, STATE_BRANCHES, BRANCH_CHANNELS) * jnp.transpose(fading_speed_multiplier)[:, :, None] + jnp.transpose(fading_extra_exponent)[:, :, None])
    rate_low = matmul(normed, adaptation_first_lowrank).astype(jnp.bfloat16)
    learn = jax.nn.sigmoid(adaptation_channel_bias + matmul(rate_low, adaptation_second_lowrank)).reshape(TOKEN_SPAN, STATE_BRANCHES, BRANCH_CHANNELS)
    unit = state_address * lax.rsqrt(lax.optimization_barrier(jnp.sum(state_address * state_address, axis=-1, keepdims=True)) + 1e-06)
    start_state = jnp.zeros((STATE_BRANCHES, BRANCH_CHANNELS, BRANCH_CHANNELS), jnp.float32)
    _, read = lax.scan(recur, start_state, (decay_factor, unit, learn, state_content, state_address, acceptance_tokens_flat))
    center = lax.optimization_barrier(jnp.mean(read, axis=-1, keepdims=True))
    spread = lax.optimization_barrier(jnp.mean(jnp.square(read - center), axis=-1, keepdims=True))
    retrieved_rescaled = (read - center) * lax.rsqrt(spread + group_epsilon) * branch_rms_coefficients.reshape(STATE_BRANCHES, BRANCH_CHANNELS)
    present_token_term = lax.optimization_barrier(jnp.sum(acceptance_tokens_flat * state_address * present_token_coefficients, axis=-1, keepdims=True)) * state_content
    state_branch_result = (retrieved_rescaled + present_token_term).reshape(TOKEN_SPAN, STATE_BRANCHES * BRANCH_CHANNELS).astype(jnp.bfloat16)
    attn_cols = MHEADS * VHEAD // N_TP
    rec_cols = STATE_BRANCHES * BRANCH_CHANNELS // N_TP
    mixed = jnp.zeros((TOKEN_SPAN, D), jnp.float32)
    for group in range(N_TP):
        partial_sum = matmul(attended[:, group * attn_cols:(group + 1) * attn_cols], softmax_merge_projection[group * attn_cols:(group + 1) * attn_cols]) + matmul(state_branch_result[:, group * rec_cols:(group + 1) * rec_cols], state_merge_projection[group * rec_cols:(group + 1) * rec_cols])
        mixed = mixed + partial_sum.astype(jnp.bfloat16).astype(jnp.float32)
    return (mixed.astype(jnp.bfloat16), log_total)

def reference(layer_entering_vectors, entering_rms_coefficients, question_projection, compressing_projection, spinning_address_projection, compact_rms_coefficients, compact_to_plain_address, compact_to_content, question_rms_coefficients, address_rms_coefficients, acceptance_projection, state_address_projection, state_content_projection, fading_first_lowrank, fading_second_lowrank, fading_channel_bias, fading_speed_multiplier, fading_extra_exponent, adaptation_first_lowrank, adaptation_second_lowrank, adaptation_channel_bias, present_token_coefficients, branch_rms_coefficients, softmax_merge_projection, state_merge_projection):
    mixed_all = []
    logs_all = []
    for stream_position_entry in range(SEQS):
        solo_blended, solo_exponent_trace = solo_stream(layer_entering_vectors[stream_position_entry], entering_rms_coefficients, question_projection, compressing_projection, spinning_address_projection, compact_rms_coefficients, compact_to_plain_address, compact_to_content, question_rms_coefficients, address_rms_coefficients, acceptance_projection, state_address_projection, state_content_projection, fading_first_lowrank, fading_second_lowrank, fading_channel_bias, fading_speed_multiplier[stream_position_entry], fading_extra_exponent[stream_position_entry], adaptation_first_lowrank, adaptation_second_lowrank, adaptation_channel_bias, present_token_coefficients, branch_rms_coefficients, softmax_merge_projection, state_merge_projection)
        mixed_all.append(solo_blended)
        logs_all.append(solo_exponent_trace)
    return (jnp.stack(mixed_all), jnp.stack(logs_all))
```

```python
import jax
import jax.numpy as jnp
import numpy as np
from jax import lax
from jax.experimental import pallas as pl
from jax.experimental.pallas import tpu as pltpu
from jax.sharding import PartitionSpec as P

F32 = jnp.float32
BF16 = jnp.bfloat16
HIGHEST = lax.Precision.HIGHEST

ROWS = 256
NOPE = 64
ROPE = 32
QK = NOPE + ROPE
CHUNK = 64
CHUNKS = ROWS // CHUNK
EPS = 1e-6
GROUP_EPS = 0.00064
NN = (((1,), (0,)), ((), ()))
NT = (((1,), (1,)), ((), ()))
TN = (((0,), (0,)), ((), ()))

VMEM = pl.BlockSpec(memory_space=pltpu.VMEM)
SMEM = pl.BlockSpec(memory_space=pltpu.SMEM)


def dot(a, b, dims=NN):
    return lax.dot_general(a, b, dims, preferred_element_type=F32)


def exact(a, b, dims=NN):
    return lax.dot_general(a, b, dims, precision=HIGHEST, preferred_element_type=F32)


def halves(a):
    high = a.astype(BF16)
    return high, (a - high.astype(F32)).astype(BF16)


def dot_wide(a, b):
    high, low = halves(a)
    return dot(jnp.concatenate([high, low], axis=1), jnp.concatenate([b, b], axis=0))


def iota(shape, dim):
    return lax.broadcasted_iota(jnp.int32, shape, dim)


def call(body, outs, args, flops, scratch=(), specs=None):
    return pl.pallas_call(
        body,
        out_shape=outs,
        in_specs=specs or [VMEM] * len(args),
        out_specs=jax.tree.map(lambda _: VMEM, outs),
        scratch_shapes=scratch,
        cost_estimate=pl.CostEstimate(flops=flops, bytes_accessed=4 << 20, transcendentals=0),
    )(*args)


def turned(n, table):
    half = ROPE // 2
    a, b = n[NOPE : NOPE + half], n[NOPE + half :]
    cosine, sine = table[:half], table[half:]
    return a * cosine - b * sine, b * cosine + a * sine


def project_body(place, x, w, fd, fa, table, gain, rkv, pay, q, dlow, rlow):
    y = dot(x[...], w[...]).astype(BF16)
    rkv[...] = y[:, :384]
    t = y[:, 384:640].astype(F32).T
    tp = place[1]
    group = jnp.zeros((8, ROWS), F32)
    for g in range(4):
        group += jnp.where(tp // 2 == g, t[224 + 8 * g : 232 + 8 * g], 0.0)
    group = jnp.where(iota((8, ROWS), 0) // 4 == lax.rem(tp, 2), group, 0.0)
    pay[...] = jnp.concatenate([t[192:224], group], axis=0).astype(BF16)
    turn = table[place[0]]
    for h in range(2):
        v = t[QK * h : QK * (h + 1)]
        n = v * lax.rsqrt(jnp.mean(v * v, axis=0, keepdims=True) + EPS) * gain[...]
        a, b = turned(n, turn)
        ready = jnp.concatenate([n[:NOPE], a, b, jnp.zeros((128 - QK, ROWS), F32)], axis=0)
        q[h] = ready.T.astype(BF16)
    dlow[...] = jnp.tanh(dot(x[...], fd[...]).astype(BF16).astype(F32)).astype(BF16)
    rlow[...] = dot(x[...], fa[...]).astype(BF16)


def project(place, x, w, fd, fa, table, gain):
    outs = [
        jax.ShapeDtypeStruct((ROWS, 384), BF16),
        jax.ShapeDtypeStruct((40, ROWS), BF16),
        jax.ShapeDtypeStruct((2, ROWS, 128), BF16),
        jax.ShapeDtypeStruct((ROWS, 128), BF16),
        jax.ShapeDtypeStruct((ROWS, 128), BF16),
    ]
    args = (place, x, w, fd, fa, table, gain)
    return call(project_body, outs, args, 4 << 30, specs=[SMEM] + [VMEM] * 6)


def recur_body(rkv, dlow, rlow, wd, bd, wa, ba, mult, extra, present, free, along, bonus, state):
    lane = iota((ROWS, 128), 1)
    recept, key, value = (rkv[:, 128 * i : 128 * (i + 1)].astype(F32) for i in range(3))
    speed = jax.nn.sigmoid(bd[...] + dot(dlow[...], wd[...])) * np.float32(np.exp(-0.5))
    added = jnp.where(lane < 64, extra[:, 0:1], extra[:, 1:2])
    ld = added - speed * mult[...]
    learn = jax.nn.sigmoid(ba[...] + dot(rlow[...], wa[...]))
    same = (iota((128, 128), 0) // 64 == iota((128, 128), 1) // 64).astype(F32)
    unit = key * lax.rsqrt(exact(key * key, same) + EPS)
    bonus[...] = exact(recept * key * present[...], same) * value
    r, c = iota((ROWS, ROWS), 0), iota((ROWS, ROWS), 1)
    block = r // CHUNK == c // CHUNK
    sums = jnp.concatenate(
        [
            jnp.where(block & (c <= r), 1.0, 0.0),
            jnp.where(block & (lax.rem(c, CHUNK) < CHUNK // 2), 1.0, 0.0),
            jnp.where(block, 1.0, 0.0),
        ],
        axis=0,
    )
    sums = exact(sums, ld)
    cum, mid, end = sums[:ROWS], sums[ROWS : 2 * ROWS], sums[2 * ROWS :]
    prev = cum - ld
    toward = -unit
    remove = unit * learn
    grow, shrink = jnp.exp(cum - mid), jnp.exp(mid - cum)
    left1, left2 = toward * jnp.exp(prev - mid), recept * grow
    right1, right2 = remove * shrink, key * shrink
    start1, start2 = toward * jnp.exp(prev), recept * jnp.exp(cum)
    tail = jnp.exp(end - cum)
    tail1, tail2 = remove * tail, key * tail
    whole = jnp.exp(end)
    m0 = iota((CHUNK, 128), 1) < 64

    def stacked(v, k):
        v = v[CHUNK * k : CHUNK * (k + 1)]
        return jnp.concatenate([jnp.where(m0, v, 0.0), jnp.where(m0, 0.0, v)], axis=0)

    rr, cc = iota((128, 128), 0), iota((128, 128), 1)
    head = rr // 64 == cc // 64
    eye = jnp.where(rr == cc, 1.0, 0.0)
    in16, in32 = rr // 16 == cc // 16, rr // 32 == cc // 32
    strict, upto = head & (rr > cc), head & (rr >= cc)

    def square(top, mask):
        both = jnp.concatenate([top, top], axis=1)
        return jnp.where(mask, both, 0.0)

    stage = []
    for k in range(CHUNKS):
        rows = jnp.concatenate([stacked(left1, k), stacked(left2, k)], axis=0)
        part = slice(CHUNK * k, CHUNK * (k + 1))
        cols = jnp.concatenate([right1[part], right2[part]], axis=0)
        g = exact(rows, cols, NT)
        a = square(g[:128, :64], strict)
        kb = square(g[:128, 64:], strict)
        ru = square(g[128:, :64], upto)
        ku = square(g[128:, 64:], upto)
        stage.append([a, kb, ru, ku])
    inverse = []
    for k in range(CHUNKS):
        a = stage[k][0]
        small = jnp.where(in16, a, 0.0)
        power = small
        t = eye + small
        for _ in range(3):
            power = exact(power, power)
            t = t + exact(t, power)
        t = t + exact(exact(t, jnp.where(in32 & ~in16, a, 0.0)), t)
        t = t + exact(exact(t, jnp.where(in32, 0.0, a)), t)
        inverse.append(t)
    pair = jnp.concatenate([jnp.zeros((128, 128), F32), eye], axis=0)
    for k in range(CHUNKS):
        _, kb, ru, ku = stage[k]
        v = stacked(value, k)
        xy = exact(inverse[k], jnp.concatenate([stacked(start1, k), exact(kb, v)], axis=1))
        read = exact(ru, xy)
        coef = stacked(start2, k) + read[:, :128]
        rest = read[:, 128:] + exact(ku, v)
        t1, t2 = stacked(tail1, k), stacked(tail2, k)
        moved = exact(xy, t1, TN)
        decay = whole[CHUNK * k : CHUNK * k + 1]
        step = moved[:128] + jnp.where(rr == cc, decay, 0.0)
        add = moved[128:] + exact(v, t2, TN)
        out = exact(coef, pair, NT)
        near = out[:, :128] + rest
        far = out[:, 128:]
        part = slice(CHUNK * k, CHUNK * (k + 1))
        free[part] = near[:64] + near[64:]
        along[part] = far[:64] + far[64:]
        pair = exact(pair, step) + jnp.concatenate([add, jnp.zeros((128, 128), F32)], axis=0)
    state[0] = (pair[128:192] + pair[192:]).astype(BF16)
    state[1] = (pair[:64] + pair[64:128]).astype(BF16)


def recur(*args):
    wide = jax.ShapeDtypeStruct((ROWS, 128), F32)
    outs = [wide, wide, wide, jax.ShapeDtypeStruct((2, 64, 128), BF16)]
    return call(recur_body, outs, args, 8 << 30)


def attend_body(place, q, own, peer, w, glat, gain, table, att, logs, acc, top):
    sp = place[0]
    factor = np.float32(QK**-0.5 * np.log2(np.e))
    ones = jnp.where(iota((NOPE, ROWS), 0) == 0, 1.0, 0.0).astype(BF16)

    def block(j, first):
        lat = jnp.concatenate(
            [own[:, j, 0:32, :].reshape(128, ROWS), peer[:, j, 0:32, :].reshape(128, ROWS)], axis=0
        ).astype(F32)
        rope = (own[:, j, 32:40, :].astype(F32) + peer[:, j, 32:40, :].astype(F32)).reshape(
            ROPE, ROWS
        )
        lat = lat * lax.rsqrt(jnp.mean(lat * lat, axis=0, keepdims=True) + EPS) * glat[...]
        kv = dot(w[...], lat.astype(BF16)).astype(BF16)
        rope_sum = jnp.sum(rope * rope, axis=0, keepdims=True)
        turn = table[j]
        cosine, sine = turn[:16], turn[16:]
        ra, rb = rope[:16] * gain[64:80], rope[16:] * gain[80:96]
        ra, rb = ra * cosine - rb * sine, rb * cosine + ra * sine
        for h in range(2):
            k = kv[64 * h : 64 * (h + 1)].astype(F32)
            scale = lax.rsqrt(
                (jnp.sum(k * k, axis=0, keepdims=True) + rope_sum) * np.float32(1 / QK) + EPS
            )
            ready = jnp.concatenate(
                [k * scale * gain[0:64], ra * scale, rb * scale], axis=0
            ).astype(BF16)
            s = dot(q[h, :, 0:QK], ready) * factor
            if first:
                s = jnp.where(iota((ROWS, ROWS), 1) <= iota((ROWS, ROWS), 0), s, -jnp.inf)
            peak = jnp.max(s, axis=1, keepdims=True)
            v = jnp.concatenate([kv[128 + 64 * h : 192 + 64 * h], ones], axis=0)
            if first:
                top[h] = jnp.broadcast_to(peak, (ROWS, 128))
                acc[h] = dot(jnp.exp2(s - peak).astype(BF16), v, NT)
            else:
                old = top[h]
                new = jnp.maximum(old, peak)
                top[h] = new
                p = jnp.exp2(s - new[:, 0:1]).astype(BF16)
                acc[h] = acc[h] * jnp.exp2(old - new) + dot(p, v, NT)

    block(sp, True)

    def loop(j, carry):
        block(j, False)
        return carry

    lax.fori_loop(0, sp, loop, 0)
    parts = []
    rows = []
    for h in range(2):
        total = acc[h][:, 64:65]
        parts.append(acc[h][:, 0:64] / total)
        full = top[h] * np.float32(np.log(2.0)) + jnp.log(jnp.broadcast_to(total, (ROWS, 128)))
        rows.append(full.T[0:1])
    att[...] = jnp.concatenate(parts, axis=1).astype(BF16)
    logs[...] = jnp.concatenate(rows, axis=0)


def attend(*args):
    outs = [jax.ShapeDtypeStruct((ROWS, 128), BF16), jax.ShapeDtypeStruct((2, ROWS), F32)]
    scratch = [pltpu.VMEM((2, ROWS, 128), F32), pltpu.VMEM((2, ROWS, 128), F32)]
    return call(attend_body, outs, args, 8 << 30, scratch, [SMEM] + [VMEM] * 7)


def merge_body(place, att, free, along, bonus, states, branch, wo, out):
    head = iota((128, 128), 0) // 64 == iota((128, 128), 1) // 64

    def spread(v):
        return jnp.where(head, jnp.concatenate([v, v], axis=0), jnp.zeros((), v.dtype))

    def step(r, entering):
        return dot_wide(entering, spread(states[r, 0])) + spread(states[r, 1]).astype(F32)

    entering = lax.fori_loop(0, place[0], step, jnp.zeros((128, 128), F32))
    read = free[...] + exact(along[...], entering, NT)
    mean = jnp.where(head, 1.0 / 64, 0.0).astype(BF16)
    read = read - dot_wide(read, mean)
    spread_of = dot_wide(read * read, mean)
    rec = read * lax.rsqrt(spread_of + GROUP_EPS) * branch[...] + bonus[...]
    both = jnp.concatenate([att[...], rec.astype(BF16)], axis=1)
    for f in range(4):
        out[:, 512 * f : 512 * (f + 1)] = dot(both, wo[f]).astype(BF16)


def merge(*args):
    outs = jax.ShapeDtypeStruct((ROWS, 2048), BF16)
    return call(merge_body, outs, args, 4 << 30, specs=[SMEM] + [VMEM] * 7)


def from_everyone(value, axis, groups=None):
    count = len(groups[0]) if groups else lax.axis_size(axis)
    return lax.all_to_all(
        jnp.broadcast_to(value[None], (count, *value.shape)),
        axis,
        0,
        0,
        axis_index_groups=groups,
        tiled=True,
    )


def other_core(value):
    return lax.ppermute(value, "tp", [(i, i ^ 1) for i in range(8)])


def turn_table():
    half = ROPE // 2
    inverse = np.float32(10000.0) ** (-np.arange(half, dtype=np.float32) / np.float32(half))
    angle = np.arange(4096, dtype=np.float32)[:, None] * inverse.astype(np.float32)[None, :]
    both = np.concatenate([np.cos(angle), np.sin(angle)], axis=1).astype(np.float32)
    return both.reshape(16, ROWS, ROPE).transpose(0, 2, 1)


def shards(
    entering,
    entering_gain,
    wq,
    wc,
    wr,
    compact_gain,
    wk_up,
    wv_up,
    q_gain,
    k_gain,
    w_accept,
    w_key,
    w_value,
    fade1,
    fade2,
    fade_bias,
    fade_mult,
    fade_extra,
    adapt1,
    adapt2,
    adapt_bias,
    present,
    branch,
    wo_att,
    wo_rec,
):
    tp = lax.axis_index("tp")
    sp = lax.axis_index("sp")
    core = lax.rem(tp, 2)
    place = jnp.stack([sp, tp]).astype(jnp.int32)
    own_cols = lax.dynamic_slice_in_dim(wc, tp * 32, 32, 1)
    joined = jnp.concatenate([w_accept, w_key, w_value, wq, own_cols, wr], axis=1)
    weights = from_everyone(joined, "fs").reshape(2048, 640)
    x = entering[0].astype(F32)
    x = x * lax.rsqrt(jnp.mean(x * x, axis=-1, keepdims=True) + EPS) * entering_gain
    normed = from_everyone(x.astype(BF16), "tp").reshape(ROWS, 2048)
    table = jnp.asarray(turn_table())
    rkv, pay, q, dlow, rlow = project(
        place, normed, weights, fade1, adapt1, table, q_gain.reshape(QK, 1)
    )
    lat = from_everyone(pay, "sp")
    same_core = [[0, 2, 4, 6], [1, 3, 5, 7]]
    lat_own = from_everyone(lat, "tp", same_core)
    lat_peer = other_core(lat_own)
    free, along, bonus, state = recur(
        rkv,
        dlow,
        rlow,
        fade2,
        fade_bias.reshape(1, 128),
        adapt2,
        adapt_bias.reshape(1, 128),
        jnp.repeat(fade_mult[0, :, 0], 64).reshape(1, 128),
        fade_extra[0].T,
        present.reshape(1, 128),
    )
    states = from_everyone(state, "sp")

    def reordered(v):
        v = v.reshape(4, 2, 32, *v.shape[1:])
        v = jnp.where(core == 0, v, v[:, ::-1])
        return jnp.moveaxis(v, 1, 0).reshape(256, *v.shape[3:])

    up = reordered(jnp.concatenate([wk_up, wv_up], axis=1)).T
    att, logs = attend(
        place,
        q,
        lat_own,
        lat_peer,
        up,
        reordered(compact_gain).reshape(256, 1),
        k_gain.reshape(QK, 1),
        table,
    )
    wo = from_everyone(jnp.concatenate([wo_att, wo_rec], axis=0), "fs")
    partial = merge(place, att, free, along, bonus, states, branch.reshape(1, 128), wo)
    parts = lax.all_to_all(partial.reshape(8, 32, 2048), "tp", 0, 0, tiled=True)
    mixed = jnp.sum(parts.astype(F32), axis=0).astype(BF16)
    return mixed[None], logs[None]


def solution(mesh):
    placed = (
        P("fs", ("sp", "tp"), None),
        P(),
        P("fs", "tp"),
        P("fs", None),
        P("fs", None),
        P(),
        P(None, "tp"),
        P(None, "tp"),
        P(),
        P(),
        P("fs", "tp"),
        P("fs", "tp"),
        P("fs", "tp"),
        P(),
        P(None, "tp"),
        P("tp"),
        P("fs", "tp", "sp"),
        P("fs", "tp", "sp"),
        P(),
        P(None, "tp"),
        P("tp"),
        P("tp", None),
        P("tp"),
        P("tp", "fs"),
        P("tp", "fs"),
    )
    return jax.shard_map(
        shards,
        mesh=mesh,
        in_specs=placed,
        out_specs=(P("fs", ("sp", "tp"), None), P("fs", "tp", "sp")),
        check_vma=False,
    )
```

```python
import jax
import jax.numpy as jnp
import numpy as np
from jax import lax
from jax.experimental import pallas as pl
from jax.experimental.pallas import tpu as pltpu
from jax.sharding import PartitionSpec as P


F32 = jnp.float32
BF16 = jnp.bfloat16

ROWS = 256
NOPE = 64
ROPE = 32
QK = NOPE + ROPE
CHUNK = 64
CHUNKS = ROWS // CHUNK
EPS = 1e-6
GROUP_EPS = 0.00064
NN = (((1,), (0,)), ((), ()))
NT = (((1,), (1,)), ((), ()))
TN = (((0,), (0,)), ((), ()))

VMEM = pl.BlockSpec(memory_space=pltpu.VMEM)
SMEM = pl.BlockSpec(memory_space=pltpu.SMEM)
ANY = pl.BlockSpec(memory_space=pl.ANY)


def dot(a, b, dims=NN):
    return lax.dot_general(a, b, dims, preferred_element_type=F32)


def halves(a):
    high = a.astype(BF16)
    return high, (a - high.astype(F32)).astype(BF16)


def fine(a, b, dims=NN):
    (i,), (j,) = dims[0]
    ah, al = halves(a)
    bh, bl = halves(b)
    wide = dot(jnp.concatenate([ah, al], axis=i), jnp.concatenate([bh, bh], axis=j), dims)
    return wide + dot(ah, bl, dims)


def dot_wide(a, b):
    high, low = halves(a)
    return dot(jnp.concatenate([high, low], axis=1), jnp.concatenate([b, b], axis=0))


def iota(shape, dim):
    return lax.broadcasted_iota(jnp.int32, shape, dim)


def call(body, outs, args, flops, scratch=(), specs=None, limit=24):
    return pl.pallas_call(
        body,
        out_shape=outs,
        in_specs=specs or [VMEM] * len(args),
        out_specs=jax.tree.map(lambda _: VMEM, outs),
        scratch_shapes=scratch,
        compiler_params=pltpu.CompilerParams(vmem_limit_bytes=limit << 20),
        cost_estimate=pl.CostEstimate(flops=flops, bytes_accessed=4 << 20, transcendentals=0),
    )(*args)


def turned(n, table):
    half = ROPE // 2
    a, b = n[NOPE : NOPE + half], n[NOPE + half :]
    cosine, sine = table[:half], table[half:]
    return a * cosine - b * sine, b * cosine + a * sine


def prepare_body(place, x, gain, wa, wk, wv, wq, wc, wr, xs, small, big, turned_wc):
    v = x[...].astype(F32)
    v = v * lax.rsqrt(jnp.mean(v * v, axis=-1, keepdims=True) + EPS) * gain[...]
    v = v.astype(BF16)
    for i in range(8):
        xs[i] = v
    turned_wc[...] = wc[...].astype(F32).T
    start = pl.multiple_of(place[1] * 32, 32)
    small[0:32] = turned_wc[pl.ds(start, 32), :].astype(BF16)
    small[32:64] = wr[...]
    big[:, 0:128] = wa[...]
    big[:, 128:256] = wk[...]
    big[:, 256:384] = wv[...]
    big[0:192, 384:640] = wq[:, 0:256]
    big[192:384, 384:640] = wq[:, 256:512]
    big[384:512, 384:640] = jnp.zeros((128, 256), BF16)


def prepare(*args):
    outs = [
        jax.ShapeDtypeStruct((8, 32, 2048), BF16),
        jax.ShapeDtypeStruct((64, 512), BF16),
        jax.ShapeDtypeStruct((512, 640), BF16),
    ]
    scratch = [pltpu.VMEM((256, 512), F32)]
    return call(prepare_body, outs, args, 1 << 29, scratch, [SMEM] + [VMEM] * 8)


def columns(place, k):
    shard = lax.rem(place[2] + (0, 3, 1, 2)[k], 4)
    return pl.ds(pl.multiple_of(shard * 512, 512), 512)


def latents_body(place, x, w0, w1, w2, w3, pay):
    t = jnp.zeros((64, ROWS), F32)
    for k, w in enumerate((w0, w1, w2, w3)):
        t += dot(w[...], x[:, columns(place, k)], NT)
    tp = place[1]
    group = jnp.zeros((8, ROWS), F32)
    for g in range(4):
        group += jnp.where(tp // 2 == g, t[32 + 8 * g : 40 + 8 * g], 0.0)
    group = jnp.where(iota((8, ROWS), 0) // 4 == lax.rem(tp, 2), group, 0.0)
    both = jnp.concatenate([t[0:32], group], axis=0).astype(BF16)
    for i in range(16):
        pay[i] = both


def latents(*args):
    outs = jax.ShapeDtypeStruct((16, 40, ROWS), BF16)
    return call(latents_body, outs, args, 1 << 29, specs=[SMEM] + [VMEM] * 5)


def project_body(
    place, x, w0, w1, w2, w3, fd, fa, table, gain, up, glat, kgain, mult, extra, present,
    rkv, q, dlow, rlow,
):
    y = jnp.zeros((ROWS, 384), F32)
    t = jnp.zeros((192, ROWS), F32)
    for k, w in enumerate((w0, w1, w2, w3)):
        part = x[:, columns(place, k)]
        y += dot(part, w[:, 0:384])
        t += dot(jnp.concatenate([w[0:192, 384:640], w[192:384, 384:640]], axis=1), part, NT)
    rkv[...] = y.astype(BF16)
    t = t.astype(BF16).astype(F32)
    turn = table[place[0]]
    for h in range(2):
        v = t[QK * h : QK * (h + 1)]
        n = v * lax.rsqrt(jnp.mean(v * v, axis=0, keepdims=True) + EPS) * gain[...]
        a, b = turned(n, turn)
        ready = jnp.concatenate([n[:NOPE], a, b, jnp.zeros((128 - QK, ROWS), F32)], axis=0)
        q[h] = ready.T.astype(BF16)
    dlow[...] = jnp.tanh(dot(x[...], fd[...]).astype(BF16).astype(F32)).astype(BF16)
    rlow[...] = dot(x[...], fa[...]).astype(BF16)


def project(*args):
    outs = [
        jax.ShapeDtypeStruct((ROWS, 384), BF16),
        jax.ShapeDtypeStruct((2, ROWS, 128), BF16),
        jax.ShapeDtypeStruct((ROWS, 128), BF16),
        jax.ShapeDtypeStruct((ROWS, 128), BF16),
    ]
    return call(project_body, outs, args, 4 << 30, specs=[SMEM] + [VMEM] * 9 + [ANY] * 6)


def recur_body(rkv, dlow, rlow, wd, bd, wa, ba, mult, extra, present, free, along, bonus, state):
    lane = iota((ROWS, 128), 1)
    recept, key, value = (rkv[:, 128 * i : 128 * (i + 1)].astype(F32) for i in range(3))
    speed = jax.nn.sigmoid(bd[...] + dot(dlow[...], wd[...])) * np.float32(np.exp(-0.5))
    added = jnp.where(lane < 64, extra[:, 0:1], extra[:, 1:2])
    ld = added - speed * mult[...]
    learn = jax.nn.sigmoid(ba[...] + dot(rlow[...], wa[...]))
    same = (iota((128, 128), 0) // 64 == iota((128, 128), 1) // 64).astype(BF16)
    unit = key * lax.rsqrt(dot_wide(key * key, same) + EPS)
    bonus[...] = dot_wide(recept * key * present[...], same) * value
    r, c = iota((ROWS, ROWS), 0), iota((ROWS, ROWS), 1)
    block = r // CHUNK == c // CHUNK
    sums = jnp.concatenate(
        [
            jnp.where(block & (c <= r), 1.0, 0.0),
            jnp.where(block & (lax.rem(c, CHUNK) < CHUNK // 2), 1.0, 0.0),
            jnp.where(block, 1.0, 0.0),
        ],
        axis=0,
    )
    sums = sums.astype(BF16)
    high, low = halves(ld)
    last = (ld - high.astype(F32) - low.astype(F32)).astype(BF16)
    sums = dot(
        jnp.concatenate([sums, sums, sums], axis=1), jnp.concatenate([high, low, last], axis=0)
    )
    cum, mid, end = sums[:ROWS], sums[ROWS : 2 * ROWS], sums[2 * ROWS :]
    prev = cum - ld
    toward = -unit
    remove = unit * learn
    grow, shrink = jnp.exp(cum - mid), jnp.exp(mid - cum)
    left1, left2 = toward * jnp.exp(prev - mid), recept * grow
    right1, right2 = remove * shrink, key * shrink
    start1, start2 = toward * jnp.exp(prev), recept * jnp.exp(cum)
    tail = jnp.exp(end - cum)
    tail1, tail2 = remove * tail, key * tail
    whole = jnp.exp(end)
    m0 = iota((CHUNK, 128), 1) < 64

    def stacked(v, k):
        v = v[CHUNK * k : CHUNK * (k + 1)]
        return jnp.concatenate([jnp.where(m0, v, 0.0), jnp.where(m0, 0.0, v)], axis=0)

    rr, cc = iota((128, 128), 0), iota((128, 128), 1)
    head = rr // 64 == cc // 64
    eye = jnp.where(rr == cc, 1.0, 0.0)
    in16, in32 = rr // 16 == cc // 16, rr // 32 == cc // 32
    strict, upto = head & (rr > cc), head & (rr >= cc)

    def square(top, mask):
        both = jnp.concatenate([top, top], axis=1)
        return jnp.where(mask, both, 0.0)

    stage = []
    for k in range(CHUNKS):
        rows = jnp.concatenate([stacked(left1, k), stacked(left2, k)], axis=0)
        part = slice(CHUNK * k, CHUNK * (k + 1))
        cols = jnp.concatenate([right1[part], right2[part]], axis=0)
        g = fine(rows, cols, NT)
        a = square(g[:128, :64], strict)
        kb = square(g[:128, 64:], strict)
        ru = square(g[128:, :64], upto)
        ku = square(g[128:, 64:], upto)
        stage.append([a, kb, ru, ku])
    inverse = []
    for k in range(CHUNKS):
        a = stage[k][0]
        small = jnp.where(in16, a, 0.0)
        power = small
        t = eye + small
        for _ in range(3):
            power = fine(power, power)
            t = t + fine(t, power)
        t = t + fine(fine(t, jnp.where(in32 & ~in16, a, 0.0)), t)
        t = t + fine(fine(t, jnp.where(in32, 0.0, a)), t)
        inverse.append(t)
    pair = jnp.concatenate([jnp.zeros((128, 128), F32), eye], axis=0)
    for k in range(CHUNKS):
        _, kb, ru, ku = stage[k]
        v = stacked(value, k)
        xy = fine(inverse[k], jnp.concatenate([stacked(start1, k), fine(kb, v)], axis=1))
        read = fine(ru, xy)
        coef = stacked(start2, k) + read[:, :128]
        rest = read[:, 128:] + fine(ku, v)
        t1, t2 = stacked(tail1, k), stacked(tail2, k)
        moved = fine(xy, t1, TN)
        decay = whole[CHUNK * k : CHUNK * k + 1]
        step = moved[:128] + jnp.where(rr == cc, decay, 0.0)
        add = moved[128:] + fine(v, t2, TN)
        out = fine(coef, pair, NT)
        near = out[:, :128] + rest
        far = out[:, 128:]
        part = slice(CHUNK * k, CHUNK * (k + 1))
        free[part] = near[:64] + near[64:]
        along[part] = far[:64] + far[64:]
        pair = fine(pair, step) + jnp.concatenate([add, jnp.zeros((128, 128), F32)], axis=0)
    far = (pair[128:192] + pair[192:]).astype(BF16)
    near = (pair[:64] + pair[64:128]).astype(BF16)
    for i in range(16):
        state[i, 0] = far
        state[i, 1] = near


def recur(*args):
    wide = jax.ShapeDtypeStruct((ROWS, 128), F32)
    outs = [wide, wide, wide, jax.ShapeDtypeStruct((16, 2, 64, 128), BF16)]
    return call(recur_body, outs, args, 8 << 30)


def attend_body(place, q, own, peer, w, glat, gain, table, att, logs, acc, top):
    sp = place[0]
    factor = np.float32(QK**-0.5 * np.log2(np.e))
    ones = jnp.where(iota((NOPE, ROWS), 0) == 0, 1.0, 0.0).astype(BF16)

    def keys(j):
        lat = jnp.concatenate(
            [own[:, j, 0:32, :].reshape(128, ROWS), peer[:, j, 0:32, :].reshape(128, ROWS)], axis=0
        ).astype(F32)
        rope = (own[:, j, 32:40, :].astype(F32) + peer[:, j, 32:40, :].astype(F32)).reshape(
            ROPE, ROWS
        )
        lat = lat * lax.rsqrt(jnp.mean(lat * lat, axis=0, keepdims=True) + EPS) * glat[...]
        kv = dot(w[...], lat.astype(BF16)).astype(BF16)
        rope_sum = jnp.sum(rope * rope, axis=0, keepdims=True)
        turn = table[j]
        cosine, sine = turn[:16], turn[16:]
        ra, rb = rope[:16] * gain[64:80], rope[16:] * gain[80:96]
        ra, rb = ra * cosine - rb * sine, rb * cosine + ra * sine
        ready, values = [], []
        for h in range(2):
            k = kv[64 * h : 64 * (h + 1)].astype(F32)
            scale = lax.rsqrt(
                (jnp.sum(k * k, axis=0, keepdims=True) + rope_sum) * np.float32(1 / QK) + EPS
            )
            ready.append(
                jnp.concatenate([k * scale * gain[0:64], ra * scale, rb * scale], axis=0).astype(
                    BF16
                )
            )
            values.append(jnp.concatenate([kv[128 + 64 * h : 192 + 64 * h], ones], axis=0))
        return ready, values

    def block(places, first):
        made = [keys(j) for j in places]
        for h in range(2):
            ready = jnp.concatenate([m[0][h] for m in made], axis=1)
            v = jnp.concatenate([m[1][h] for m in made], axis=1)
            s = dot(q[h, :, 0:QK], ready) * factor
            if first:
                s = jnp.where(iota((ROWS, ROWS), 1) <= iota((ROWS, ROWS), 0), s, -jnp.inf)
            peak = jnp.max(s, axis=1, keepdims=True)
            if first:
                top[h] = jnp.broadcast_to(peak, (ROWS, 128))
                acc[h] = dot(jnp.exp2(s - peak).astype(BF16), v, NT)
            else:
                old = top[h]
                new = jnp.maximum(old, peak)
                top[h] = new
                p = jnp.exp2(s - new[:, 0:1]).astype(BF16)
                acc[h] = acc[h] * jnp.exp2(old - new) + dot(p, v, NT)

    block([sp], True)

    def loop(i, carry):
        block([2 * i, 2 * i + 1], False)
        return carry

    lax.fori_loop(0, sp // 2, loop, 0)

    @pl.when(lax.rem(sp, 2) == 1)
    def _():
        block([sp - 1], False)

    parts = []
    rows = []
    for h in range(2):
        total = acc[h][:, 64:65]
        parts.append(acc[h][:, 0:64] / total)
        full = top[h] * np.float32(np.log(2.0)) + jnp.log(jnp.broadcast_to(total, (ROWS, 128)))
        rows.append(full.T[0:1])
    att[...] = jnp.concatenate(parts, axis=1).astype(BF16)
    logs[...] = jnp.concatenate(rows, axis=0)


def attend(*args):
    outs = [jax.ShapeDtypeStruct((ROWS, 128), BF16), jax.ShapeDtypeStruct((2, ROWS), F32)]
    scratch = [pltpu.VMEM((2, ROWS, 128), F32), pltpu.VMEM((2, ROWS, 128), F32)]
    return call(attend_body, outs, args, 8 << 30, scratch, [SMEM] + [VMEM] * 7)


def merge_body(place, att, free, along, bonus, states, branch, o0, o1, o2, o3, out):
    head = iota((128, 128), 0) // 64 == iota((128, 128), 1) // 64

    def spread(v):
        return jnp.where(head, jnp.concatenate([v, v], axis=0), jnp.zeros((), v.dtype))

    def step(r, entering):
        return dot_wide(entering, spread(states[r, 0])) + spread(states[r, 1]).astype(F32)

    entering = lax.fori_loop(0, place[0], step, jnp.zeros((128, 128), F32))
    read = free[...] + fine(along[...], entering, NT)
    mean = jnp.where(head, 1.0 / 64, 0.0).astype(BF16)
    read = read - dot_wide(read, mean)
    spread_of = dot_wide(read * read, mean)
    rec = read * lax.rsqrt(spread_of + GROUP_EPS) * branch[...] + bonus[...]
    both = jnp.concatenate([att[...], rec.astype(BF16)], axis=1)
    for k, o in enumerate((o0, o1, o2, o3)):
        out[:, columns(place, k)] = dot(both, o[...]).astype(BF16)


def merge(*args):
    outs = jax.ShapeDtypeStruct((ROWS, 2048), BF16)
    return call(merge_body, outs, args, 4 << 30, specs=[SMEM] + [VMEM] * 10)


def exchanged(copies, axis, groups=None):
    return lax.all_to_all(copies, axis, 0, 0, axis_index_groups=groups, tiled=True)


def around(value):
    moves = [[(i, (i + by) % 4) for i in range(4)] for by in (1, 3, 2)]
    return [value] + [lax.ppermute(value, "fs", move) for move in moves]


def other_core(value):
    return lax.ppermute(value, "tp", [(i, i ^ 1) for i in range(8)])


def turn_table():
    half = ROPE // 2
    inverse = np.float32(10000.0) ** (-np.arange(half, dtype=np.float32) / np.float32(half))
    angle = np.arange(4096, dtype=np.float32)[:, None] * inverse.astype(np.float32)[None, :]
    both = np.concatenate([np.cos(angle), np.sin(angle)], axis=1).astype(np.float32)
    return both.reshape(16, ROWS, ROPE).transpose(0, 2, 1)


def shards(
    entering,
    entering_gain,
    wq,
    wc,
    wr,
    compact_gain,
    wk_up,
    wv_up,
    q_gain,
    k_gain,
    w_accept,
    w_key,
    w_value,
    fade1,
    fade2,
    fade_bias,
    fade_mult,
    fade_extra,
    adapt1,
    adapt2,
    adapt_bias,
    present,
    branch,
    wo_att,
    wo_rec,
):
    tp = lax.axis_index("tp")
    sp = lax.axis_index("sp")
    core = lax.rem(tp, 2)
    place = jnp.stack([sp, tp, lax.axis_index("fs")]).astype(jnp.int32)
    xs, small, big = prepare(
        place,
        entering[0],
        entering_gain.reshape(1, 2048),
        w_accept,
        w_key,
        w_value,
        wq.T,
        wc,
        wr.T,
    )
    normed = exchanged(xs, "tp").reshape(ROWS, 2048)
    smalls = around(small)
    bigs = around(big)

    def reordered(v):
        v = v.reshape(4, 2, 32, *v.shape[1:])
        v = jnp.where(core == 0, v, v[:, ::-1])
        return jnp.moveaxis(v, 1, 0).reshape(256, *v.shape[3:])

    up = reordered(jnp.concatenate([wk_up, wv_up], axis=1)).T
    glat = reordered(compact_gain).reshape(256, 1)
    key_gain = k_gain.reshape(QK, 1)
    mult = jnp.repeat(fade_mult[0, :, 0], 64).reshape(1, 128)
    extra = fade_extra[0].T
    present = present.reshape(1, 128)
    table = jnp.asarray(turn_table())
    pay = latents(place, normed, *smalls)
    lat = exchanged(pay, "sp")
    wo = around(jnp.concatenate([wo_att, wo_rec], axis=0))
    projected = project(
        place,
        normed,
        *bigs,
        fade1,
        adapt1,
        table,
        q_gain.reshape(QK, 1),
        up,
        glat,
        key_gain,
        mult,
        extra,
        present,
    )
    lat, (rkv, q, dlow, rlow) = lax.optimization_barrier((lat, tuple(projected)))
    same_core = [[0, 2, 4, 6], [1, 3, 5, 7]]
    lat_own = exchanged(jnp.broadcast_to(lat[None], (4, *lat.shape)), "tp", same_core)
    recurrent = recur(
        rkv,
        dlow,
        rlow,
        fade2,
        fade_bias.reshape(1, 128),
        adapt2,
        adapt_bias.reshape(1, 128),
        mult,
        extra,
        present,
    )
    lat_own, (free, along, bonus, state) = lax.optimization_barrier((lat_own, tuple(recurrent)))
    states = exchanged(state, "sp")
    lat_peer = other_core(lat_own)
    att, logs = attend(place, q, lat_own, lat_peer, up, glat, key_gain, table)
    partial = merge(place, att, free, along, bonus, states, branch.reshape(1, 128), *wo)
    parts = exchanged(partial.reshape(8, 32, 2048), "tp")
    mixed = jnp.sum(parts.astype(F32), axis=0).astype(BF16)
    return mixed[None], logs[None]


def solution(mesh):
    placed = (
        P("fs", ("sp", "tp"), None),
        P(),
        P("fs", "tp"),
        P("fs", None),
        P("fs", None),
        P(),
        P(None, "tp"),
        P(None, "tp"),
        P(),
        P(),
        P("fs", "tp"),
        P("fs", "tp"),
        P("fs", "tp"),
        P(),
        P(None, "tp"),
        P("tp"),
        P("fs", "tp", "sp"),
        P("fs", "tp", "sp"),
        P(),
        P(None, "tp"),
        P("tp"),
        P("tp", None),
        P("tp"),
        P("tp", "fs"),
        P("tp", "fs"),
    )

    return jax.shard_map(
        shards,
        mesh=mesh,
        in_specs=placed,
        out_specs=(P("fs", ("sp", "tp"), None), P("fs", "tp", "sp")),
        check_vma=False,
    )
```

```python
import jax
import jax.numpy as jnp
import numpy as np
from jax import lax
from jax.experimental import pallas as pl
from jax.experimental.pallas import tpu as pltpu
from jax.sharding import PartitionSpec as P


F32 = jnp.float32
BF16 = jnp.bfloat16

ROWS = 256
NOPE = 64
ROPE = 32
QK = NOPE + ROPE
CHUNK = 64
CHUNKS = ROWS // CHUNK
EPS = 1e-6
GROUP_EPS = 0.00064
NN = (((1,), (0,)), ((), ()))
NT = (((1,), (1,)), ((), ()))
TN = (((0,), (0,)), ((), ()))

VMEM = pl.BlockSpec(memory_space=pltpu.VMEM)
SMEM = pl.BlockSpec(memory_space=pltpu.SMEM)
ANY = pl.BlockSpec(memory_space=pl.ANY)
HBM = pl.BlockSpec(memory_space=pltpu.HBM)


def dot(a, b, dims=NN):
    return lax.dot_general(a, b, dims, preferred_element_type=F32)


def halves(a):
    high = a.astype(BF16)
    return high, (a - high.astype(F32)).astype(BF16)


def fine(a, b, dims=NN):
    (i,), (j,) = dims[0]
    ah, al = halves(a)
    bh, bl = halves(b)
    wide = dot(jnp.concatenate([ah, al], axis=i), jnp.concatenate([bh, bh], axis=j), dims)
    return wide + dot(ah, bl, dims)


def dot_wide(a, b):
    high, low = halves(a)
    return dot(jnp.concatenate([high, low], axis=1), jnp.concatenate([b, b], axis=0))


def iota(shape, dim):
    return lax.broadcasted_iota(jnp.int32, shape, dim)


def call(body, outs, args, flops, scratch=(), specs=None, limit=24):
    return pl.pallas_call(
        body,
        out_shape=outs,
        in_specs=specs or [VMEM] * len(args),
        out_specs=jax.tree.map(lambda _: VMEM, outs),
        scratch_shapes=scratch,
        compiler_params=pltpu.CompilerParams(vmem_limit_bytes=int(limit * (1 << 20))),
        cost_estimate=pl.CostEstimate(flops=flops, bytes_accessed=4 << 20, transcendentals=0),
    )(*args)


def turned(n, table):
    half = ROPE // 2
    a, b = n[NOPE : NOPE + half], n[NOPE + half :]
    cosine, sine = table[:half], table[half:]
    return a * cosine - b * sine, b * cosine + a * sine


def prepare_body(
    place, x_in, gain_in, wa_in, wk_in, wv_in, wq_in, wc_in, wr_in, xs, small, big,
    x, gain, wa, wk, wv, wq, wc, wr, turned_wc, arrived,
):
    pairs = [
        (x_in, x), (gain_in, gain), (wc_in, wc), (wr_in, wr),
        (wa_in, wa), (wk_in, wk), (wv_in, wv), (wq_in, wq),
    ]
    copies = [pltpu.make_async_copy(a, b, arrived.at[i]) for i, (a, b) in enumerate(pairs)]
    for copy in copies:
        copy.start()
    copies[0].wait()
    copies[1].wait()
    v = x[...].astype(F32)
    v = v * lax.rsqrt(jnp.mean(v * v, axis=-1, keepdims=True) + EPS) * gain[...]
    v = v.astype(BF16)
    for i in range(8):
        xs[i] = v
    copies[2].wait()
    copies[3].wait()
    turned_wc[...] = wc[...].astype(F32).T
    start = pl.multiple_of(place[1] * 32, 32)
    small[0:32] = turned_wc[pl.ds(start, 32), :].astype(BF16)
    small[32:64] = wr[...]
    for copy in copies[4:]:
        copy.wait()
    big[:, 0:128] = wa[...]
    big[:, 128:256] = wk[...]
    big[:, 256:384] = wv[...]
    big[0:192, 384:640] = wq[:, 0:256]
    big[192:384, 384:640] = wq[:, 256:512]
    big[384:512, 384:640] = jnp.zeros((128, 256), BF16)


def prepare(*args):
    outs = [
        jax.ShapeDtypeStruct((8, 32, 2048), BF16),
        jax.ShapeDtypeStruct((64, 512), BF16),
        jax.ShapeDtypeStruct((512, 640), BF16),
    ]
    scratch = [pltpu.VMEM(a.shape, a.dtype) for a in args[1:]]
    scratch += [pltpu.VMEM((256, 512), F32), pltpu.SemaphoreType.DMA((8,))]
    return call(prepare_body, outs, args, 1 << 29, scratch, [SMEM] + [HBM] * 8, 63.9)


def fan_body(value, out):
    v = value[...]
    for i in range(4):
        out[i] = v


def fan(value):
    return call(fan_body, jax.ShapeDtypeStruct((4, *value.shape), value.dtype), (value,), 1 << 29)


def lowrank_body(place, x, fd, fa, table, dlow, rlow, turn):
    dlow[...] = jnp.tanh(dot(x[...], fd[...]).astype(BF16).astype(F32)).astype(BF16)
    rlow[...] = dot(x[...], fa[...]).astype(BF16)
    turn[...] = table[place[0]]


def lowrank(*args):
    outs = [
        jax.ShapeDtypeStruct((ROWS, 128), BF16),
        jax.ShapeDtypeStruct((ROWS, 128), BF16),
        jax.ShapeDtypeStruct((ROPE, ROWS), F32),
    ]
    return call(lowrank_body, outs, args, 1 << 29, specs=[SMEM] + [VMEM] * 4)


def columns(place, k):
    shard = lax.rem(place[2] + (0, 3, 1, 2)[k], 4)
    return pl.ds(pl.multiple_of(shard * 512, 512), 512)


def latents_body(place, x, w0, w1, w2, w3, pay):
    t = jnp.zeros((64, ROWS), F32)
    for k, w in enumerate((w0, w1, w2, w3)):
        t += dot(w[...], x[:, columns(place, k)], NT)
    tp = place[1]
    group = jnp.zeros((8, ROWS), F32)
    for g in range(4):
        group += jnp.where(tp // 2 == g, t[32 + 8 * g : 40 + 8 * g], 0.0)
    group = jnp.where(iota((8, ROWS), 0) // 4 == lax.rem(tp, 2), group, 0.0)
    both = jnp.concatenate([t[0:32], group], axis=0).astype(BF16)
    for i in range(16):
        pay[i] = both


def latents(*args):
    outs = jax.ShapeDtypeStruct((16, 40, ROWS), BF16)
    return call(latents_body, outs, args, 1 << 29, specs=[SMEM] + [VMEM] * 5)


def project_body(
    place, x, w0, w1, w2, w3, turn, gain, up, glat, kgain, mult, extra, present, rkv, q,
):
    y = jnp.zeros((ROWS, 384), F32)
    t = jnp.zeros((192, ROWS), F32)
    for k, w in enumerate((w0, w1, w2, w3)):
        part = x[:, columns(place, k)]
        y += dot(part, w[:, 0:384])
        t += dot(jnp.concatenate([w[0:192, 384:640], w[192:384, 384:640]], axis=1), part, NT)
    rkv[...] = y.astype(BF16)
    t = t.astype(BF16).astype(F32)
    for h in range(2):
        v = t[QK * h : QK * (h + 1)]
        n = v * lax.rsqrt(jnp.mean(v * v, axis=0, keepdims=True) + EPS) * gain[...]
        a, b = turned(n, turn[...])
        ready = jnp.concatenate([n[:NOPE], a, b, jnp.zeros((128 - QK, ROWS), F32)], axis=0)
        q[h] = ready.T.astype(BF16)


def project(*args):
    outs = [
        jax.ShapeDtypeStruct((ROWS, 384), BF16),
        jax.ShapeDtypeStruct((2, ROWS, 128), BF16),
    ]
    return call(project_body, outs, args, 4 << 30, specs=[SMEM] + [VMEM] * 7 + [ANY] * 6)


def recur_body(rkv, dlow, rlow, wd, bd, wa, ba, mult, extra, present, free, along, bonus, state):
    lane = iota((ROWS, 128), 1)
    recept, key, value = (rkv[:, 128 * i : 128 * (i + 1)].astype(F32) for i in range(3))
    speed = jax.nn.sigmoid(bd[...] + dot(dlow[...], wd[...])) * np.float32(np.exp(-0.5))
    added = jnp.where(lane < 64, extra[:, 0:1], extra[:, 1:2])
    ld = added - speed * mult[...]
    learn = jax.nn.sigmoid(ba[...] + dot(rlow[...], wa[...]))
    same = (iota((128, 128), 0) // 64 == iota((128, 128), 1) // 64).astype(BF16)
    unit = key * lax.rsqrt(dot_wide(key * key, same) + EPS)
    bonus[...] = dot_wide(recept * key * present[...], same) * value
    r, c = iota((ROWS, ROWS), 0), iota((ROWS, ROWS), 1)
    block = r // CHUNK == c // CHUNK
    sums = jnp.concatenate(
        [
            jnp.where(block & (c <= r), 1.0, 0.0),
            jnp.where(block & (lax.rem(c, CHUNK) < CHUNK // 2), 1.0, 0.0),
            jnp.where(block, 1.0, 0.0),
        ],
        axis=0,
    )
    sums = sums.astype(BF16)
    high, low = halves(ld)
    last = (ld - high.astype(F32) - low.astype(F32)).astype(BF16)
    sums = dot(
        jnp.concatenate([sums, sums, sums], axis=1), jnp.concatenate([high, low, last], axis=0)
    )
    cum, mid, end = sums[:ROWS], sums[ROWS : 2 * ROWS], sums[2 * ROWS :]
    prev = cum - ld
    toward = -unit
    remove = unit * learn
    grow, shrink = jnp.exp(cum - mid), jnp.exp(mid - cum)
    left1, left2 = toward * jnp.exp(prev - mid), recept * grow
    right1, right2 = remove * shrink, key * shrink
    start1, start2 = toward * jnp.exp(prev), recept * jnp.exp(cum)
    tail = jnp.exp(end - cum)
    tail1, tail2 = remove * tail, key * tail
    whole = jnp.exp(end)
    m0 = iota((CHUNK, 128), 1) < 64

    def stacked(v, k):
        v = v[CHUNK * k : CHUNK * (k + 1)]
        return jnp.concatenate([jnp.where(m0, v, 0.0), jnp.where(m0, 0.0, v)], axis=0)

    rr, cc = iota((128, 128), 0), iota((128, 128), 1)
    head = rr // 64 == cc // 64
    eye = jnp.where(rr == cc, 1.0, 0.0)
    in16, in32 = rr // 16 == cc // 16, rr // 32 == cc // 32
    strict, upto = head & (rr > cc), head & (rr >= cc)

    def square(top, mask):
        both = jnp.concatenate([top, top], axis=1)
        return jnp.where(mask, both, 0.0)

    stage = []
    for k in range(CHUNKS):
        rows = jnp.concatenate([stacked(left1, k), stacked(left2, k)], axis=0)
        part = slice(CHUNK * k, CHUNK * (k + 1))
        cols = jnp.concatenate([right1[part], right2[part]], axis=0)
        g = fine(rows, cols, NT)
        a = square(g[:128, :64], strict)
        kb = square(g[:128, 64:], strict)
        ru = square(g[128:, :64], upto)
        ku = square(g[128:, 64:], upto)
        stage.append([a, kb, ru, ku])
    inverse = []
    for k in range(CHUNKS):
        a = stage[k][0]
        small = jnp.where(in16, a, 0.0)
        power = small
        t = eye + small
        for _ in range(3):
            power = fine(power, power)
            t = t + fine(t, power)
        t = t + fine(fine(t, jnp.where(in32 & ~in16, a, 0.0)), t)
        t = t + fine(fine(t, jnp.where(in32, 0.0, a)), t)
        inverse.append(t)
    pair = jnp.concatenate([jnp.zeros((128, 128), F32), eye], axis=0)
    for k in range(CHUNKS):
        _, kb, ru, ku = stage[k]
        v = stacked(value, k)
        xy = fine(inverse[k], jnp.concatenate([stacked(start1, k), fine(kb, v)], axis=1))
        read = fine(ru, xy)
        coef = stacked(start2, k) + read[:, :128]
        rest = read[:, 128:] + fine(ku, v)
        t1, t2 = stacked(tail1, k), stacked(tail2, k)
        moved = fine(xy, t1, TN)
        decay = whole[CHUNK * k : CHUNK * k + 1]
        step = moved[:128] + jnp.where(rr == cc, decay, 0.0)
        add = moved[128:] + fine(v, t2, TN)
        out = fine(coef, pair, NT)
        near = out[:, :128] + rest
        far = out[:, 128:]
        part = slice(CHUNK * k, CHUNK * (k + 1))
        free[part] = near[:64] + near[64:]
        along[part] = far[:64] + far[64:]
        pair = fine(pair, step) + jnp.concatenate([add, jnp.zeros((128, 128), F32)], axis=0)
    far = (pair[128:192] + pair[192:]).astype(BF16)
    near = (pair[:64] + pair[64:128]).astype(BF16)
    for i in range(16):
        state[i, 0] = far
        state[i, 1] = near


def recur(*args):
    wide = jax.ShapeDtypeStruct((ROWS, 128), F32)
    outs = [wide, wide, wide, jax.ShapeDtypeStruct((16, 2, 64, 128), BF16)]
    return call(recur_body, outs, args, 8 << 30, limit=60)


def attend_body(place, q, own, peer, w, glat, gain, table, att, logs, acc, top):
    sp = place[0]
    factor = np.float32(QK**-0.5 * np.log2(np.e))
    ones = jnp.where(iota((NOPE, ROWS), 0) == 0, 1.0, 0.0).astype(BF16)

    def keys(j):
        lat = jnp.concatenate(
            [own[:, j, 0:32, :].reshape(128, ROWS), peer[:, j, 0:32, :].reshape(128, ROWS)], axis=0
        ).astype(F32)
        rope = (own[:, j, 32:40, :].astype(F32) + peer[:, j, 32:40, :].astype(F32)).reshape(
            ROPE, ROWS
        )
        lat = lat * lax.rsqrt(jnp.mean(lat * lat, axis=0, keepdims=True) + EPS) * glat[...]
        kv = dot(w[...], lat.astype(BF16)).astype(BF16)
        rope_sum = jnp.sum(rope * rope, axis=0, keepdims=True)
        turn = table[j]
        cosine, sine = turn[:16], turn[16:]
        ra, rb = rope[:16] * gain[64:80], rope[16:] * gain[80:96]
        ra, rb = ra * cosine - rb * sine, rb * cosine + ra * sine
        ready, values = [], []
        for h in range(2):
            k = kv[64 * h : 64 * (h + 1)].astype(F32)
            scale = lax.rsqrt(
                (jnp.sum(k * k, axis=0, keepdims=True) + rope_sum) * np.float32(1 / QK) + EPS
            )
            ready.append(
                jnp.concatenate([k * scale * gain[0:64], ra * scale, rb * scale], axis=0).astype(
                    BF16
                )
            )
            values.append(jnp.concatenate([kv[128 + 64 * h : 192 + 64 * h], ones], axis=0))
        return ready, values

    def block(places, first):
        made = [keys(j) for j in places]
        for h in range(2):
            ready = jnp.concatenate([m[0][h] for m in made], axis=1)
            v = jnp.concatenate([m[1][h] for m in made], axis=1)
            s = dot(q[h, :, 0:QK], ready) * factor
            if first:
                s = jnp.where(iota((ROWS, ROWS), 1) <= iota((ROWS, ROWS), 0), s, -jnp.inf)
            peak = jnp.max(s, axis=1, keepdims=True)
            if first:
                top[h] = jnp.broadcast_to(peak, (ROWS, 128))
                acc[h] = dot(jnp.exp2(s - peak).astype(BF16), v, NT)
            else:
                old = top[h]
                new = jnp.maximum(old, peak)
                top[h] = new
                p = jnp.exp2(s - new[:, 0:1]).astype(BF16)
                acc[h] = acc[h] * jnp.exp2(old - new) + dot(p, v, NT)

    block([sp], True)

    def loop(i, carry):
        block([2 * i, 2 * i + 1], False)
        return carry

    lax.fori_loop(0, sp // 2, loop, 0)

    @pl.when(lax.rem(sp, 2) == 1)
    def _():
        block([sp - 1], False)

    parts = []
    rows = []
    for h in range(2):
        total = acc[h][:, 64:65]
        parts.append(acc[h][:, 0:64] / total)
        full = top[h] * np.float32(np.log(2.0)) + jnp.log(jnp.broadcast_to(total, (ROWS, 128)))
        rows.append(full.T[0:1])
    att[...] = jnp.concatenate(parts, axis=1).astype(BF16)
    logs[...] = jnp.concatenate(rows, axis=0)


def attend(*args):
    outs = [jax.ShapeDtypeStruct((ROWS, 128), BF16), jax.ShapeDtypeStruct((2, ROWS), F32)]
    scratch = [pltpu.VMEM((2, ROWS, 128), F32), pltpu.VMEM((2, ROWS, 128), F32)]
    return call(attend_body, outs, args, 8 << 30, scratch, [SMEM] + [VMEM] * 7)


def merge_body(place, att, free, along, bonus, states, branch, o0, o1, o2, o3, out):
    head = iota((128, 128), 0) // 64 == iota((128, 128), 1) // 64

    def spread(v):
        return jnp.where(head, jnp.concatenate([v, v], axis=0), jnp.zeros((), v.dtype))

    def step(r, entering):
        return dot_wide(entering, spread(states[r, 0])) + spread(states[r, 1]).astype(F32)

    entering = lax.fori_loop(0, place[0], step, jnp.zeros((128, 128), F32))
    read = free[...] + fine(along[...], entering, NT)
    mean = jnp.where(head, 1.0 / 64, 0.0).astype(BF16)
    read = read - dot_wide(read, mean)
    spread_of = dot_wide(read * read, mean)
    rec = read * lax.rsqrt(spread_of + GROUP_EPS) * branch[...] + bonus[...]
    both = jnp.concatenate([att[...], rec.astype(BF16)], axis=1)
    for k, o in enumerate((o0, o1, o2, o3)):
        out[:, columns(place, k)] = dot(both, o[...]).astype(BF16)


def merge(*args):
    outs = jax.ShapeDtypeStruct((ROWS, 2048), BF16)
    return call(merge_body, outs, args, 4 << 30, specs=[SMEM] + [VMEM] * 10)


def exchanged(copies, axis, groups=None):
    return lax.all_to_all(copies, axis, 0, 0, axis_index_groups=groups, tiled=True)


def around(value):
    moves = [[(i, (i + by) % 4) for i in range(4)] for by in (1, 3, 2)]
    return [value] + [lax.ppermute(value, "fs", move) for move in moves]


def other_core(value):
    return lax.ppermute(value, "tp", [(i, i ^ 1) for i in range(8)])


def turn_table():
    half = ROPE // 2
    inverse = np.float32(10000.0) ** (-np.arange(half, dtype=np.float32) / np.float32(half))
    angle = np.arange(4096, dtype=np.float32)[:, None] * inverse.astype(np.float32)[None, :]
    both = np.concatenate([np.cos(angle), np.sin(angle)], axis=1).astype(np.float32)
    return both.reshape(16, ROWS, ROPE).transpose(0, 2, 1)


def shards(
    entering,
    entering_gain,
    wq,
    wc,
    wr,
    compact_gain,
    wk_up,
    wv_up,
    q_gain,
    k_gain,
    w_accept,
    w_key,
    w_value,
    fade1,
    fade2,
    fade_bias,
    fade_mult,
    fade_extra,
    adapt1,
    adapt2,
    adapt_bias,
    present,
    branch,
    wo_att,
    wo_rec,
):
    tp = lax.axis_index("tp")
    sp = lax.axis_index("sp")
    core = lax.rem(tp, 2)
    place = jnp.stack([sp, tp, lax.axis_index("fs")]).astype(jnp.int32)
    xs, small, big = prepare(
        place,
        entering[0],
        entering_gain.reshape(1, 2048),
        w_accept,
        w_key,
        w_value,
        wq.T,
        wc,
        wr.T,
    )
    normed = exchanged(xs, "tp").reshape(ROWS, 2048)
    smalls = around(small)
    bigs = around(big)

    def reordered(v):
        v = v.reshape(4, 2, 32, *v.shape[1:])
        v = jnp.where(core == 0, v, v[:, ::-1])
        return jnp.moveaxis(v, 1, 0).reshape(256, *v.shape[3:])

    up = reordered(jnp.concatenate([wk_up, wv_up], axis=1)).T
    glat = reordered(compact_gain).reshape(256, 1)
    key_gain = k_gain.reshape(QK, 1)
    mult = jnp.repeat(fade_mult[0, :, 0], 64).reshape(1, 128)
    extra = fade_extra[0].T
    present = present.reshape(1, 128)
    table = jnp.asarray(turn_table())
    pay = latents(place, normed, *smalls)
    lat = exchanged(pay, "sp")
    dlow, rlow, turn = lowrank(place, normed, fade1, adapt1, table)
    wo = around(jnp.concatenate([wo_att, wo_rec], axis=0))
    projected = project(
        place,
        normed,
        *bigs,
        turn,
        q_gain.reshape(QK, 1),
        up,
        glat,
        key_gain,
        mult,
        extra,
        present,
    )
    lat, (rkv, q) = lax.optimization_barrier((lat, tuple(projected)))
    same_core = [[0, 2, 4, 6], [1, 3, 5, 7]]
    lat_own = exchanged(fan(lat), "tp", same_core)
    recurrent = recur(
        rkv,
        dlow,
        rlow,
        fade2,
        fade_bias.reshape(1, 128),
        adapt2,
        adapt_bias.reshape(1, 128),
        mult,
        extra,
        present,
    )
    lat_own, (free, along, bonus, state) = lax.optimization_barrier((lat_own, tuple(recurrent)))
    states = exchanged(state, "sp")
    lat_peer = other_core(lat_own)
    att, logs = attend(place, q, lat_own, lat_peer, up, glat, key_gain, table)
    partial = merge(place, att, free, along, bonus, states, branch.reshape(1, 128), *wo)
    parts = exchanged(partial.reshape(8, 32, 2048), "tp")
    mixed = jnp.sum(parts.astype(F32), axis=0).astype(BF16)
    return mixed[None], logs[None]


def solution(mesh):
    placed = (
        P("fs", ("sp", "tp"), None),
        P(),
        P("fs", "tp"),
        P("fs", None),
        P("fs", None),
        P(),
        P(None, "tp"),
        P(None, "tp"),
        P(),
        P(),
        P("fs", "tp"),
        P("fs", "tp"),
        P("fs", "tp"),
        P(),
        P(None, "tp"),
        P("tp"),
        P("fs", "tp", "sp"),
        P("fs", "tp", "sp"),
        P(),
        P(None, "tp"),
        P("tp"),
        P("tp", None),
        P("tp"),
        P("tp", "fs"),
        P("tp", "fs"),
    )

    return jax.shard_map(
        shards,
        mesh=mesh,
        in_specs=placed,
        out_specs=(P("fs", ("sp", "tp"), None), P("fs", "tp", "sp")),
        check_vma=False,
    )
```

```python
import jax
import jax.numpy as jnp
import numpy as np
from jax import lax
from jax.experimental import pallas as pl
from jax.experimental.pallas import tpu as pltpu
from jax.sharding import PartitionSpec as P


F32 = jnp.float32
BF16 = jnp.bfloat16

ROWS = 256
NOPE = 64
ROPE = 32
QK = NOPE + ROPE
CHUNK = 64
CHUNKS = ROWS // CHUNK
EPS = 1e-6
GROUP_EPS = 0.00064
NN = (((1,), (0,)), ((), ()))
NT = (((1,), (1,)), ((), ()))
TN = (((0,), (0,)), ((), ()))

VMEM = pl.BlockSpec(memory_space=pltpu.VMEM)
SMEM = pl.BlockSpec(memory_space=pltpu.SMEM)
ANY = pl.BlockSpec(memory_space=pl.ANY)
HBM = pl.BlockSpec(memory_space=pltpu.HBM)


def dot(a, b, dims=NN):
    return lax.dot_general(a, b, dims, preferred_element_type=F32)


def halves(a):
    high = a.astype(BF16)
    return high, (a - high.astype(F32)).astype(BF16)


def fine(a, b, dims=NN):
    (i,), (j,) = dims[0]
    ah, al = halves(a)
    bh, bl = halves(b)
    wide = dot(jnp.concatenate([ah, al], axis=i), jnp.concatenate([bh, bh], axis=j), dims)
    return wide + dot(ah, bl, dims)


def dot_wide(a, b):
    high, low = halves(a)
    return dot(jnp.concatenate([high, low], axis=1), jnp.concatenate([b, b], axis=0))


def iota(shape, dim):
    return lax.broadcasted_iota(jnp.int32, shape, dim)


def call(body, outs, args, flops, scratch=(), specs=None, limit=24):
    return pl.pallas_call(
        body,
        out_shape=outs,
        in_specs=specs or [VMEM] * len(args),
        out_specs=jax.tree.map(lambda _: VMEM, outs),
        scratch_shapes=scratch,
        compiler_params=pltpu.CompilerParams(vmem_limit_bytes=int(limit * (1 << 20))),
        cost_estimate=pl.CostEstimate(flops=flops, bytes_accessed=4 << 20, transcendentals=0),
    )(*args)


def turned(n, table):
    half = ROPE // 2
    a, b = n[NOPE : NOPE + half], n[NOPE + half :]
    cosine, sine = table[:half], table[half:]
    return a * cosine - b * sine, b * cosine + a * sine


def prepare_body(
    place, x_in, gain_in, wa_in, wk_in, wv_in, wq_in, wc_in, wr_in, oa_in, or_in,
    xs, small, big, late, x, gain, wa, wk, wv, wq, wc, wr, oa, orr, turned_wc, arrived,
):
    pairs = [
        (x_in, x), (gain_in, gain), (wc_in, wc), (wr_in, wr), (wa_in, wa), (wk_in, wk),
        (wv_in, wv), (wq_in, wq), (oa_in, oa), (or_in, orr),
    ]
    copies = [pltpu.make_async_copy(a, b, arrived.at[i]) for i, (a, b) in enumerate(pairs)]
    for copy in copies:
        copy.start()
    copies[0].wait()
    copies[1].wait()
    v = x[...].astype(F32)
    v = v * lax.rsqrt(jnp.mean(v * v, axis=-1, keepdims=True) + EPS) * gain[...]
    v = v.astype(BF16)
    for i in range(8):
        xs[i] = v
    copies[2].wait()
    copies[3].wait()
    turned_wc[...] = wc[...].astype(F32).T
    start = pl.multiple_of(place[1] * 32, 32)
    small[0:32] = turned_wc[pl.ds(start, 32), :].astype(BF16)
    small[32:64] = wr[...]
    for copy in copies[4:]:
        copy.wait()
    big[:, 0:128] = wa[...]
    big[:, 128:256] = wk[...]
    big[:, 256:384] = wv[...]
    late[0:192] = wq[...]
    late[192:320] = oa[...]
    late[320:448] = orr[...]


def prepare(*args):
    outs = [
        jax.ShapeDtypeStruct((8, 32, 2048), BF16),
        jax.ShapeDtypeStruct((64, 512), BF16),
        jax.ShapeDtypeStruct((512, 384), BF16),
        jax.ShapeDtypeStruct((448, 512), BF16),
    ]
    scratch = [pltpu.VMEM(a.shape, a.dtype) for a in args[1:]]
    scratch += [pltpu.VMEM((256, 512), F32), pltpu.SemaphoreType.DMA((10,))]
    return call(prepare_body, outs, args, 1 << 29, scratch, [SMEM] + [HBM] * 10, 63.9)


def collect_body(place, own, left, right, far, out):
    chip = place[1] // 2
    for by, part in ((0, own), (3, left), (1, right), (2, far)):
        out[lax.rem(chip + by, 4)] = part[...]


def collect(place, *parts):
    outs = jax.ShapeDtypeStruct((4, *parts[0].shape), BF16)
    return call(collect_body, outs, (place, *parts), 1 << 29, specs=[SMEM] + [VMEM] * 4)


def lowrank_body(place, x, fd, fa, table, dlow, rlow, turn):
    dlow[...] = jnp.tanh(dot(x[...], fd[...]).astype(BF16).astype(F32)).astype(BF16)
    rlow[...] = dot(x[...], fa[...]).astype(BF16)
    turn[...] = table[place[0]]


def lowrank(*args):
    outs = [
        jax.ShapeDtypeStruct((ROWS, 128), BF16),
        jax.ShapeDtypeStruct((ROWS, 128), BF16),
        jax.ShapeDtypeStruct((ROPE, ROWS), F32),
    ]
    return call(lowrank_body, outs, args, 1 << 29, specs=[SMEM] + [VMEM] * 4)


def columns(place, k):
    shard = lax.rem(place[2] + (0, 3, 1, 2)[k], 4)
    return pl.ds(pl.multiple_of(shard * 512, 512), 512)


def latents_body(place, x, w0, w1, w2, w3, pay):
    t = jnp.zeros((64, ROWS), F32)
    for k, w in enumerate((w0, w1, w2, w3)):
        t += dot(w[...], x[:, columns(place, k)], NT)
    tp = place[1]
    group = jnp.zeros((8, ROWS), F32)
    for g in range(4):
        group += jnp.where(tp // 2 == g, t[32 + 8 * g : 40 + 8 * g], 0.0)
    group = jnp.where(iota((8, ROWS), 0) // 4 == lax.rem(tp, 2), group, 0.0)
    both = jnp.concatenate([t[0:32], group], axis=0).astype(BF16)
    for i in range(16):
        pay[i] = both


def latents(*args):
    outs = jax.ShapeDtypeStruct((16, 40, ROWS), BF16)
    return call(latents_body, outs, args, 1 << 29, specs=[SMEM] + [VMEM] * 5)


def project_body(
    place, x, w0, w1, w2, w3, up, glat, kgain, mult, extra, present, gain, rkv
):
    y = jnp.zeros((ROWS, 384), F32)
    for k, w in enumerate((w0, w1, w2, w3)):
        y += dot(x[:, columns(place, k)], w[...])
    rkv[...] = y.astype(BF16)


def project(*args):
    outs = jax.ShapeDtypeStruct((ROWS, 384), BF16)
    return call(project_body, outs, args, 4 << 30, specs=[SMEM] + [VMEM] * 5 + [ANY] * 7)


def queries_body(place, x, w0, w1, w2, w3, turn, gain, q):
    t = jnp.zeros((192, ROWS), F32)
    for k, w in enumerate((w0, w1, w2, w3)):
        t += dot(w[0:192], x[:, columns(place, k)], NT)
    t = t.astype(BF16).astype(F32)
    factor = np.float32(QK**-0.5 * np.log2(np.e))
    for h in range(2):
        v = t[QK * h : QK * (h + 1)]
        n = v * (lax.rsqrt(jnp.mean(v * v, axis=0, keepdims=True) + EPS) * factor) * gain[...]
        a, b = turned(n, turn[...])
        ready = jnp.concatenate([n[:NOPE], a, b, jnp.zeros((128 - QK, ROWS), F32)], axis=0)
        q[h] = ready.T.astype(BF16)


def queries(*args):
    outs = jax.ShapeDtypeStruct((2, ROWS, 128), BF16)
    return call(queries_body, outs, args, 1 << 29, specs=[SMEM] + [VMEM] * 7)


def recur_body(rkv, dlow, rlow, wd, bd, wa, ba, mult, extra, present, free, along, bonus, state):
    lane = iota((ROWS, 128), 1)
    recept, key, value = (rkv[:, 128 * i : 128 * (i + 1)].astype(F32) for i in range(3))
    speed = jax.nn.sigmoid(bd[...] + dot(dlow[...], wd[...])) * np.float32(np.exp(-0.5))
    added = jnp.where(lane < 64, extra[:, 0:1], extra[:, 1:2])
    ld = added - speed * mult[...]
    learn = jax.nn.sigmoid(ba[...] + dot(rlow[...], wa[...]))
    same = (iota((128, 128), 0) // 64 == iota((128, 128), 1) // 64).astype(BF16)
    unit = key * lax.rsqrt(dot_wide(key * key, same) + EPS)
    bonus[...] = dot_wide(recept * key * present[...], same) * value
    r, c = iota((ROWS, ROWS), 0), iota((ROWS, ROWS), 1)
    block = r // CHUNK == c // CHUNK
    sums = jnp.concatenate(
        [
            jnp.where(block & (c <= r), 1.0, 0.0),
            jnp.where(block & (lax.rem(c, CHUNK) < CHUNK // 2), 1.0, 0.0),
            jnp.where(block, 1.0, 0.0),
        ],
        axis=0,
    )
    sums = sums.astype(BF16)
    high, low = halves(ld)
    last = (ld - high.astype(F32) - low.astype(F32)).astype(BF16)
    sums = dot(
        jnp.concatenate([sums, sums, sums], axis=1), jnp.concatenate([high, low, last], axis=0)
    )
    cum, mid, end = sums[:ROWS], sums[ROWS : 2 * ROWS], sums[2 * ROWS :]
    prev = cum - ld
    toward = -unit
    remove = unit * learn
    grow, shrink = jnp.exp(cum - mid), jnp.exp(mid - cum)
    left1, left2 = toward * jnp.exp(prev - mid), recept * grow
    right1, right2 = remove * shrink, key * shrink
    start1, start2 = toward * jnp.exp(prev), recept * jnp.exp(cum)
    tail = jnp.exp(end - cum)
    tail1, tail2 = remove * tail, key * tail
    whole = jnp.exp(end)
    m0 = iota((CHUNK, 128), 1) < 64

    def stacked(v, k):
        v = v[CHUNK * k : CHUNK * (k + 1)]
        return jnp.concatenate([jnp.where(m0, v, 0.0), jnp.where(m0, 0.0, v)], axis=0)

    rr, cc = iota((128, 128), 0), iota((128, 128), 1)
    head = rr // 64 == cc // 64
    eye = jnp.where(rr == cc, 1.0, 0.0)
    in16, in32 = rr // 16 == cc // 16, rr // 32 == cc // 32
    strict, upto = head & (rr > cc), head & (rr >= cc)

    def square(top, mask):
        both = jnp.concatenate([top, top], axis=1)
        return jnp.where(mask, both, 0.0)

    stage = []
    for k in range(CHUNKS):
        rows = jnp.concatenate([stacked(left1, k), stacked(left2, k)], axis=0)
        part = slice(CHUNK * k, CHUNK * (k + 1))
        cols = jnp.concatenate([right1[part], right2[part]], axis=0)
        g = fine(rows, cols, NT)
        a = square(g[:128, :64], strict)
        kb = square(g[:128, 64:], strict)
        ru = square(g[128:, :64], upto)
        ku = square(g[128:, 64:], upto)
        stage.append([a, kb, ru, ku])
    inverse = []
    for k in range(CHUNKS):
        a = stage[k][0]
        small = jnp.where(in16, a, 0.0)
        power = small
        t = eye + small
        for _ in range(3):
            power = fine(power, power)
            t = t + fine(t, power)
        t = t + fine(fine(t, jnp.where(in32 & ~in16, a, 0.0)), t)
        t = t + fine(fine(t, jnp.where(in32, 0.0, a)), t)
        inverse.append(t)
    pair = jnp.concatenate([jnp.zeros((128, 128), F32), eye], axis=0)
    for k in range(CHUNKS):
        _, kb, ru, ku = stage[k]
        v = stacked(value, k)
        xy = fine(inverse[k], jnp.concatenate([stacked(start1, k), fine(kb, v)], axis=1))
        read = fine(ru, xy)
        coef = stacked(start2, k) + read[:, :128]
        rest = read[:, 128:] + fine(ku, v)
        t1, t2 = stacked(tail1, k), stacked(tail2, k)
        moved = fine(xy, t1, TN)
        decay = whole[CHUNK * k : CHUNK * k + 1]
        step = moved[:128] + jnp.where(rr == cc, decay, 0.0)
        add = moved[128:] + fine(v, t2, TN)
        out = fine(coef, pair, NT)
        near = out[:, :128] + rest
        far = out[:, 128:]
        part = slice(CHUNK * k, CHUNK * (k + 1))
        free[part] = near[:64] + near[64:]
        along[part] = far[:64] + far[64:]
        pair = fine(pair, step) + jnp.concatenate([add, jnp.zeros((128, 128), F32)], axis=0)
    far = (pair[128:192] + pair[192:]).astype(BF16)
    near = (pair[:64] + pair[64:128]).astype(BF16)
    for i in range(16):
        state[i, 0] = far
        state[i, 1] = near


def recur(*args):
    wide = jax.ShapeDtypeStruct((ROWS, 128), F32)
    outs = [wide, wide, wide, jax.ShapeDtypeStruct((16, 2, 64, 128), BF16)]
    return call(recur_body, outs, args, 8 << 30, limit=60)


def attend_body(place, q, own, peer, w, glat, gain, table, att, logs, acc, top):
    sp = place[0]
    ones = jnp.where(iota((NOPE, ROWS), 0) == 0, 1.0, 0.0).astype(BF16)

    def keys(j):
        lat = jnp.concatenate(
            [own[:, j, 0:32, :].reshape(128, ROWS), peer[:, j, 0:32, :].reshape(128, ROWS)], axis=0
        ).astype(F32)
        rope = (own[:, j, 32:40, :].astype(F32) + peer[:, j, 32:40, :].astype(F32)).reshape(
            ROPE, ROWS
        )
        lat = lat * lax.rsqrt(jnp.mean(lat * lat, axis=0, keepdims=True) + EPS) * glat[...]
        kv = dot(w[...], lat.astype(BF16)).astype(BF16)
        rope_sum = jnp.sum(rope * rope, axis=0, keepdims=True)
        turn = table[j]
        cosine, sine = turn[:16], turn[16:]
        ra, rb = rope[:16] * gain[64:80], rope[16:] * gain[80:96]
        ra, rb = ra * cosine - rb * sine, rb * cosine + ra * sine
        ready, values = [], []
        for h in range(2):
            k = kv[64 * h : 64 * (h + 1)].astype(F32)
            scale = lax.rsqrt(
                (jnp.sum(k * k, axis=0, keepdims=True) + rope_sum) * np.float32(1 / QK) + EPS
            )
            ready.append(
                jnp.concatenate([k * scale * gain[0:64], ra * scale, rb * scale], axis=0).astype(
                    BF16
                )
            )
            values.append(jnp.concatenate([kv[128 + 64 * h : 192 + 64 * h], ones], axis=0))
        return ready, values

    def block(places, first):
        made = [keys(j) for j in places]
        for h in range(2):
            ready = jnp.concatenate([m[0][h] for m in made], axis=1)
            v = jnp.concatenate([m[1][h] for m in made], axis=1)
            s = dot(q[h, :, 0:QK], ready)
            if first:
                s = jnp.where(iota((ROWS, ROWS), 1) <= iota((ROWS, ROWS), 0), s, -jnp.inf)
            peak = jnp.max(s, axis=1, keepdims=True)
            if first:
                top[h] = jnp.broadcast_to(peak, (ROWS, 128))
                acc[h] = dot(jnp.exp2(s - peak).astype(BF16), v, NT)
            else:
                old = top[h]
                new = jnp.maximum(old, peak)
                top[h] = new
                p = jnp.exp2(s - new[:, 0:1]).astype(BF16)
                acc[h] = acc[h] * jnp.exp2(old - new) + dot(p, v, NT)

    block([sp], True)

    def loop(i, carry):
        block([3 * i, 3 * i + 1, 3 * i + 2], False)
        return carry

    lax.fori_loop(0, sp // 3, loop, 0)

    @pl.when(lax.rem(sp, 3) == 1)
    def _():
        block([sp - 1], False)

    @pl.when(lax.rem(sp, 3) == 2)
    def _():
        block([sp - 2, sp - 1], False)

    parts = []
    rows = []
    for h in range(2):
        total = acc[h][:, 64:65]
        parts.append(acc[h][:, 0:64] / total)
        full = top[h] * np.float32(np.log(2.0)) + jnp.log(jnp.broadcast_to(total, (ROWS, 128)))
        rows.append(full.T[0:1])
    att[...] = jnp.concatenate(parts, axis=1).astype(BF16)
    logs[...] = jnp.concatenate(rows, axis=0)


def attend(*args):
    outs = [jax.ShapeDtypeStruct((ROWS, 128), BF16), jax.ShapeDtypeStruct((2, ROWS), F32)]
    scratch = [pltpu.VMEM((2, ROWS, 128), F32), pltpu.VMEM((2, ROWS, 128), F32)]
    return call(attend_body, outs, args, 8 << 30, scratch, [SMEM] + [VMEM] * 7)


def merge_body(place, att, free, along, bonus, states, branch, o0, o1, o2, o3, keep, send):
    head = iota((128, 128), 0) // 64 == iota((128, 128), 1) // 64

    def spread(v):
        return jnp.where(head, jnp.concatenate([v, v], axis=0), jnp.zeros((), v.dtype))

    def step(r, entering):
        return dot_wide(entering, spread(states[r, 0])) + spread(states[r, 1]).astype(F32)

    entering = lax.fori_loop(0, place[0], step, jnp.zeros((128, 128), F32))
    read = free[...] + fine(along[...], entering, NT)
    mean = jnp.where(head, 1.0 / 64, 0.0).astype(BF16)
    read = read - dot_wide(read, mean)
    spread_of = dot_wide(read * read, mean)
    rec = read * lax.rsqrt(spread_of + GROUP_EPS) * branch[...] + bonus[...]
    both = jnp.concatenate([att[...].astype(F32), rec], axis=1).reshape(4, 2, 32, 256)
    core = lax.rem(place[1], 2)
    even, odd = both[:, 0].reshape(128, 256), both[:, 1].reshape(128, 256)
    kept = jnp.where(core == 0, even, odd).astype(BF16)
    sent = jnp.where(core == 0, odd, even).astype(BF16)
    for k, o in enumerate((o0, o1, o2, o3)):
        send[:, columns(place, k)] = dot(sent, o[192:448]).astype(BF16)
    for k, o in enumerate((o0, o1, o2, o3)):
        keep[:, columns(place, k)] = dot(kept, o[192:448])


def merge(*args):
    outs = [jax.ShapeDtypeStruct((128, 2048), F32), jax.ShapeDtypeStruct((128, 2048), BF16)]
    return call(merge_body, outs, args, 4 << 30, specs=[SMEM] + [VMEM] * 10)


def exchanged(copies, axis, groups=None):
    return lax.all_to_all(copies, axis, 0, 0, axis_index_groups=groups, tiled=True)


def around(value):
    moves = [[(i, (i + by) % 4) for i in range(4)] for by in (1, 3, 2)]
    return [value] + [lax.ppermute(value, "fs", move) for move in moves]


def other_core(value):
    return lax.ppermute(value, "tp", [(i, i ^ 1) for i in range(8)])


def turn_table():
    half = ROPE // 2
    inverse = np.float32(10000.0) ** (-np.arange(half, dtype=np.float32) / np.float32(half))
    angle = np.arange(4096, dtype=np.float32)[:, None] * inverse.astype(np.float32)[None, :]
    both = np.concatenate([np.cos(angle), np.sin(angle)], axis=1).astype(np.float32)
    return both.reshape(16, ROWS, ROPE).transpose(0, 2, 1)


def shards(
    entering,
    entering_gain,
    wq,
    wc,
    wr,
    compact_gain,
    wk_up,
    wv_up,
    q_gain,
    k_gain,
    w_accept,
    w_key,
    w_value,
    fade1,
    fade2,
    fade_bias,
    fade_mult,
    fade_extra,
    adapt1,
    adapt2,
    adapt_bias,
    present,
    branch,
    wo_att,
    wo_rec,
):
    tp = lax.axis_index("tp")
    sp = lax.axis_index("sp")
    core = lax.rem(tp, 2)
    place = jnp.stack([sp, tp, lax.axis_index("fs")]).astype(jnp.int32)
    xs, small, big, late = prepare(
        place,
        entering[0],
        entering_gain.reshape(1, 2048),
        w_accept,
        w_key,
        w_value,
        wq.T,
        wc,
        wr.T,
        wo_att,
        wo_rec,
    )
    normed = exchanged(xs, "tp").reshape(ROWS, 2048)
    smalls = around(small)
    bigs = around(big)
    lates = around(late)

    table = jnp.asarray(turn_table())
    pay = latents(place, normed, *smalls)
    pay, (wk_up, wv_up, compact_gain, k_gain, q_gain, fade_mult, fade_extra, present) = (
        lax.optimization_barrier(
            (pay, (wk_up, wv_up, compact_gain, k_gain, q_gain, fade_mult, fade_extra, present))
        )
    )
    lat = exchanged(pay, "sp")

    def reordered(v):
        v = v.reshape(4, 2, 32, *v.shape[1:])
        v = jnp.where(core == 0, v, v[:, ::-1])
        return jnp.moveaxis(v, 1, 0).reshape(256, *v.shape[3:])

    up = reordered(jnp.concatenate([wk_up, wv_up], axis=1)).T
    glat = reordered(compact_gain).reshape(256, 1)
    key_gain = k_gain.reshape(QK, 1)
    query_gain = q_gain.reshape(QK, 1)
    mult = jnp.repeat(fade_mult[0, :, 0], 64).reshape(1, 128)
    extra = fade_extra[0].T
    present = present.reshape(1, 128)
    dlow, rlow, turn = lowrank(place, normed, fade1, adapt1, table)
    rkv = project(
        place, normed, *bigs, up, glat, key_gain, mult, extra, present, query_gain
    )
    free, along, bonus, state = recur(
        rkv,
        dlow,
        rlow,
        fade2,
        fade_bias.reshape(1, 128),
        adapt2,
        adapt_bias.reshape(1, 128),
        mult,
        extra,
        present,
    )
    lat, state = lax.optimization_barrier((lat, state))
    states = exchanged(state, "sp")
    others = [lax.ppermute(lat, "tp", [(i, (i + by) % 8) for i in range(8)]) for by in (2, 6, 4)]
    lat_own = collect(place, lat, *others)
    lat_peer = other_core(lat_own)
    q = queries(place, normed, *lates, turn, query_gain)
    att, logs = attend(place, q, lat_own, lat_peer, up, glat, key_gain, table)
    keep, send = merge(place, att, free, along, bonus, states, branch.reshape(1, 128), *lates)
    pair = (keep + other_core(send).astype(F32)).astype(BF16)
    same_core = [[0, 2, 4, 6], [1, 3, 5, 7]]
    parts = exchanged(pair.reshape(4, 32, 2048), "tp", same_core)
    mixed = jnp.sum(parts.astype(F32), axis=0).astype(BF16)
    return mixed[None], logs[None]


def solution(mesh):
    placed = (
        P("fs", ("sp", "tp"), None),
        P(),
        P("fs", "tp"),
        P("fs", None),
        P("fs", None),
        P(),
        P(None, "tp"),
        P(None, "tp"),
        P(),
        P(),
        P("fs", "tp"),
        P("fs", "tp"),
        P("fs", "tp"),
        P(),
        P(None, "tp"),
        P("tp"),
        P("fs", "tp", "sp"),
        P("fs", "tp", "sp"),
        P(),
        P(None, "tp"),
        P("tp"),
        P("tp", None),
        P("tp"),
        P("tp", "fs"),
        P("tp", "fs"),
    )

    return jax.shard_map(
        shards,
        mesh=mesh,
        in_specs=placed,
        out_specs=(P("fs", ("sp", "tp"), None), P("fs", "tp", "sp")),
        check_vma=False,
    )
```

```python
import jax
import jax.numpy as jnp
import numpy as np
from jax import lax
from jax.experimental import pallas as pl
from jax.experimental.pallas import tpu as pltpu
from jax.sharding import PartitionSpec as P


F32 = jnp.float32
BF16 = jnp.bfloat16

ROWS = 256
NOPE = 64
ROPE = 32
QK = NOPE + ROPE
CHUNK = 64
RECUR_LIMIT = 40
CHUNKS = ROWS // CHUNK
EPS = 1e-6
GROUP_EPS = 0.00064
NN = (((1,), (0,)), ((), ()))
NT = (((1,), (1,)), ((), ()))
TN = (((0,), (0,)), ((), ()))

VMEM = pl.BlockSpec(memory_space=pltpu.VMEM)
SMEM = pl.BlockSpec(memory_space=pltpu.SMEM)
ANY = pl.BlockSpec(memory_space=pl.ANY)
HBM = pl.BlockSpec(memory_space=pltpu.HBM)


def dot(a, b, dims=NN):
    return lax.dot_general(a, b, dims, preferred_element_type=F32)


def halves(a):
    high = a.astype(BF16)
    return high, (a - high.astype(F32)).astype(BF16)


def fine(a, b, dims=NN):
    (i,), (j,) = dims[0]
    ah, al = halves(a)
    bh, bl = halves(b)
    wide = dot(jnp.concatenate([ah, al], axis=i), jnp.concatenate([bh, bh], axis=j), dims)
    return wide + dot(ah, bl, dims)


def dot_wide(a, b):
    high, low = halves(a)
    return dot(jnp.concatenate([high, low], axis=1), jnp.concatenate([b, b], axis=0))


def iota(shape, dim):
    return lax.broadcasted_iota(jnp.int32, shape, dim)


def call(body, outs, args, flops, scratch=(), specs=None, limit=24):
    return pl.pallas_call(
        body,
        out_shape=outs,
        in_specs=specs or [VMEM] * len(args),
        out_specs=jax.tree.map(lambda _: VMEM, outs),
        scratch_shapes=scratch,
        compiler_params=pltpu.CompilerParams(vmem_limit_bytes=int(limit * (1 << 20))),
        cost_estimate=pl.CostEstimate(flops=flops, bytes_accessed=4 << 20, transcendentals=0),
    )(*args)


def turned(n, table):
    half = ROPE // 2
    a, b = n[NOPE : NOPE + half], n[NOPE + half :]
    cosine, sine = table[:half], table[half:]
    return a * cosine - b * sine, b * cosine + a * sine


def prepare_body(
    place, x_in, gain_in, wa_in, wk_in, wv_in, wq_in, wc_in, wr_in, oa_in, or_in,
    xs, small, big, late, x, gain, wa, wk, wv, wq, wc, wr, oa, orr, turned_wc, arrived,
):
    pairs = [
        (x_in, x), (gain_in, gain), (wc_in, wc), (wr_in, wr), (wa_in, wa), (wk_in, wk),
        (wv_in, wv), (wq_in, wq), (oa_in, oa), (or_in, orr),
    ]
    copies = [pltpu.make_async_copy(a, b, arrived.at[i]) for i, (a, b) in enumerate(pairs)]
    for copy in copies:
        copy.start()
    copies[0].wait()
    copies[1].wait()
    v = x[...].astype(F32)
    v = v * lax.rsqrt(jnp.mean(v * v, axis=-1, keepdims=True) + EPS) * gain[...]
    v = v.astype(BF16)
    for i in range(8):
        xs[i] = v
    copies[2].wait()
    copies[3].wait()
    turned_wc[...] = wc[...].astype(F32).T
    start = pl.multiple_of(place[1] * 32, 32)
    small[0:32] = turned_wc[pl.ds(start, 32), :].astype(BF16)
    small[32:64] = wr[...]
    for copy in copies[4:]:
        copy.wait()
    big[:, 0:128] = wa[...]
    big[:, 128:256] = wk[...]
    big[:, 256:384] = wv[...]
    late[0:192] = wq[...]
    late[192:320] = oa[...]
    late[320:448] = orr[...]


def prepare(*args):
    outs = [
        jax.ShapeDtypeStruct((8, 32, 2048), BF16),
        jax.ShapeDtypeStruct((64, 512), BF16),
        jax.ShapeDtypeStruct((512, 384), BF16),
        jax.ShapeDtypeStruct((448, 512), BF16),
    ]
    scratch = [pltpu.VMEM(a.shape, a.dtype) for a in args[1:]]
    scratch += [pltpu.VMEM((256, 512), F32), pltpu.SemaphoreType.DMA((10,))]
    return call(prepare_body, outs, args, 1 << 29, scratch, [SMEM] + [HBM] * 10, 63.9)


def collect_body(place, own, left, right, far, out):
    chip = place[1] // 2
    for by, part in ((0, own), (3, left), (1, right), (2, far)):
        out[lax.rem(chip + by, 4)] = part[...]


def collect(place, *parts):
    outs = jax.ShapeDtypeStruct((4, *parts[0].shape), BF16)
    return call(collect_body, outs, (place, *parts), 1 << 29, specs=[SMEM] + [VMEM] * 4)


def lowrank_body(
    place, x, fd, fa, table, wk_up, wv_up, compact_gain, kg, qg,
    dlow, rlow, turn, up, glat, key_gain, query_gain,
):
    core = lax.rem(place[1], 2)
    dlow[...] = jnp.tanh(dot(x[...], fd[...]).astype(BF16).astype(F32)).astype(BF16)
    rlow[...] = dot(x[...], fa[...]).astype(BF16)
    turn[...] = table[place[0]]

    def reordered(v):
        v = v.reshape(4, 2, 32, v.shape[-1])
        even, odd = v[:, 0].reshape(128, -1), v[:, 1].reshape(128, -1)
        first, second = jnp.where(core == 0, even, odd), jnp.where(core == 0, odd, even)
        return jnp.concatenate([first, second], axis=0)

    both = jnp.concatenate([wk_up[...], wv_up[...]], axis=1).astype(F32)
    up[...] = reordered(both).T.astype(BF16)
    glat[...] = reordered(jnp.broadcast_to(compact_gain[...], (128, 256)).T)
    for source, out in ((kg, key_gain), (qg, query_gain)):
        wide = jnp.concatenate([source[...], jnp.zeros((1, 128 - QK), F32)], axis=1)
        out[...] = jnp.broadcast_to(wide, (128, 128)).T[0:QK]


def lowrank(*args):
    column = jax.ShapeDtypeStruct((QK, 128), F32)
    outs = [
        jax.ShapeDtypeStruct((ROWS, 128), BF16),
        jax.ShapeDtypeStruct((ROWS, 128), BF16),
        jax.ShapeDtypeStruct((ROPE, ROWS), F32),
        jax.ShapeDtypeStruct((256, 256), BF16),
        jax.ShapeDtypeStruct((256, 128), F32),
        column,
        column,
    ]
    return call(lowrank_body, outs, args, 1 << 29, specs=[SMEM] + [VMEM] * 9)


def columns(place, k):
    shard = lax.rem(place[2] + (0, 3, 1, 2)[k], 4)
    return pl.ds(pl.multiple_of(shard * 512, 512), 512)


def latents_body(place, x, w0, w1, w2, w3, pay):
    t = jnp.zeros((64, ROWS), F32)
    for k, w in enumerate((w0, w1, w2, w3)):
        t += dot(w[...], x[:, columns(place, k)], NT)
    tp = place[1]
    group = jnp.zeros((8, ROWS), F32)
    for g in range(4):
        group += jnp.where(tp // 2 == g, t[32 + 8 * g : 40 + 8 * g], 0.0)
    group = jnp.where(iota((8, ROWS), 0) // 4 == lax.rem(tp, 2), group, 0.0)
    both = jnp.concatenate([t[0:32], group], axis=0).astype(BF16)
    for i in range(16):
        pay[i] = both


def latents(*args):
    outs = jax.ShapeDtypeStruct((16, 40, ROWS), BF16)
    return call(latents_body, outs, args, 1 << 29, specs=[SMEM] + [VMEM] * 5, limit=63.9)


def queries_body(place, x, w0, w1, w2, w3, turn, gain, q):
    t = jnp.zeros((192, ROWS), F32)
    for k, w in enumerate((w0, w1, w2, w3)):
        t += dot(w[0:192], x[:, columns(place, k)], NT)
    t = t.astype(BF16).astype(F32)
    factor = np.float32(QK**-0.5 * np.log2(np.e))
    for h in range(2):
        v = t[QK * h : QK * (h + 1)]
        n = v * (lax.rsqrt(jnp.mean(v * v, axis=0, keepdims=True) + EPS) * factor) * gain[:, 0:1]
        a, b = turned(n, turn[...])
        ready = jnp.concatenate([n[:NOPE], a, b, jnp.zeros((128 - QK, ROWS), F32)], axis=0)
        q[h] = ready.T.astype(BF16)


def queries(*args):
    outs = jax.ShapeDtypeStruct((2, ROWS, 128), BF16)
    return call(queries_body, outs, args, 1 << 29, specs=[SMEM] + [VMEM] * 7)


def recur_body(
    place, x, w0, w1, w2, w3, dlow, rlow, wd, bd, wa, ba, mult, extra, present, up, glat, kgain,
    qgain, free, along, bonus, state,
):
    lane = iota((1, 128), 1)
    y = jnp.zeros((ROWS, 384), F32)
    for k, w in enumerate((w0, w1, w2, w3)):
        y += dot(x[:, columns(place, k)], w[...])
    y = y.astype(BF16).astype(F32)
    recept, key, value = (y[:, 128 * i : 128 * (i + 1)] for i in range(3))
    speed = jax.nn.sigmoid(bd[...] + dot(dlow[...], wd[...])) * np.float32(np.exp(-0.5))
    added = jnp.where(iota((128, ROWS), 0) < 64, extra[0:1], extra[1:2]).T
    ld = added - speed * jnp.where(lane < 64, mult[0:1, 0:1], mult[1:2, 0:1])
    here = jnp.concatenate([present[0:1], present[1:2]], axis=1)
    learn = jax.nn.sigmoid(ba[...] + dot(rlow[...], wa[...]))
    same = (iota((128, 128), 0) // 64 == iota((128, 128), 1) // 64).astype(BF16)
    unit = key * lax.rsqrt(dot_wide(key * key, same) + EPS)
    bonus[...] = dot_wide(recept * key * here, same) * value
    r, c = iota((ROWS, ROWS), 0), iota((ROWS, ROWS), 1)
    block = r // CHUNK == c // CHUNK
    sums = jnp.concatenate(
        [
            jnp.where(block & (c <= r), 1.0, 0.0),
            jnp.where(block & (lax.rem(c, CHUNK) < CHUNK // 2), 1.0, 0.0),
            jnp.where(block, 1.0, 0.0),
        ],
        axis=0,
    )
    sums = sums.astype(BF16)
    high, low = halves(ld)
    last = (ld - high.astype(F32) - low.astype(F32)).astype(BF16)
    sums = dot(
        jnp.concatenate([sums, sums, sums], axis=1), jnp.concatenate([high, low, last], axis=0)
    )
    cum, mid, end = sums[:ROWS], sums[ROWS : 2 * ROWS], sums[2 * ROWS :]
    prev = cum - ld
    toward = -unit
    remove = unit * learn
    grow, shrink = jnp.exp(cum - mid), jnp.exp(mid - cum)
    left1, left2 = toward * jnp.exp(prev - mid), recept * grow
    right1, right2 = remove * shrink, key * shrink
    start1, start2 = toward * jnp.exp(prev), recept * jnp.exp(cum)
    tail = jnp.exp(end - cum)
    tail1, tail2 = remove * tail, key * tail
    whole = jnp.exp(end)
    m0 = iota((CHUNK, 128), 1) < 64

    def stacked(v, k):
        v = v[CHUNK * k : CHUNK * (k + 1)]
        return jnp.concatenate([jnp.where(m0, v, 0.0), jnp.where(m0, 0.0, v)], axis=0)

    rr, cc = iota((128, 128), 0), iota((128, 128), 1)
    head = rr // 64 == cc // 64
    eye = jnp.where(rr == cc, 1.0, 0.0)
    in16, in32 = rr // 16 == cc // 16, rr // 32 == cc // 32
    strict, upto = head & (rr > cc), head & (rr >= cc)

    def square(top, mask):
        both = jnp.concatenate([top, top], axis=1)
        return jnp.where(mask, both, 0.0)

    stage = []
    for k in range(CHUNKS):
        rows = jnp.concatenate([stacked(left1, k), stacked(left2, k)], axis=0)
        part = slice(CHUNK * k, CHUNK * (k + 1))
        cols = jnp.concatenate([right1[part], right2[part]], axis=0)
        g = fine(rows, cols, NT)
        a = square(g[:128, :64], strict)
        kb = square(g[:128, 64:], strict)
        ru = square(g[128:, :64], upto)
        ku = square(g[128:, 64:], upto)
        stage.append([a, kb, ru, ku])
    inverse = []
    for k in range(CHUNKS):
        a = stage[k][0]
        small = jnp.where(in16, a, 0.0)
        power = small
        t = eye + small
        for _ in range(3):
            power = fine(power, power)
            t = t + fine(t, power)
        t = t + fine(fine(t, jnp.where(in32 & ~in16, a, 0.0)), t)
        t = t + fine(fine(t, jnp.where(in32, 0.0, a)), t)
        inverse.append(t)
    pair = jnp.concatenate([jnp.zeros((128, 128), F32), eye], axis=0)
    for k in range(CHUNKS):
        _, kb, ru, ku = stage[k]
        v = stacked(value, k)
        xy = fine(inverse[k], jnp.concatenate([stacked(start1, k), fine(kb, v)], axis=1))
        read = fine(ru, xy)
        coef = stacked(start2, k) + read[:, :128]
        rest = read[:, 128:] + fine(ku, v)
        t1, t2 = stacked(tail1, k), stacked(tail2, k)
        moved = fine(xy, t1, TN)
        decay = whole[CHUNK * k : CHUNK * k + 1]
        step = moved[:128] + jnp.where(rr == cc, decay, 0.0)
        add = moved[128:] + fine(v, t2, TN)
        out = fine(coef, pair, NT)
        near = out[:, :128] + rest
        far = out[:, 128:]
        part = slice(CHUNK * k, CHUNK * (k + 1))
        free[part] = near[:64] + near[64:]
        along[part] = far[:64] + far[64:]
        pair = fine(pair, step) + jnp.concatenate([add, jnp.zeros((128, 128), F32)], axis=0)
    far = (pair[128:192] + pair[192:]).astype(BF16)
    near = (pair[:64] + pair[64:128]).astype(BF16)
    for i in range(16):
        state[i, 0] = far
        state[i, 1] = near


def recur(*args):
    wide = jax.ShapeDtypeStruct((ROWS, 128), F32)
    outs = [wide, wide, wide, jax.ShapeDtypeStruct((16, 2, 64, 128), BF16)]
    specs = [SMEM] + [VMEM] * 14 + [ANY] * 4
    return call(recur_body, outs, args, 8 << 30, specs=specs, limit=RECUR_LIMIT)


def attend_body(place, q, own, peer, w, glat, gain, table, att, logs, acc, top):
    sp = place[0]
    ones = jnp.where(iota((NOPE, ROWS), 0) == 0, 1.0, 0.0).astype(BF16)

    def keys(j):
        lat = jnp.concatenate(
            [own[:, j, 0:32, :].reshape(128, ROWS), peer[:, j, 0:32, :].reshape(128, ROWS)], axis=0
        ).astype(F32)
        rope = (own[:, j, 32:40, :].astype(F32) + peer[:, j, 32:40, :].astype(F32)).reshape(
            ROPE, ROWS
        )
        lat = lat * lax.rsqrt(jnp.mean(lat * lat, axis=0, keepdims=True) + EPS) * glat[:, 0:1]
        kv = dot(w[...], lat.astype(BF16)).astype(BF16)
        rope_sum = jnp.sum(rope * rope, axis=0, keepdims=True)
        turn = table[j]
        cosine, sine = turn[:16], turn[16:]
        ra, rb = rope[:16] * gain[64:80, 0:1], rope[16:] * gain[80:96, 0:1]
        ra, rb = ra * cosine - rb * sine, rb * cosine + ra * sine
        ready, values = [], []
        for h in range(2):
            k = kv[64 * h : 64 * (h + 1)].astype(F32)
            scale = lax.rsqrt(
                (jnp.sum(k * k, axis=0, keepdims=True) + rope_sum) * np.float32(1 / QK) + EPS
            )
            ready.append(
                jnp.concatenate([k * scale * gain[0:64, 0:1], ra * scale, rb * scale], axis=0).astype(
                    BF16
                )
            )
            values.append(jnp.concatenate([kv[128 + 64 * h : 192 + 64 * h], ones], axis=0))
        return ready, values

    def block(places, first):
        made = [keys(j) for j in places]
        for h in range(2):
            ready = jnp.concatenate([m[0][h] for m in made], axis=1)
            v = jnp.concatenate([m[1][h] for m in made], axis=1)
            s = dot(q[h, :, 0:QK], ready)
            if first:
                s = jnp.where(iota((ROWS, ROWS), 1) <= iota((ROWS, ROWS), 0), s, -jnp.inf)
            peak = jnp.max(s, axis=1, keepdims=True)
            if first:
                top[h] = jnp.broadcast_to(peak, (ROWS, 128))
                acc[h] = dot(jnp.exp2(s - peak).astype(BF16), v, NT)
            else:
                old = top[h]
                new = jnp.maximum(old, peak)
                top[h] = new
                p = jnp.exp2(s - new[:, 0:1]).astype(BF16)
                acc[h] = acc[h] * jnp.exp2(old - new) + dot(p, v, NT)

    block([sp], True)

    def loop(i, carry):
        block([3 * i, 3 * i + 1, 3 * i + 2], False)
        return carry

    lax.fori_loop(0, sp // 3, loop, 0)

    @pl.when(lax.rem(sp, 3) == 1)
    def _():
        block([sp - 1], False)

    @pl.when(lax.rem(sp, 3) == 2)
    def _():
        block([sp - 2, sp - 1], False)

    parts = []
    rows = []
    for h in range(2):
        total = acc[h][:, 64:65]
        parts.append(acc[h][:, 0:64] / total)
        full = top[h] * np.float32(np.log(2.0)) + jnp.log(jnp.broadcast_to(total, (ROWS, 128)))
        rows.append(full.T[0:1])
    att[...] = jnp.concatenate(parts, axis=1).astype(BF16)
    logs[...] = jnp.concatenate(rows, axis=0)


def attend(*args):
    outs = [jax.ShapeDtypeStruct((ROWS, 128), BF16), jax.ShapeDtypeStruct((2, ROWS), F32)]
    scratch = [pltpu.VMEM((2, ROWS, 128), F32), pltpu.VMEM((2, ROWS, 128), F32)]
    return call(attend_body, outs, args, 8 << 30, scratch, [SMEM] + [VMEM] * 7)


def merge_body(place, att, free, along, bonus, states, branch, o0, o1, o2, o3, keep, send):
    head = iota((128, 128), 0) // 64 == iota((128, 128), 1) // 64

    def spread(v):
        return jnp.where(head, jnp.concatenate([v, v], axis=0), jnp.zeros((), v.dtype))

    sp = place[0]
    eye = jnp.where(iota((128, 128), 0) == iota((128, 128), 1), 1.0, 0.0).astype(BF16)
    below = jnp.zeros((128, 128), F32)
    entering = below
    groups = []
    for g in range(4):
        pair = None
        for r in range(4 * g, 4 * g + 4):
            move = jnp.where(r < sp, spread(states[r, 0]), eye)
            add = jnp.where(r < sp, spread(states[r, 1]).astype(F32), 0.0)
            if pair is None:
                pair = jnp.concatenate([add, move.astype(F32)], axis=0)
            else:
                pair = dot_wide(pair, move) + jnp.concatenate([add, below], axis=0)
        groups.append(pair)
    entering = groups[0][:128]
    for pair in groups[1:]:
        entering = fine(entering, pair[128:]) + pair[:128]
    read = free[...] + fine(along[...], entering, NT)
    mean = jnp.where(head, 1.0 / 64, 0.0).astype(BF16)
    read = read - dot_wide(read, mean)
    spread_of = dot_wide(read * read, mean)
    rec = read * lax.rsqrt(spread_of + GROUP_EPS) * branch[...] + bonus[...]
    both = jnp.concatenate([att[...].astype(F32), rec], axis=1).reshape(4, 2, 32, 256)
    core = lax.rem(place[1], 2)
    even, odd = both[:, 0].reshape(128, 256), both[:, 1].reshape(128, 256)
    kept = jnp.where(core == 0, even, odd).astype(BF16)
    sent = jnp.where(core == 0, odd, even).astype(BF16)
    for k, o in enumerate((o0, o1, o2, o3)):
        send[:, columns(place, k)] = dot(sent, o[192:448]).astype(BF16)
    for k, o in enumerate((o0, o1, o2, o3)):
        keep[:, columns(place, k)] = dot(kept, o[192:448])


def merge(*args):
    outs = [jax.ShapeDtypeStruct((128, 2048), F32), jax.ShapeDtypeStruct((128, 2048), BF16)]
    return call(merge_body, outs, args, 4 << 30, specs=[SMEM] + [VMEM] * 10)


def exchanged(copies, axis, groups=None):
    return lax.all_to_all(copies, axis, 0, 0, axis_index_groups=groups, tiled=True)


def around(value):
    moves = [[(i, (i + by) % 4) for i in range(4)] for by in (1, 3, 2)]
    return [value] + [lax.ppermute(value, "fs", move) for move in moves]


def other_core(value):
    return lax.ppermute(value, "tp", [(i, i ^ 1) for i in range(8)])


def turn_table():
    half = ROPE // 2
    inverse = np.float32(10000.0) ** (-np.arange(half, dtype=np.float32) / np.float32(half))
    angle = np.arange(4096, dtype=np.float32)[:, None] * inverse.astype(np.float32)[None, :]
    both = np.concatenate([np.cos(angle), np.sin(angle)], axis=1).astype(np.float32)
    return both.reshape(16, ROWS, ROPE).transpose(0, 2, 1)


def shards(
    entering,
    entering_gain,
    wq,
    wc,
    wr,
    compact_gain,
    wk_up,
    wv_up,
    q_gain,
    k_gain,
    w_accept,
    w_key,
    w_value,
    fade1,
    fade2,
    fade_bias,
    fade_mult,
    fade_extra,
    adapt1,
    adapt2,
    adapt_bias,
    present,
    branch,
    wo_att,
    wo_rec,
):
    tp = lax.axis_index("tp")
    sp = lax.axis_index("sp")
    place = jnp.stack([sp, tp, lax.axis_index("fs")]).astype(jnp.int32)
    xs, small, big, late = prepare(
        place,
        entering[0],
        entering_gain.reshape(1, 2048),
        w_accept,
        w_key,
        w_value,
        wq.T,
        wc,
        wr.T,
        wo_att,
        wo_rec,
    )
    normed = exchanged(xs, "tp").reshape(ROWS, 2048)
    smalls = around(small)
    bigs = around(big)
    lates = around(late)

    table = jnp.asarray(turn_table())
    pay = latents(place, normed, *smalls)
    lat = exchanged(pay, "sp")

    dlow, rlow, turn, up, glat, key_gain, query_gain = lowrank(
        place,
        normed,
        fade1,
        adapt1,
        table,
        wk_up,
        wv_up,
        compact_gain.reshape(1, 256),
        k_gain.reshape(1, QK),
        q_gain.reshape(1, QK),
    )
    free, along, bonus, state = recur(
        place,
        normed,
        *bigs,
        dlow,
        rlow,
        fade2,
        fade_bias.reshape(1, 128),
        adapt2,
        adapt_bias.reshape(1, 128),
        fade_mult[0],
        fade_extra[0],
        present,
        up,
        glat,
        key_gain,
        query_gain,
    )
    lat, state = lax.optimization_barrier((lat, state))
    states = exchanged(state, "sp")
    others = [lax.ppermute(lat, "tp", [(i, (i + by) % 8) for i in range(8)]) for by in (2, 6, 4)]
    lat_own = collect(place, lat, *others)
    lat_peer = other_core(lat_own)
    q = queries(place, normed, *lates, turn, query_gain)
    att, logs = attend(place, q, lat_own, lat_peer, up, glat, key_gain, table)
    keep, send = merge(place, att, free, along, bonus, states, branch.reshape(1, 128), *lates)
    pair = (keep + other_core(send).astype(F32)).astype(BF16)
    same_core = [[0, 2, 4, 6], [1, 3, 5, 7]]
    parts = exchanged(pair.reshape(4, 32, 2048), "tp", same_core)
    mixed = jnp.sum(parts.astype(F32), axis=0).astype(BF16)
    return mixed[None], logs[None]


def solution(mesh):
    placed = (
        P("fs", ("sp", "tp"), None),
        P(),
        P("fs", "tp"),
        P("fs", None),
        P("fs", None),
        P(),
        P(None, "tp"),
        P(None, "tp"),
        P(),
        P(),
        P("fs", "tp"),
        P("fs", "tp"),
        P("fs", "tp"),
        P(),
        P(None, "tp"),
        P("tp"),
        P("fs", "tp", "sp"),
        P("fs", "tp", "sp"),
        P(),
        P(None, "tp"),
        P("tp"),
        P("tp", None),
        P("tp"),
        P("tp", "fs"),
        P("tp", "fs"),
    )

    return jax.shard_map(
        shards,
        mesh=mesh,
        in_specs=placed,
        out_specs=(P("fs", ("sp", "tp"), None), P("fs", "tp", "sp")),
        check_vma=False,
    )
```

```python
import jax
import jax.numpy as jnp
import numpy as np
from jax import lax
from jax.experimental import pallas as pl
from jax.experimental.pallas import tpu as pltpu
from jax.sharding import PartitionSpec as P


F32 = jnp.float32
BF16 = jnp.bfloat16

ROWS = 256
NOPE = 64
ROPE = 32
QK = NOPE + ROPE
CHUNK = 64
RECUR_LIMIT = 63.9
CHUNKS = ROWS // CHUNK
EPS = 1e-6
GROUP_EPS = 0.00064
NN = (((1,), (0,)), ((), ()))
NT = (((1,), (1,)), ((), ()))
TN = (((0,), (0,)), ((), ()))

VMEM = pl.BlockSpec(memory_space=pltpu.VMEM)
HBM = pl.BlockSpec(memory_space=pltpu.HBM)


def dot(a, b, dims=NN):
    return lax.dot_general(a, b, dims, preferred_element_type=F32)


def halves(a):
    high = a.astype(BF16)
    return high, (a - high.astype(F32)).astype(BF16)


def fine(a, b, dims=NN):
    (i,), (j,) = dims[0]
    ah, al = halves(a)
    bh, bl = halves(b)
    wide = dot(jnp.concatenate([ah, al], axis=i), jnp.concatenate([bh, bh], axis=j), dims)
    return wide + dot(ah, bl, dims)


def dot_wide(a, b):
    high, low = halves(a)
    return dot(jnp.concatenate([high, low], axis=1), jnp.concatenate([b, b], axis=0))


def iota(shape, dim):
    return lax.broadcasted_iota(jnp.int32, shape, dim)


def call(body, outs, args, flops, scratch=(), specs=None, limit=24):
    return pl.pallas_call(
        body,
        out_shape=outs,
        in_specs=specs or [VMEM] * len(args),
        out_specs=jax.tree.map(lambda _: VMEM, outs),
        scratch_shapes=scratch,
        compiler_params=pltpu.CompilerParams(vmem_limit_bytes=int(limit * (1 << 20))),
        cost_estimate=pl.CostEstimate(flops=flops, bytes_accessed=4 << 20, transcendentals=0),
    )(*args)


def turned(n, table):
    half = ROPE // 2
    a, b = n[NOPE : NOPE + half], n[NOPE + half :]
    cosine, sine = table[:half], table[half:]
    return a * cosine - b * sine, b * cosine + a * sine


def prepare_body(
    x_in, gain_in, wa_in, wk_in, wv_in, wq_in, wc_in, wr_in, oa_in, or_in,
    xs, small, big, late, x, gain, wa, wk, wv, wq, wc, wr, oa, orr, turned_wc, arrived,
):
    pairs = [
        (x_in, x), (gain_in, gain), (wc_in, wc), (wr_in, wr), (wa_in, wa), (wk_in, wk),
        (wv_in, wv), (wq_in, wq), (oa_in, oa), (or_in, orr),
    ]
    copies = [pltpu.make_async_copy(a, b, arrived.at[i]) for i, (a, b) in enumerate(pairs)]
    for copy in copies:
        copy.start()
    copies[0].wait()
    copies[1].wait()
    v = x[...].astype(F32)
    v = v * lax.rsqrt(jnp.mean(v * v, axis=-1, keepdims=True) + EPS) * gain[...]
    v = v.astype(BF16)
    for i in range(8):
        xs[i] = v
    copies[2].wait()
    copies[3].wait()
    turned_wc[...] = wc[...].astype(F32).T
    start = pl.multiple_of(lax.axis_index("tp") * 32, 32)
    small[0:32] = turned_wc[pl.ds(start, 32), :].astype(BF16)
    small[32:64] = wr[...]
    for copy in copies[4:]:
        copy.wait()
    big[:, 0:128] = wa[...]
    big[:, 128:256] = wk[...]
    big[:, 256:384] = wv[...]
    late[0:192] = wq[...]
    late[192:320] = oa[...]
    late[320:448] = orr[...]


def prepare(*args):
    outs = [
        jax.ShapeDtypeStruct((8, 32, 2048), BF16),
        jax.ShapeDtypeStruct((64, 512), BF16),
        jax.ShapeDtypeStruct((512, 384), BF16),
        jax.ShapeDtypeStruct((448, 512), BF16),
    ]
    scratch = [pltpu.VMEM(a.shape, a.dtype) for a in args]
    scratch += [pltpu.VMEM((256, 512), F32), pltpu.SemaphoreType.DMA((10,))]
    return call(prepare_body, outs, args, 1 << 29, scratch, [HBM] * 10, 63.9)


def collect_body(own, left, right, far, out):
    chip = lax.axis_index("tp") // 2
    for by, part in ((0, own), (3, left), (1, right), (2, far)):
        out[lax.rem(chip + by, 4)] = part[...]


def collect(*parts):
    outs = jax.ShapeDtypeStruct((4, *parts[0].shape), BF16)
    return call(collect_body, outs, parts, 1 << 29)


def lowrank_body(
    x, fd, fa, table, wk_up, wv_up, compact_gain, kg, qg,
    dlow, rlow, turn, up, glat, key_gain, query_gain,
):
    core = lax.rem(lax.axis_index("tp"), 2)
    dlow[...] = jnp.tanh(dot(x[...], fd[...]).astype(BF16).astype(F32)).astype(BF16)
    rlow[...] = dot(x[...], fa[...]).astype(BF16)
    turn[...] = table[lax.axis_index("sp")]

    def reordered(v):
        v = v.reshape(4, 2, 32, v.shape[-1])
        even, odd = v[:, 0].reshape(128, -1), v[:, 1].reshape(128, -1)
        first, second = jnp.where(core == 0, even, odd), jnp.where(core == 0, odd, even)
        return jnp.concatenate([first, second], axis=0)

    both = jnp.concatenate([wk_up[...], wv_up[...]], axis=1).astype(F32)
    up[...] = reordered(both).T.astype(BF16)
    glat[...] = reordered(jnp.broadcast_to(compact_gain[...], (128, 256)).T)
    for source, out in ((kg, key_gain), (qg, query_gain)):
        wide = jnp.concatenate([source[...], jnp.zeros((1, 128 - QK), F32)], axis=1)
        out[...] = jnp.broadcast_to(wide, (128, 128)).T[0:QK]


def lowrank(*args):
    column = jax.ShapeDtypeStruct((QK, 128), F32)
    outs = [
        jax.ShapeDtypeStruct((ROWS, 128), BF16),
        jax.ShapeDtypeStruct((ROWS, 128), BF16),
        jax.ShapeDtypeStruct((ROPE, ROWS), F32),
        jax.ShapeDtypeStruct((256, 256), BF16),
        jax.ShapeDtypeStruct((256, 128), F32),
        column,
        column,
    ]
    return call(lowrank_body, outs, args, 1 << 29, specs=[VMEM] * 9, limit=63.9)


def columns(k):
    shard = lax.rem(lax.axis_index("fs") + (0, 3, 1, 2)[k], 4)
    return pl.ds(pl.multiple_of(shard * 512, 512), 512)


def latents_body(x, w0, w1, w2, w3, pay):
    t = jnp.zeros((64, ROWS), F32)
    for k, w in enumerate((w0, w1, w2, w3)):
        t += dot(w[...], x[:, columns(k)], NT)
    tp = lax.axis_index("tp")
    group = jnp.zeros((8, ROWS), F32)
    for g in range(4):
        group += jnp.where(tp // 2 == g, t[32 + 8 * g : 40 + 8 * g], 0.0)
    group = jnp.where(iota((8, ROWS), 0) // 4 == lax.rem(tp, 2), group, 0.0)
    both = jnp.concatenate([t[0:32], group], axis=0).astype(BF16)
    for i in range(16):
        pay[i] = both


def latents(*args):
    outs = jax.ShapeDtypeStruct((16, 40, ROWS), BF16)
    return call(latents_body, outs, args, 1 << 29, specs=[VMEM] * 5, limit=63.9)


def queries_body(x, w0, w1, w2, w3, turn, gain, q):
    t = jnp.zeros((192, ROWS), F32)
    for k, w in enumerate((w0, w1, w2, w3)):
        t += dot(w[0:192], x[:, columns(k)], NT)
    t = t.astype(BF16).astype(F32)
    factor = np.float32(QK**-0.5 * np.log2(np.e))
    for h in range(2):
        v = t[QK * h : QK * (h + 1)]
        n = v * (lax.rsqrt(jnp.mean(v * v, axis=0, keepdims=True) + EPS) * factor) * gain[:, 0:1]
        a, b = turned(n, turn[...])
        ready = jnp.concatenate([n[:NOPE], a, b, jnp.zeros((128 - QK, ROWS), F32)], axis=0)
        q[h] = ready.T.astype(BF16)


def queries(*args):
    outs = jax.ShapeDtypeStruct((2, ROWS, 128), BF16)
    return call(queries_body, outs, args, 1 << 29, specs=[VMEM] * 7)


def recur_body(
    x, w0, w1, w2, w3, dlow, rlow, wd, bd, wa, ba, mult, extra, present,
    free, along, bonus, state,
):
    lane = iota((1, 128), 1)
    y = jnp.zeros((ROWS, 384), F32)
    for k, w in enumerate((w0, w1, w2, w3)):
        y += dot(x[:, columns(k)], w[...])
    y = y.astype(BF16).astype(F32)
    recept, key, value = (y[:, 128 * i : 128 * (i + 1)] for i in range(3))
    speed = jax.nn.sigmoid(bd[...] + dot(dlow[...], wd[...])) * np.float32(np.exp(-0.5))
    added = jnp.where(iota((128, ROWS), 0) < 64, extra[0:1], extra[1:2]).T
    ld = added - speed * jnp.where(lane < 64, mult[0:1, 0:1], mult[1:2, 0:1])
    here = jnp.concatenate([present[0:1], present[1:2]], axis=1)
    learn = jax.nn.sigmoid(ba[...] + dot(rlow[...], wa[...]))
    same = (iota((128, 128), 0) // 64 == iota((128, 128), 1) // 64).astype(BF16)
    unit = key * lax.rsqrt(dot_wide(key * key, same) + EPS)
    bonus[...] = dot_wide(recept * key * here, same) * value
    r, c = iota((ROWS, ROWS), 0), iota((ROWS, ROWS), 1)
    block = r // CHUNK == c // CHUNK
    sums = jnp.concatenate(
        [
            jnp.where(block & (c <= r), 1.0, 0.0),
            jnp.where(block & (lax.rem(c, CHUNK) < CHUNK // 2), 1.0, 0.0),
            jnp.where(block, 1.0, 0.0),
        ],
        axis=0,
    )
    sums = sums.astype(BF16)
    high, low = halves(ld)
    last = (ld - high.astype(F32) - low.astype(F32)).astype(BF16)
    sums = dot(
        jnp.concatenate([sums, sums, sums], axis=1), jnp.concatenate([high, low, last], axis=0)
    )
    cum, mid, end = sums[:ROWS], sums[ROWS : 2 * ROWS], sums[2 * ROWS :]
    prev = cum - ld
    toward = -unit
    remove = unit * learn
    grow, shrink = jnp.exp(cum - mid), jnp.exp(mid - cum)
    left1, left2 = toward * jnp.exp(prev - mid), recept * grow
    right1, right2 = remove * shrink, key * shrink
    start1, start2 = toward * jnp.exp(prev), recept * jnp.exp(cum)
    tail = jnp.exp(end - cum)
    tail1, tail2 = remove * tail, key * tail
    whole = jnp.exp(end)
    m0 = iota((CHUNK, 128), 1) < 64

    def stacked(v, k):
        v = v[CHUNK * k : CHUNK * (k + 1)]
        return jnp.concatenate([jnp.where(m0, v, 0.0), jnp.where(m0, 0.0, v)], axis=0)

    rr, cc = iota((128, 128), 0), iota((128, 128), 1)
    head = rr // 64 == cc // 64
    eye = jnp.where(rr == cc, 1.0, 0.0)
    in16, in32 = rr // 16 == cc // 16, rr // 32 == cc // 32
    strict, upto = head & (rr > cc), head & (rr >= cc)

    def square(top, mask):
        both = jnp.concatenate([top, top], axis=1)
        return jnp.where(mask, both, 0.0)

    stage = []
    for k in range(CHUNKS):
        rows = jnp.concatenate([stacked(left1, k), stacked(left2, k)], axis=0)
        part = slice(CHUNK * k, CHUNK * (k + 1))
        cols = jnp.concatenate([right1[part], right2[part]], axis=0)
        g = fine(rows, cols, NT)
        a = square(g[:128, :64], strict)
        kb = square(g[:128, 64:], strict)
        ru = square(g[128:, :64], upto)
        ku = square(g[128:, 64:], upto)
        stage.append([a, kb, ru, ku])
    inverse = []
    for k in range(CHUNKS):
        a = stage[k][0]
        small = jnp.where(in16, a, 0.0)
        power = small
        t = eye + small
        for _ in range(3):
            power = fine(power, power)
            t = t + fine(t, power)
        t = t + fine(fine(t, jnp.where(in32 & ~in16, a, 0.0)), t)
        t = t + fine(fine(t, jnp.where(in32, 0.0, a)), t)
        inverse.append(t)
    pair = jnp.concatenate([jnp.zeros((128, 128), F32), eye], axis=0)
    for k in range(CHUNKS):
        _, kb, ru, ku = stage[k]
        v = stacked(value, k)
        xy = fine(inverse[k], jnp.concatenate([stacked(start1, k), fine(kb, v)], axis=1))
        read = fine(ru, xy)
        coef = stacked(start2, k) + read[:, :128]
        rest = read[:, 128:] + fine(ku, v)
        t1, t2 = stacked(tail1, k), stacked(tail2, k)
        moved = fine(xy, t1, TN)
        decay = whole[CHUNK * k : CHUNK * k + 1]
        step = moved[:128] + jnp.where(rr == cc, decay, 0.0)
        add = moved[128:] + fine(v, t2, TN)
        out = fine(coef, pair, NT)
        near = out[:, :128] + rest
        far = out[:, 128:]
        part = slice(CHUNK * k, CHUNK * (k + 1))
        free[part] = near[:64] + near[64:]
        along[part] = far[:64] + far[64:]
        pair = fine(pair, step) + jnp.concatenate([add, jnp.zeros((128, 128), F32)], axis=0)
    far = (pair[128:192] + pair[192:]).astype(BF16)
    near = (pair[:64] + pair[64:128]).astype(BF16)
    for i in range(16):
        state[i, 0] = far
        state[i, 1] = near


def recur(*args):
    wide = jax.ShapeDtypeStruct((ROWS, 128), F32)
    outs = [wide, wide, wide, jax.ShapeDtypeStruct((16, 2, 64, 128), BF16)]
    specs = [VMEM] * 14
    return call(recur_body, outs, args, 8 << 30, specs=specs, limit=RECUR_LIMIT)


def attend_body(q, own, peer, w, glat, gain, table, att, logs, acc, top):
    sp = lax.axis_index("sp")
    ones = jnp.where(iota((NOPE, ROWS), 0) == 0, 1.0, 0.0).astype(BF16)

    def keys(j):
        lat = jnp.concatenate(
            [own[:, j, 0:32, :].reshape(128, ROWS), peer[:, j, 0:32, :].reshape(128, ROWS)], axis=0
        ).astype(F32)
        rope = (own[:, j, 32:40, :].astype(F32) + peer[:, j, 32:40, :].astype(F32)).reshape(
            ROPE, ROWS
        )
        lat = lat * lax.rsqrt(jnp.mean(lat * lat, axis=0, keepdims=True) + EPS) * glat[:, 0:1]
        kv = dot(w[...], lat.astype(BF16)).astype(BF16)
        rope_sum = jnp.sum(rope * rope, axis=0, keepdims=True)
        turn = table[j]
        cosine, sine = turn[:16], turn[16:]
        ra, rb = rope[:16] * gain[64:80, 0:1], rope[16:] * gain[80:96, 0:1]
        ra, rb = ra * cosine - rb * sine, rb * cosine + ra * sine
        ready, values = [], []
        for h in range(2):
            k = kv[64 * h : 64 * (h + 1)].astype(F32)
            scale = lax.rsqrt(
                (jnp.sum(k * k, axis=0, keepdims=True) + rope_sum) * np.float32(1 / QK) + EPS
            )
            ready.append(
                jnp.concatenate([k * scale * gain[0:64, 0:1], ra * scale, rb * scale], axis=0).astype(
                    BF16
                )
            )
            values.append(jnp.concatenate([kv[128 + 64 * h : 192 + 64 * h], ones], axis=0))
        return ready, values

    def block(places, first):
        made = [keys(j) for j in places]
        for h in range(2):
            ready = jnp.concatenate([m[0][h] for m in made], axis=1)
            v = jnp.concatenate([m[1][h] for m in made], axis=1)
            s = dot(q[h, :, 0:QK], ready)
            if first:
                s = jnp.where(iota((ROWS, ROWS), 1) <= iota((ROWS, ROWS), 0), s, -jnp.inf)
            peak = jnp.max(s, axis=1, keepdims=True)
            if first:
                top[h] = jnp.broadcast_to(peak, (ROWS, 128))
                acc[h] = dot(jnp.exp2(s - peak).astype(BF16), v, NT)
            else:
                old = top[h]
                new = jnp.maximum(old, peak)
                top[h] = new
                p = jnp.exp2(s - new[:, 0:1]).astype(BF16)
                acc[h] = acc[h] * jnp.exp2(old - new) + dot(p, v, NT)

    block([sp], True)

    def loop(i, carry):
        block([3 * i, 3 * i + 1, 3 * i + 2], False)
        return carry

    lax.fori_loop(0, sp // 3, loop, 0)

    @pl.when(lax.rem(sp, 3) == 1)
    def _():
        block([sp - 1], False)

    @pl.when(lax.rem(sp, 3) == 2)
    def _():
        block([sp - 2, sp - 1], False)

    parts = []
    rows = []
    for h in range(2):
        total = acc[h][:, 64:65]
        parts.append(acc[h][:, 0:64] / total)
        full = top[h] * np.float32(np.log(2.0)) + jnp.log(jnp.broadcast_to(total, (ROWS, 128)))
        rows.append(full.T[0:1])
    att[...] = jnp.concatenate(parts, axis=1).astype(BF16)
    logs[...] = jnp.concatenate(rows, axis=0)


def attend(*args):
    outs = [jax.ShapeDtypeStruct((ROWS, 128), BF16), jax.ShapeDtypeStruct((2, ROWS), F32)]
    scratch = [pltpu.VMEM((2, ROWS, 128), F32), pltpu.VMEM((2, ROWS, 128), F32)]
    return call(attend_body, outs, args, 8 << 30, scratch, [VMEM] * 7)


def merge_body(att, free, along, bonus, states, branch, o0, o1, o2, o3, keep, send):
    head = iota((128, 128), 0) // 64 == iota((128, 128), 1) // 64

    def spread(v):
        return jnp.where(head, jnp.concatenate([v, v], axis=0), jnp.zeros((), v.dtype))

    sp = lax.axis_index("sp")
    eye = jnp.where(iota((128, 128), 0) == iota((128, 128), 1), 1.0, 0.0).astype(BF16)
    below = jnp.zeros((128, 128), F32)
    entering = below
    groups = []
    for g in range(4):
        pair = None
        for r in range(4 * g, 4 * g + 4):
            move = jnp.where(r < sp, spread(states[r, 0]), eye)
            add = jnp.where(r < sp, spread(states[r, 1]).astype(F32), 0.0)
            if pair is None:
                pair = jnp.concatenate([add, move.astype(F32)], axis=0)
            else:
                pair = dot_wide(pair, move) + jnp.concatenate([add, below], axis=0)
        groups.append(pair)
    entering = groups[0][:128]
    for pair in groups[1:]:
        entering = fine(entering, pair[128:]) + pair[:128]
    read = free[...] + fine(along[...], entering, NT)
    mean = jnp.where(head, 1.0 / 64, 0.0).astype(BF16)
    read = read - dot_wide(read, mean)
    spread_of = dot_wide(read * read, mean)
    rec = read * lax.rsqrt(spread_of + GROUP_EPS) * branch[...] + bonus[...]
    both = jnp.concatenate([att[...].astype(F32), rec], axis=1).reshape(4, 2, 32, 256)
    core = lax.rem(lax.axis_index("tp"), 2)
    even, odd = both[:, 0].reshape(128, 256), both[:, 1].reshape(128, 256)
    kept = jnp.where(core == 0, even, odd).astype(BF16)
    sent = jnp.where(core == 0, odd, even).astype(BF16)
    for k, o in enumerate((o0, o1, o2, o3)):
        send[:, columns(k)] = dot(sent, o[192:448]).astype(BF16)
    for k, o in enumerate((o0, o1, o2, o3)):
        keep[:, columns(k)] = dot(kept, o[192:448])


def merge(*args):
    outs = [jax.ShapeDtypeStruct((128, 2048), F32), jax.ShapeDtypeStruct((128, 2048), BF16)]
    return call(merge_body, outs, args, 4 << 30, specs=[VMEM] * 10)


def exchanged(copies, axis, groups=None):
    return lax.all_to_all(copies, axis, 0, 0, axis_index_groups=groups, tiled=True)


def around(value):
    moves = [[(i, (i + by) % 4) for i in range(4)] for by in (1, 3, 2)]
    return [value] + [lax.ppermute(value, "fs", move) for move in moves]


def other_core(value):
    return lax.ppermute(value, "tp", [(i, i ^ 1) for i in range(8)])


def turn_table():
    half = ROPE // 2
    inverse = np.float32(10000.0) ** (-np.arange(half, dtype=np.float32) / np.float32(half))
    angle = np.arange(4096, dtype=np.float32)[:, None] * inverse.astype(np.float32)[None, :]
    both = np.concatenate([np.cos(angle), np.sin(angle)], axis=1).astype(np.float32)
    return both.reshape(16, ROWS, ROPE).transpose(0, 2, 1)


def shards(
    entering,
    entering_gain,
    wq,
    wc,
    wr,
    compact_gain,
    wk_up,
    wv_up,
    q_gain,
    k_gain,
    w_accept,
    w_key,
    w_value,
    fade1,
    fade2,
    fade_bias,
    fade_mult,
    fade_extra,
    adapt1,
    adapt2,
    adapt_bias,
    present,
    branch,
    wo_att,
    wo_rec,
):
    xs, small, big, late = prepare(
        entering[0],
        entering_gain.reshape(1, 2048),
        w_accept,
        w_key,
        w_value,
        wq.T,
        wc,
        wr.T,
        wo_att,
        wo_rec,
    )
    normed = exchanged(xs, "tp").reshape(ROWS, 2048)
    smalls = around(small)
    bigs = around(big)
    lates = around(late)

    table = jnp.asarray(turn_table())
    pay = latents(normed, *smalls)
    lat = exchanged(pay, "sp")

    dlow, rlow, turn, up, glat, key_gain, query_gain = lowrank(
        normed,
        fade1,
        adapt1,
        table,
        wk_up,
        wv_up,
        compact_gain.reshape(1, 256),
        k_gain.reshape(1, QK),
        q_gain.reshape(1, QK),
    )
    free, along, bonus, state = recur(
        normed,
        *bigs,
        dlow,
        rlow,
        fade2,
        fade_bias.reshape(1, 128),
        adapt2,
        adapt_bias.reshape(1, 128),
        fade_mult[0],
        fade_extra[0],
        present,
    )
    lat, state = lax.optimization_barrier((lat, state))
    states = exchanged(state, "sp")
    others = [lax.ppermute(lat, "tp", [(i, (i + by) % 8) for i in range(8)]) for by in (2, 6, 4)]
    lat_own = collect(lat, *others)
    lat_peer = other_core(lat_own)
    q = queries(normed, *lates, turn, query_gain)
    att, logs = attend(q, lat_own, lat_peer, up, glat, key_gain, table)
    keep, send = merge(att, free, along, bonus, states, branch.reshape(1, 128), *lates)
    pair = (keep + other_core(send).astype(F32)).astype(BF16)
    same_core = [[0, 2, 4, 6], [1, 3, 5, 7]]
    parts = exchanged(pair.reshape(4, 32, 2048), "tp", same_core)
    mixed = jnp.sum(parts.astype(F32), axis=0).astype(BF16)
    return mixed[None], logs[None]


def solution(mesh):
    placed = (
        P("fs", ("sp", "tp"), None),
        P(),
        P("fs", "tp"),
        P("fs", None),
        P("fs", None),
        P(),
        P(None, "tp"),
        P(None, "tp"),
        P(),
        P(),
        P("fs", "tp"),
        P("fs", "tp"),
        P("fs", "tp"),
        P(),
        P(None, "tp"),
        P("tp"),
        P("fs", "tp", "sp"),
        P("fs", "tp", "sp"),
        P(),
        P(None, "tp"),
        P("tp"),
        P("tp", None),
        P("tp"),
        P("tp", "fs"),
        P("tp", "fs"),
    )

    return jax.shard_map(
        shards,
        mesh=mesh,
        in_specs=placed,
        out_specs=(P("fs", ("sp", "tp"), None), P("fs", "tp", "sp")),
        check_vma=False,
    )
```

```python
import jax
import jax.numpy as jnp
import numpy as np
from jax import lax
from jax.experimental import pallas as pl
from jax.experimental.pallas import tpu as pltpu
from jax.sharding import PartitionSpec as P


F32 = jnp.float32
BF16 = jnp.bfloat16

ROWS = 256
NOPE = 64
ROPE = 32
QK = NOPE + ROPE
CHUNK = 64
RECUR_LIMIT = 63.9
CHUNKS = ROWS // CHUNK
EPS = 1e-6
GROUP_EPS = 0.00064
NN = (((1,), (0,)), ((), ()))
NT = (((1,), (1,)), ((), ()))
TN = (((0,), (0,)), ((), ()))

VMEM = pl.BlockSpec(memory_space=pltpu.VMEM)
HBM = pl.BlockSpec(memory_space=pltpu.HBM)


def dot(a, b, dims=NN):
    return lax.dot_general(a, b, dims, preferred_element_type=F32)


def halves(a):
    high = a.astype(BF16)
    return high, (a - high.astype(F32)).astype(BF16)


def fine(a, b, dims=NN):
    (i,), (j,) = dims[0]
    ah, al = halves(a)
    bh, bl = halves(b)
    wide = dot(jnp.concatenate([ah, al], axis=i), jnp.concatenate([bh, bh], axis=j), dims)
    return wide + dot(ah, bl, dims)


def dot_wide(a, b):
    high, low = halves(a)
    return dot(jnp.concatenate([high, low], axis=1), jnp.concatenate([b, b], axis=0))


def iota(shape, dim):
    return lax.broadcasted_iota(jnp.int32, shape, dim)


def call(body, outs, args, flops, scratch=(), specs=None, limit=24):
    return pl.pallas_call(
        body,
        out_shape=outs,
        in_specs=specs or [VMEM] * len(args),
        out_specs=jax.tree.map(lambda _: VMEM, outs),
        scratch_shapes=scratch,
        compiler_params=pltpu.CompilerParams(vmem_limit_bytes=int(limit * (1 << 20))),
        cost_estimate=pl.CostEstimate(flops=flops, bytes_accessed=4 << 20, transcendentals=0),
    )(*args)


def turned(n, table):
    half = ROPE // 2
    a, b = n[NOPE : NOPE + half], n[NOPE + half :]
    cosine, sine = table[:half], table[half:]
    return a * cosine - b * sine, b * cosine + a * sine


def prepare_body(
    x_in, gain_in, wa_in, wk_in, wv_in, wq_in, wc_in, wr_in, oa_in, or_in,
    xs, small, big, late, x, gain, wa, wk, wv, wq, wc, wr, oa, orr, turned_wc, arrived,
):
    pairs = [
        (x_in, x), (gain_in, gain), (wc_in, wc), (wr_in, wr), (wa_in, wa), (wk_in, wk),
        (wv_in, wv), (wq_in, wq), (oa_in, oa), (or_in, orr),
    ]
    copies = [pltpu.make_async_copy(a, b, arrived.at[i]) for i, (a, b) in enumerate(pairs)]
    for copy in copies:
        copy.start()
    copies[0].wait()
    copies[1].wait()
    v = x[...].astype(F32)
    v = v * lax.rsqrt(jnp.mean(v * v, axis=-1, keepdims=True) + EPS) * gain[...]
    v = v.astype(BF16)
    for i in range(8):
        xs[i] = v
    copies[2].wait()
    copies[3].wait()
    turned_wc[...] = wc[...].astype(F32).T
    start = pl.multiple_of(lax.axis_index("tp") * 32, 32)
    small[0:32] = turned_wc[pl.ds(start, 32), :].astype(BF16)
    small[32:64] = wr[...]
    for copy in copies[4:]:
        copy.wait()
    big[:, 0:128] = wa[...]
    big[:, 128:256] = wk[...]
    big[:, 256:384] = wv[...]
    late[0:192] = wq[...]
    late[192:320] = oa[...]
    late[320:448] = orr[...]


def prepare(*args):
    outs = [
        jax.ShapeDtypeStruct((8, 32, 2048), BF16),
        jax.ShapeDtypeStruct((64, 512), BF16),
        jax.ShapeDtypeStruct((512, 384), BF16),
        jax.ShapeDtypeStruct((448, 512), BF16),
    ]
    scratch = [pltpu.VMEM(a.shape, a.dtype) for a in args]
    scratch += [pltpu.VMEM((256, 512), F32), pltpu.SemaphoreType.DMA((10,))]
    return call(prepare_body, outs, args, 1 << 29, scratch, [HBM] * 10, 63.9)


def collect_body(own, left, right, far, out):
    chip = lax.axis_index("tp") // 2
    for by, part in ((0, own), (3, left), (1, right), (2, far)):
        out[lax.rem(chip + by, 4)] = part[...]


def collect(*parts):
    outs = jax.ShapeDtypeStruct((4, *parts[0].shape), BF16)
    return call(collect_body, outs, parts, 1 << 29)


def lowrank_body(
    x, fd, fa, table, wk_up, wv_up, compact_gain, kg, qg,
    dlow, rlow, turn, up, glat, key_gain, query_gain,
):
    core = lax.rem(lax.axis_index("tp"), 2)
    dlow[...] = jnp.tanh(dot(x[...], fd[...]).astype(BF16).astype(F32)).astype(BF16)
    rlow[...] = dot(x[...], fa[...]).astype(BF16)
    turn[...] = table[lax.axis_index("sp")]

    def reordered(v):
        v = v.reshape(4, 2, 32, v.shape[-1])
        even, odd = v[:, 0].reshape(128, -1), v[:, 1].reshape(128, -1)
        first, second = jnp.where(core == 0, even, odd), jnp.where(core == 0, odd, even)
        return jnp.concatenate([first, second], axis=0)

    both = jnp.concatenate([wk_up[...], wv_up[...]], axis=1).astype(F32)
    up[...] = reordered(both).T.astype(BF16)
    glat[...] = reordered(jnp.broadcast_to(compact_gain[...], (128, 256)).T)
    for source, out in ((kg, key_gain), (qg, query_gain)):
        wide = jnp.concatenate([source[...], jnp.zeros((1, 128 - QK), F32)], axis=1)
        out[...] = jnp.broadcast_to(wide, (128, 128)).T[0:QK]


def lowrank(*args):
    column = jax.ShapeDtypeStruct((QK, 128), F32)
    outs = [
        jax.ShapeDtypeStruct((ROWS, 128), BF16),
        jax.ShapeDtypeStruct((ROWS, 128), BF16),
        jax.ShapeDtypeStruct((ROPE, ROWS), F32),
        jax.ShapeDtypeStruct((256, 256), BF16),
        jax.ShapeDtypeStruct((256, 128), F32),
        column,
        column,
    ]
    return call(lowrank_body, outs, args, 1 << 29, specs=[VMEM] * 9, limit=63.9)


def columns(k):
    shard = lax.rem(lax.axis_index("fs") + (0, 3, 1, 2)[k], 4)
    return pl.ds(pl.multiple_of(shard * 512, 512), 512)


def latents_body(x, w0, w1, w2, w3, pay):
    t = jnp.zeros((64, ROWS), F32)
    for k, w in enumerate((w0, w1, w2, w3)):
        t += dot(w[...], x[:, columns(k)], NT)
    tp = lax.axis_index("tp")
    group = jnp.zeros((8, ROWS), F32)
    for g in range(4):
        group += jnp.where(tp // 2 == g, t[32 + 8 * g : 40 + 8 * g], 0.0)
    group = jnp.where(iota((8, ROWS), 0) // 4 == lax.rem(tp, 2), group, 0.0)
    both = jnp.concatenate([t[0:32], group], axis=0).astype(BF16)
    for i in range(16):
        pay[i] = both


def latents(*args):
    outs = jax.ShapeDtypeStruct((16, 40, ROWS), BF16)
    return call(latents_body, outs, args, 1 << 29, specs=[VMEM] * 5, limit=63.9)


def queries_body(x, w0, w1, w2, w3, turn, gain, q):
    t = jnp.zeros((192, ROWS), F32)
    for k, w in enumerate((w0, w1, w2, w3)):
        t += dot(w[0:192], x[:, columns(k)], NT)
    t = t.astype(BF16).astype(F32)
    factor = np.float32(QK**-0.5 * np.log2(np.e))
    for h in range(2):
        v = t[QK * h : QK * (h + 1)]
        n = v * (lax.rsqrt(jnp.mean(v * v, axis=0, keepdims=True) + EPS) * factor) * gain[:, 0:1]
        a, b = turned(n, turn[...])
        ready = jnp.concatenate([n[:NOPE], a, b, jnp.zeros((128 - QK, ROWS), F32)], axis=0)
        q[h] = ready.T.astype(BF16)


def queries(*args):
    outs = jax.ShapeDtypeStruct((2, ROWS, 128), BF16)
    return call(queries_body, outs, args, 1 << 29, specs=[VMEM] * 7)


def recur_body(
    x, w0, w1, w2, w3, dlow, rlow, wd, bd, wa, ba, mult, extra, present,
    free, along, bonus, state,
):
    lane = iota((1, 128), 1)
    y = jnp.zeros((ROWS, 384), F32)
    for k, w in enumerate((w0, w1, w2, w3)):
        y += dot(x[:, columns(k)], w[...])
    y = y.astype(BF16).astype(F32)
    recept, key, value = (y[:, 128 * i : 128 * (i + 1)] for i in range(3))
    speed = jax.nn.sigmoid(bd[...] + dot(dlow[...], wd[...])) * np.float32(np.exp(-0.5))
    added = jnp.where(iota((128, ROWS), 0) < 64, extra[0:1], extra[1:2]).T
    ld = added - speed * jnp.where(lane < 64, mult[0:1, 0:1], mult[1:2, 0:1])
    here = jnp.concatenate([present[0:1], present[1:2]], axis=1)
    learn = jax.nn.sigmoid(ba[...] + dot(rlow[...], wa[...]))
    same = (iota((128, 128), 0) // 64 == iota((128, 128), 1) // 64).astype(BF16)
    unit = key * lax.rsqrt(dot_wide(key * key, same) + EPS)
    bonus[...] = dot_wide(recept * key * here, same) * value
    r, c = iota((ROWS, ROWS), 0), iota((ROWS, ROWS), 1)
    block = r // CHUNK == c // CHUNK
    sums = jnp.concatenate(
        [
            jnp.where(block & (c <= r), 1.0, 0.0),
            jnp.where(block & (lax.rem(c, CHUNK) < CHUNK // 2), 1.0, 0.0),
            jnp.where(block, 1.0, 0.0),
        ],
        axis=0,
    )
    sums = sums.astype(BF16)
    high, low = halves(ld)
    last = (ld - high.astype(F32) - low.astype(F32)).astype(BF16)
    sums = dot(
        jnp.concatenate([sums, sums, sums], axis=1), jnp.concatenate([high, low, last], axis=0)
    )
    cum, mid, end = sums[:ROWS], sums[ROWS : 2 * ROWS], sums[2 * ROWS :]
    prev = cum - ld
    toward = -unit
    remove = unit * learn
    grow, shrink = jnp.exp(cum - mid), jnp.exp(mid - cum)
    left1, left2 = toward * jnp.exp(prev - mid), recept * grow
    right1, right2 = remove * shrink, key * shrink
    start1, start2 = toward * jnp.exp(prev), recept * jnp.exp(cum)
    tail = jnp.exp(end - cum)
    tail1, tail2 = remove * tail, key * tail
    whole = jnp.exp(end)
    m0 = iota((CHUNK, 128), 1) < 64

    def stacked(v, k):
        v = v[CHUNK * k : CHUNK * (k + 1)]
        return jnp.concatenate([jnp.where(m0, v, 0.0), jnp.where(m0, 0.0, v)], axis=0)

    rr, cc = iota((128, 128), 0), iota((128, 128), 1)
    head = rr // 64 == cc // 64
    eye = jnp.where(rr == cc, 1.0, 0.0)
    in8, in16, in32 = (rr // n == cc // n for n in (8, 16, 32))
    strict, upto = head & (rr > cc), head & (rr >= cc)

    def square(top, mask):
        both = jnp.concatenate([top, top], axis=1)
        return jnp.where(mask, both, 0.0)

    stage = []
    for k in range(CHUNKS):
        rows = jnp.concatenate([stacked(left1, k), stacked(left2, k)], axis=0)
        part = slice(CHUNK * k, CHUNK * (k + 1))
        cols = jnp.concatenate([right1[part], right2[part]], axis=0)
        g = fine(rows, cols, NT)
        a = square(g[:128, :64], strict)
        kb = square(g[:128, 64:], strict)
        ru = square(g[128:, :64], upto)
        ku = square(g[128:, 64:], upto)
        stage.append([a, kb, ru, ku])
    inverse = []
    for k in range(CHUNKS):
        a = stage[k][0]
        small = jnp.where(in8, a, 0.0)
        power = small
        t = eye + small
        for _ in range(2):
            power = fine(power, power)
            t = t + fine(t, power)
        for wider, narrower in ((in16, in8), (in32, in16), (None, in32)):
            rest = jnp.where(narrower, 0.0, a)
            rest = rest if wider is None else jnp.where(wider, rest, 0.0)
            t = t + fine(fine(t, rest), t)
        inverse.append(t)
    pair = jnp.concatenate([jnp.zeros((128, 128), F32), eye], axis=0)
    for k in range(CHUNKS):
        _, kb, ru, ku = stage[k]
        v = stacked(value, k)
        xy = fine(inverse[k], jnp.concatenate([stacked(start1, k), fine(kb, v)], axis=1))
        read = fine(ru, xy)
        coef = stacked(start2, k) + read[:, :128]
        rest = read[:, 128:] + fine(ku, v)
        t1, t2 = stacked(tail1, k), stacked(tail2, k)
        moved = fine(xy, t1, TN)
        decay = whole[CHUNK * k : CHUNK * k + 1]
        step = moved[:128] + jnp.where(rr == cc, decay, 0.0)
        add = moved[128:] + fine(v, t2, TN)
        out = fine(coef, pair, NT)
        near = out[:, :128] + rest
        far = out[:, 128:]
        part = slice(CHUNK * k, CHUNK * (k + 1))
        free[part] = near[:64] + near[64:]
        along[part] = far[:64] + far[64:]
        pair = fine(pair, step) + jnp.concatenate([add, jnp.zeros((128, 128), F32)], axis=0)
    far = (pair[128:192] + pair[192:]).astype(BF16)
    near = (pair[:64] + pair[64:128]).astype(BF16)
    for i in range(16):
        state[i, 0] = far
        state[i, 1] = near


def recur(*args):
    wide = jax.ShapeDtypeStruct((ROWS, 128), F32)
    outs = [wide, wide, wide, jax.ShapeDtypeStruct((16, 2, 64, 128), BF16)]
    specs = [VMEM] * 14
    return call(recur_body, outs, args, 8 << 30, specs=specs, limit=RECUR_LIMIT)


def attend_body(q, own, peer, w, glat, gain, table, att, logs, acc, top):
    sp = lax.axis_index("sp")
    ones = jnp.where(iota((NOPE, ROWS), 0) == 0, 1.0, 0.0).astype(BF16)

    def keys(j):
        lat = jnp.concatenate(
            [own[:, j, 0:32, :].reshape(128, ROWS), peer[:, j, 0:32, :].reshape(128, ROWS)], axis=0
        ).astype(F32)
        rope = (own[:, j, 32:40, :].astype(F32) + peer[:, j, 32:40, :].astype(F32)).reshape(
            ROPE, ROWS
        )
        lat = lat * lax.rsqrt(jnp.mean(lat * lat, axis=0, keepdims=True) + EPS) * glat[:, 0:1]
        kv = dot(w[...], lat.astype(BF16)).astype(BF16)
        rope_sum = jnp.sum(rope * rope, axis=0, keepdims=True)
        turn = table[j]
        cosine, sine = turn[:16], turn[16:]
        ra, rb = rope[:16] * gain[64:80, 0:1], rope[16:] * gain[80:96, 0:1]
        ra, rb = ra * cosine - rb * sine, rb * cosine + ra * sine
        ready, values = [], []
        for h in range(2):
            k = kv[64 * h : 64 * (h + 1)].astype(F32)
            scale = lax.rsqrt(
                (jnp.sum(k * k, axis=0, keepdims=True) + rope_sum) * np.float32(1 / QK) + EPS
            )
            ready.append(
                jnp.concatenate([k * scale * gain[0:64, 0:1], ra * scale, rb * scale], axis=0).astype(
                    BF16
                )
            )
            values.append(jnp.concatenate([kv[128 + 64 * h : 192 + 64 * h], ones], axis=0))
        return ready, values

    def block(places, first):
        made = [keys(j) for j in places]
        for h in range(2):
            ready = jnp.concatenate([m[0][h] for m in made], axis=1)
            v = jnp.concatenate([m[1][h] for m in made], axis=1)
            s = dot(q[h, :, 0:QK], ready)
            if first:
                s = jnp.where(iota((ROWS, ROWS), 1) <= iota((ROWS, ROWS), 0), s, -jnp.inf)
            peak = jnp.max(s, axis=1, keepdims=True)
            if first:
                top[h] = jnp.broadcast_to(peak, (ROWS, 128))
                acc[h] = dot(jnp.exp2(s - peak).astype(BF16), v, NT)
            else:
                old = top[h]
                new = jnp.maximum(old, peak)
                top[h] = new
                p = jnp.exp2(s - new[:, 0:1]).astype(BF16)
                acc[h] = acc[h] * jnp.exp2(old - new) + dot(p, v, NT)

    block([sp], True)

    def loop(i, carry):
        block([3 * i, 3 * i + 1, 3 * i + 2], False)
        return carry

    lax.fori_loop(0, sp // 3, loop, 0)

    @pl.when(lax.rem(sp, 3) == 1)
    def _():
        block([sp - 1], False)

    @pl.when(lax.rem(sp, 3) == 2)
    def _():
        block([sp - 2, sp - 1], False)

    parts = []
    rows = []
    for h in range(2):
        total = acc[h][:, 64:65]
        parts.append(acc[h][:, 0:64] / total)
        full = top[h] * np.float32(np.log(2.0)) + jnp.log(jnp.broadcast_to(total, (ROWS, 128)))
        rows.append(full.T[0:1])
    att[...] = jnp.concatenate(parts, axis=1).astype(BF16)
    logs[...] = jnp.concatenate(rows, axis=0)


def attend(*args):
    outs = [jax.ShapeDtypeStruct((ROWS, 128), BF16), jax.ShapeDtypeStruct((2, ROWS), F32)]
    scratch = [pltpu.VMEM((2, ROWS, 128), F32), pltpu.VMEM((2, ROWS, 128), F32)]
    return call(attend_body, outs, args, 8 << 30, scratch, [VMEM] * 7)


def merge_body(att, free, along, bonus, states, branch, o0, o1, o2, o3, keep, send):
    head = iota((128, 128), 0) // 64 == iota((128, 128), 1) // 64

    def spread(v):
        return jnp.where(head, jnp.concatenate([v, v], axis=0), jnp.zeros((), v.dtype))

    sp = lax.axis_index("sp")
    eye = jnp.where(iota((128, 128), 0) == iota((128, 128), 1), 1.0, 0.0).astype(BF16)
    below = jnp.zeros((128, 128), F32)
    entering = below
    groups = []
    for g in range(4):
        pair = None
        for r in range(4 * g, 4 * g + 4):
            move = jnp.where(r < sp, spread(states[r, 0]), eye)
            add = jnp.where(r < sp, spread(states[r, 1]).astype(F32), 0.0)
            if pair is None:
                pair = jnp.concatenate([add, move.astype(F32)], axis=0)
            else:
                pair = dot_wide(pair, move) + jnp.concatenate([add, below], axis=0)
        groups.append(pair)
    entering = groups[0][:128]
    for pair in groups[1:]:
        entering = fine(entering, pair[128:]) + pair[:128]
    read = free[...] + fine(along[...], entering, NT)
    mean = jnp.where(head, 1.0 / 64, 0.0).astype(BF16)
    read = read - dot_wide(read, mean)
    spread_of = dot_wide(read * read, mean)
    rec = read * lax.rsqrt(spread_of + GROUP_EPS) * branch[...] + bonus[...]
    both = jnp.concatenate([att[...].astype(F32), rec], axis=1).reshape(4, 2, 32, 256)
    core = lax.rem(lax.axis_index("tp"), 2)
    even, odd = both[:, 0].reshape(128, 256), both[:, 1].reshape(128, 256)
    kept = jnp.where(core == 0, even, odd).astype(BF16)
    sent = jnp.where(core == 0, odd, even).astype(BF16)
    for k, o in enumerate((o0, o1, o2, o3)):
        send[:, columns(k)] = dot(sent, o[192:448]).astype(BF16)
    for k, o in enumerate((o0, o1, o2, o3)):
        keep[:, columns(k)] = dot(kept, o[192:448])


def merge(*args):
    outs = [jax.ShapeDtypeStruct((128, 2048), F32), jax.ShapeDtypeStruct((128, 2048), BF16)]
    return call(merge_body, outs, args, 4 << 30, specs=[VMEM] * 10)


def exchanged(copies, axis, groups=None):
    return lax.all_to_all(copies, axis, 0, 0, axis_index_groups=groups, tiled=True)


def around(value):
    moves = [[(i, (i + by) % 4) for i in range(4)] for by in (1, 3, 2)]
    return [value] + [lax.ppermute(value, "fs", move) for move in moves]


def other_core(value):
    return lax.ppermute(value, "tp", [(i, i ^ 1) for i in range(8)])


def turn_table():
    half = ROPE // 2
    inverse = np.float32(10000.0) ** (-np.arange(half, dtype=np.float32) / np.float32(half))
    angle = np.arange(4096, dtype=np.float32)[:, None] * inverse.astype(np.float32)[None, :]
    both = np.concatenate([np.cos(angle), np.sin(angle)], axis=1).astype(np.float32)
    return both.reshape(16, ROWS, ROPE).transpose(0, 2, 1)


def shards(
    entering,
    entering_gain,
    wq,
    wc,
    wr,
    compact_gain,
    wk_up,
    wv_up,
    q_gain,
    k_gain,
    w_accept,
    w_key,
    w_value,
    fade1,
    fade2,
    fade_bias,
    fade_mult,
    fade_extra,
    adapt1,
    adapt2,
    adapt_bias,
    present,
    branch,
    wo_att,
    wo_rec,
):
    xs, small, big, late = prepare(
        entering[0],
        entering_gain.reshape(1, 2048),
        w_accept,
        w_key,
        w_value,
        wq.T,
        wc,
        wr.T,
        wo_att,
        wo_rec,
    )
    normed = exchanged(xs, "tp").reshape(ROWS, 2048)
    smalls = around(small)
    bigs = around(big)
    lates = around(late)

    table = jnp.asarray(turn_table())
    pay = latents(normed, *smalls)
    lat = exchanged(pay, "sp")

    dlow, rlow, turn, up, glat, key_gain, query_gain = lowrank(
        normed,
        fade1,
        adapt1,
        table,
        wk_up,
        wv_up,
        compact_gain.reshape(1, 256),
        k_gain.reshape(1, QK),
        q_gain.reshape(1, QK),
    )
    free, along, bonus, state = recur(
        normed,
        *bigs,
        dlow,
        rlow,
        fade2,
        fade_bias.reshape(1, 128),
        adapt2,
        adapt_bias.reshape(1, 128),
        fade_mult[0],
        fade_extra[0],
        present,
    )
    lat, state = lax.optimization_barrier((lat, state))
    states = exchanged(state, "sp")
    others = [lax.ppermute(lat, "tp", [(i, (i + by) % 8) for i in range(8)]) for by in (2, 6, 4)]
    lat_own = collect(lat, *others)
    lat_peer = other_core(lat_own)
    q = queries(normed, *lates, turn, query_gain)
    att, logs = attend(q, lat_own, lat_peer, up, glat, key_gain, table)
    keep, send = merge(att, free, along, bonus, states, branch.reshape(1, 128), *lates)
    pair = (keep + other_core(send).astype(F32)).astype(BF16)
    same_core = [[0, 2, 4, 6], [1, 3, 5, 7]]
    parts = exchanged(pair.reshape(4, 32, 2048), "tp", same_core)
    mixed = jnp.sum(parts.astype(F32), axis=0).astype(BF16)
    return mixed[None], logs[None]


def solution(mesh):
    placed = (
        P("fs", ("sp", "tp"), None),
        P(),
        P("fs", "tp"),
        P("fs", None),
        P("fs", None),
        P(),
        P(None, "tp"),
        P(None, "tp"),
        P(),
        P(),
        P("fs", "tp"),
        P("fs", "tp"),
        P("fs", "tp"),
        P(),
        P(None, "tp"),
        P("tp"),
        P("fs", "tp", "sp"),
        P("fs", "tp", "sp"),
        P(),
        P(None, "tp"),
        P("tp"),
        P("tp", None),
        P("tp"),
        P("tp", "fs"),
        P("tp", "fs"),
    )

    return jax.shard_map(
        shards,
        mesh=mesh,
        in_specs=placed,
        out_specs=(P("fs", ("sp", "tp"), None), P("fs", "tp", "sp")),
        check_vma=False,
    )
```

```python
import jax
import jax.numpy as jnp
import numpy as np
from jax import lax
from jax.experimental import pallas as pl
from jax.experimental.pallas import tpu as pltpu
from jax.sharding import PartitionSpec as P


F32 = jnp.float32
BF16 = jnp.bfloat16

ROWS = 256
NOPE = 64
ROPE = 32
QK = NOPE + ROPE
CHUNK = 64
RECUR_LIMIT = 63.9
CHUNKS = ROWS // CHUNK
EPS = 1e-6
GROUP_EPS = 0.00064
NN = (((1,), (0,)), ((), ()))
NT = (((1,), (1,)), ((), ()))
TN = (((0,), (0,)), ((), ()))

VMEM = pl.BlockSpec(memory_space=pltpu.VMEM)
HBM = pl.BlockSpec(memory_space=pltpu.HBM)


def dot(a, b, dims=NN):
    return lax.dot_general(a, b, dims, preferred_element_type=F32)


def halves(a):
    high = a.astype(BF16)
    return high, (a - high.astype(F32)).astype(BF16)


def fine(a, b, dims=NN):
    (i,), (j,) = dims[0]
    ah, al = halves(a)
    bh, bl = halves(b)
    wide = dot(jnp.concatenate([ah, al], axis=i), jnp.concatenate([bh, bh], axis=j), dims)
    return wide + dot(ah, bl, dims)


def dot_wide(a, b):
    high, low = halves(a)
    return dot(jnp.concatenate([high, low], axis=1), jnp.concatenate([b, b], axis=0))


def iota(shape, dim):
    return lax.broadcasted_iota(jnp.int32, shape, dim)


def call(body, outs, args, flops, scratch=(), specs=None, limit=24):
    return pl.pallas_call(
        body,
        out_shape=outs,
        in_specs=specs or [VMEM] * len(args),
        out_specs=jax.tree.map(lambda _: VMEM, outs),
        scratch_shapes=scratch,
        compiler_params=pltpu.CompilerParams(vmem_limit_bytes=int(limit * (1 << 20))),
        cost_estimate=pl.CostEstimate(flops=flops, bytes_accessed=4 << 20, transcendentals=0),
    )(*args)


def turned(n, table):
    half = ROPE // 2
    a, b = n[NOPE : NOPE + half], n[NOPE + half :]
    cosine, sine = table[:half], table[half:]
    return a * cosine - b * sine, b * cosine + a * sine


def prepare_body(
    x_in, gain_in, wa_in, wk_in, wv_in, wq_in, wc_in, wr_in, oa_in, or_in,
    xs, small, big, late, x, gain, wa, wk, wv, wq, wc, wr, oa, orr, turned_wc, arrived,
):
    pairs = [
        (x_in, x), (gain_in, gain), (wc_in, wc), (wr_in, wr), (wa_in, wa), (wk_in, wk),
        (wv_in, wv), (wq_in, wq), (oa_in, oa), (or_in, orr),
    ]
    copies = [pltpu.make_async_copy(a, b, arrived.at[i]) for i, (a, b) in enumerate(pairs)]
    for copy in copies:
        copy.start()
    copies[0].wait()
    copies[1].wait()
    v = x[...].astype(F32)
    v = v * lax.rsqrt(jnp.mean(v * v, axis=-1, keepdims=True) + EPS) * gain[...]
    v = v.astype(BF16)
    for i in range(8):
        xs[i] = v
    copies[2].wait()
    copies[3].wait()
    turned_wc[...] = wc[...].astype(F32).T
    start = pl.multiple_of(lax.axis_index("tp") * 32, 32)
    small[0:32] = turned_wc[pl.ds(start, 32), :].astype(BF16)
    small[32:64] = wr[...]
    for copy in copies[4:]:
        copy.wait()
    big[:, 0:128] = wa[...]
    big[:, 128:256] = wk[...]
    big[:, 256:384] = wv[...]
    late[0:192] = wq[...]
    late[192:320] = oa[...]
    late[320:448] = orr[...]


def prepare(*args):
    outs = [
        jax.ShapeDtypeStruct((8, 32, 2048), BF16),
        jax.ShapeDtypeStruct((64, 512), BF16),
        jax.ShapeDtypeStruct((512, 384), BF16),
        jax.ShapeDtypeStruct((448, 512), BF16),
    ]
    scratch = [pltpu.VMEM(a.shape, a.dtype) for a in args]
    scratch += [pltpu.VMEM((256, 512), F32), pltpu.SemaphoreType.DMA((10,))]
    return call(prepare_body, outs, args, 1 << 29, scratch, [HBM] * 10, 63.9)


def collect_body(own, left, right, far, out):
    chip = lax.axis_index("tp") // 2
    for by, part in ((0, own), (3, left), (1, right), (2, far)):
        out[lax.rem(chip + by, 4)] = part[...]


def collect(*parts):
    outs = jax.ShapeDtypeStruct((4, *parts[0].shape), BF16)
    return call(collect_body, outs, parts, 1 << 29)


def columns(k):
    shard = lax.rem(lax.axis_index("fs") + (0, 3, 1, 2)[k], 4)
    return pl.ds(pl.multiple_of(shard * 512, 512), 512)


def latents_body(x, w0, w1, w2, w3, pay):
    t = jnp.zeros((64, ROWS), F32)
    for k, w in enumerate((w0, w1, w2, w3)):
        t += dot(w[...], x[:, columns(k)], NT)
    tp = lax.axis_index("tp")
    group = jnp.zeros((8, ROWS), F32)
    for g in range(4):
        group += jnp.where(tp // 2 == g, t[32 + 8 * g : 40 + 8 * g], 0.0)
    group = jnp.where(iota((8, ROWS), 0) // 4 == lax.rem(tp, 2), group, 0.0)
    both = jnp.concatenate([t[0:32], group], axis=0).astype(BF16)
    for i in range(16):
        pay[i] = both


def latents(*args):
    outs = jax.ShapeDtypeStruct((16, 40, ROWS), BF16)
    return call(latents_body, outs, args, 1 << 29, limit=40)


def queries_body(
    x, w0, w1, w2, w3, table, wk_up, wv_up, compact_gain, kg, qg, q, up, glat, key_gain
):
    core = lax.rem(lax.axis_index("tp"), 2)

    def reordered(v):
        v = v.reshape(4, 2, 32, v.shape[-1])
        even, odd = v[:, 0].reshape(128, -1), v[:, 1].reshape(128, -1)
        first, second = jnp.where(core == 0, even, odd), jnp.where(core == 0, odd, even)
        return jnp.concatenate([first, second], axis=0)

    def column(source):
        wide = jnp.concatenate([source[...], jnp.zeros((1, 128 - QK), F32)], axis=1)
        return jnp.broadcast_to(wide, (128, 128)).T[0:QK]

    t = jnp.zeros((192, ROWS), F32)
    for k, w in enumerate((w0, w1, w2, w3)):
        t += dot(w[0:192], x[:, columns(k)], NT)
    t = t.astype(BF16).astype(F32)
    factor = np.float32(QK**-0.5 * np.log2(np.e))
    turn = table[lax.axis_index("sp")]
    gain = column(qg)[:, 0:1]
    for h in range(2):
        v = t[QK * h : QK * (h + 1)]
        n = v * (lax.rsqrt(jnp.mean(v * v, axis=0, keepdims=True) + EPS) * factor) * gain
        a, b = turned(n, turn)
        ready = jnp.concatenate([n[:NOPE], a, b, jnp.zeros((128 - QK, ROWS), F32)], axis=0)
        q[h] = ready.T.astype(BF16)
    both = jnp.concatenate([wk_up[...], wv_up[...]], axis=1).astype(F32)
    up[...] = reordered(both).T.astype(BF16)
    glat[...] = reordered(jnp.broadcast_to(compact_gain[...], (128, 256)).T)
    key_gain[...] = column(kg)


def queries(*args):
    outs = [
        jax.ShapeDtypeStruct((2, ROWS, 128), BF16),
        jax.ShapeDtypeStruct((256, 256), BF16),
        jax.ShapeDtypeStruct((256, 128), F32),
        jax.ShapeDtypeStruct((QK, 128), F32),
    ]
    return call(queries_body, outs, args, 1 << 29)


def recur_body(
    x, w0, w1, w2, w3, fd, fa, wd, bd, wa, ba, mult, extra, present,
    free, along, bonus, state,
):
    lane = iota((1, 128), 1)
    y = jnp.zeros((ROWS, 384), F32)
    for k, w in enumerate((w0, w1, w2, w3)):
        y += dot(x[:, columns(k)], w[...])
    y = y.astype(BF16).astype(F32)
    dlow = jnp.tanh(dot(x[...], fd[...]).astype(BF16).astype(F32)).astype(BF16)
    rlow = dot(x[...], fa[...]).astype(BF16)
    recept, key, value = (y[:, 128 * i : 128 * (i + 1)] for i in range(3))
    speed = jax.nn.sigmoid(bd[...] + dot(dlow, wd[...])) * np.float32(np.exp(-0.5))
    added = jnp.where(iota((128, ROWS), 0) < 64, extra[0:1], extra[1:2]).T
    ld = added - speed * jnp.where(lane < 64, mult[0:1, 0:1], mult[1:2, 0:1])
    here = jnp.concatenate([present[0:1], present[1:2]], axis=1)
    learn = jax.nn.sigmoid(ba[...] + dot(rlow, wa[...]))
    same = (iota((128, 128), 0) // 64 == iota((128, 128), 1) // 64).astype(BF16)
    unit = key * lax.rsqrt(dot_wide(key * key, same) + EPS)
    bonus[...] = dot_wide(recept * key * here, same) * value
    r, c = iota((ROWS, ROWS), 0), iota((ROWS, ROWS), 1)
    block = r // CHUNK == c // CHUNK
    sums = jnp.concatenate(
        [
            jnp.where(block & (c <= r), 1.0, 0.0),
            jnp.where(block & (lax.rem(c, CHUNK) < CHUNK // 2), 1.0, 0.0),
            jnp.where(block, 1.0, 0.0),
        ],
        axis=0,
    )
    sums = sums.astype(BF16)
    high, low = halves(ld)
    last = (ld - high.astype(F32) - low.astype(F32)).astype(BF16)
    sums = dot(
        jnp.concatenate([sums, sums, sums], axis=1), jnp.concatenate([high, low, last], axis=0)
    )
    cum, mid, end = sums[:ROWS], sums[ROWS : 2 * ROWS], sums[2 * ROWS :]
    prev = cum - ld
    toward = -unit
    remove = unit * learn
    grow, shrink = jnp.exp(cum - mid), jnp.exp(mid - cum)
    left1, left2 = toward * jnp.exp(prev - mid), recept * grow
    right1, right2 = remove * shrink, key * shrink
    start1, start2 = toward * jnp.exp(prev), recept * jnp.exp(cum)
    tail = jnp.exp(end - cum)
    tail1, tail2 = remove * tail, key * tail
    whole = jnp.exp(end)
    m0 = iota((CHUNK, 128), 1) < 64

    def stacked(v, k):
        v = v[CHUNK * k : CHUNK * (k + 1)]
        return jnp.concatenate([jnp.where(m0, v, 0.0), jnp.where(m0, 0.0, v)], axis=0)

    rr, cc = iota((128, 128), 0), iota((128, 128), 1)
    head = rr // 64 == cc // 64
    eye = jnp.where(rr == cc, 1.0, 0.0)
    in8, in16, in32 = (rr // n == cc // n for n in (8, 16, 32))
    strict, upto = head & (rr > cc), head & (rr >= cc)

    def square(top, mask):
        both = jnp.concatenate([top, top], axis=1)
        return jnp.where(mask, both, 0.0)

    stage = []
    for k in range(CHUNKS):
        rows = jnp.concatenate([stacked(left1, k), stacked(left2, k)], axis=0)
        part = slice(CHUNK * k, CHUNK * (k + 1))
        cols = jnp.concatenate([right1[part], right2[part]], axis=0)
        g = fine(rows, cols, NT)
        a = square(g[:128, :64], strict)
        kb = square(g[:128, 64:], strict)
        ru = square(g[128:, :64], upto)
        ku = square(g[128:, 64:], upto)
        stage.append([a, kb, ru, ku])
    inverse = []
    for k in range(CHUNKS):
        a = stage[k][0]
        small = jnp.where(in8, a, 0.0)
        power = small
        t = eye + small
        for _ in range(2):
            power = fine(power, power)
            t = t + fine(t, power)
        for wider, narrower in ((in16, in8), (in32, in16), (None, in32)):
            rest = jnp.where(narrower, 0.0, a)
            rest = rest if wider is None else jnp.where(wider, rest, 0.0)
            t = t + fine(fine(t, rest), t)
        inverse.append(t)
    pair = jnp.concatenate([jnp.zeros((128, 128), F32), eye], axis=0)
    for k in range(CHUNKS):
        _, kb, ru, ku = stage[k]
        v = stacked(value, k)
        xy = fine(inverse[k], jnp.concatenate([stacked(start1, k), fine(kb, v)], axis=1))
        read = fine(ru, xy)
        coef = stacked(start2, k) + read[:, :128]
        rest = read[:, 128:] + fine(ku, v)
        t1, t2 = stacked(tail1, k), stacked(tail2, k)
        moved = fine(xy, t1, TN)
        decay = whole[CHUNK * k : CHUNK * k + 1]
        step = moved[:128] + jnp.where(rr == cc, decay, 0.0)
        add = moved[128:] + fine(v, t2, TN)
        out = fine(coef, pair, NT)
        near = out[:, :128] + rest
        far = out[:, 128:]
        part = slice(CHUNK * k, CHUNK * (k + 1))
        free[part] = near[:64] + near[64:]
        along[part] = far[:64] + far[64:]
        pair = fine(pair, step) + jnp.concatenate([add, jnp.zeros((128, 128), F32)], axis=0)
    far = (pair[128:192] + pair[192:]).astype(BF16)
    near = (pair[:64] + pair[64:128]).astype(BF16)
    for i in range(16):
        state[i, 0] = far
        state[i, 1] = near


def recur(*args):
    wide = jax.ShapeDtypeStruct((ROWS, 128), F32)
    outs = [wide, wide, wide, jax.ShapeDtypeStruct((16, 2, 64, 128), BF16)]
    specs = [VMEM] * 14
    return call(recur_body, outs, args, 8 << 30, specs=specs, limit=RECUR_LIMIT)


def attend_body(q, own, peer, w, glat, gain, table, att, logs, acc, top):
    sp = lax.axis_index("sp")
    ones = jnp.where(iota((NOPE, ROWS), 0) == 0, 1.0, 0.0).astype(BF16)

    def keys(j):
        lat = jnp.concatenate(
            [own[:, j, 0:32, :].reshape(128, ROWS), peer[:, j, 0:32, :].reshape(128, ROWS)], axis=0
        ).astype(F32)
        rope = (own[:, j, 32:40, :].astype(F32) + peer[:, j, 32:40, :].astype(F32)).reshape(
            ROPE, ROWS
        )
        lat = lat * lax.rsqrt(jnp.mean(lat * lat, axis=0, keepdims=True) + EPS) * glat[:, 0:1]
        kv = dot(w[...], lat.astype(BF16)).astype(BF16)
        rope_sum = jnp.sum(rope * rope, axis=0, keepdims=True)
        turn = table[j]
        cosine, sine = turn[:16], turn[16:]
        ra, rb = rope[:16] * gain[64:80, 0:1], rope[16:] * gain[80:96, 0:1]
        ra, rb = ra * cosine - rb * sine, rb * cosine + ra * sine
        ready, values = [], []
        for h in range(2):
            k = kv[64 * h : 64 * (h + 1)].astype(F32)
            scale = lax.rsqrt(
                (jnp.sum(k * k, axis=0, keepdims=True) + rope_sum) * np.float32(1 / QK) + EPS
            )
            ready.append(
                jnp.concatenate([k * scale * gain[0:64, 0:1], ra * scale, rb * scale], axis=0).astype(
                    BF16
                )
            )
            values.append(jnp.concatenate([kv[128 + 64 * h : 192 + 64 * h], ones], axis=0))
        return ready, values

    def block(places, first):
        made = [keys(j) for j in places]
        for h in range(2):
            ready = jnp.concatenate([m[0][h] for m in made], axis=1)
            v = jnp.concatenate([m[1][h] for m in made], axis=1)
            s = dot(q[h, :, 0:QK], ready)
            if first:
                s = jnp.where(iota((ROWS, ROWS), 1) <= iota((ROWS, ROWS), 0), s, -jnp.inf)
            peak = jnp.max(s, axis=1, keepdims=True)
            if first:
                top[h] = jnp.broadcast_to(peak, (ROWS, 128))
                acc[h] = dot(jnp.exp2(s - peak).astype(BF16), v, NT)
            else:
                old = top[h]
                new = jnp.maximum(old, peak)
                top[h] = new
                p = jnp.exp2(s - new[:, 0:1]).astype(BF16)
                acc[h] = acc[h] * jnp.exp2(old - new) + dot(p, v, NT)

    block([sp], True)

    def loop(i, carry):
        block([3 * i, 3 * i + 1, 3 * i + 2], False)
        return carry

    lax.fori_loop(0, sp // 3, loop, 0)

    @pl.when(lax.rem(sp, 3) == 1)
    def _():
        block([sp - 1], False)

    @pl.when(lax.rem(sp, 3) == 2)
    def _():
        block([sp - 2, sp - 1], False)

    parts = []
    rows = []
    for h in range(2):
        total = acc[h][:, 64:65]
        parts.append(acc[h][:, 0:64] / total)
        full = top[h] * np.float32(np.log(2.0)) + jnp.log(jnp.broadcast_to(total, (ROWS, 128)))
        rows.append(full.T[0:1])
    att[...] = jnp.concatenate(parts, axis=1).astype(BF16)
    logs[...] = jnp.concatenate(rows, axis=0)


def attend(*args):
    outs = [jax.ShapeDtypeStruct((ROWS, 128), BF16), jax.ShapeDtypeStruct((2, ROWS), F32)]
    scratch = [pltpu.VMEM((2, ROWS, 128), F32), pltpu.VMEM((2, ROWS, 128), F32)]
    return call(attend_body, outs, args, 8 << 30, scratch, [VMEM] * 7)


def merge_body(att, free, along, bonus, states, branch, o0, o1, o2, o3, keep, send, held, arrived):
    copies = [
        pltpu.make_async_copy(o.at[pl.ds(192, 256)], held.at[k], arrived.at[k])
        for k, o in enumerate((o0, o1, o2, o3))
    ]
    for copy in copies:
        copy.start()
    head = iota((128, 128), 0) // 64 == iota((128, 128), 1) // 64

    def spread(v):
        return jnp.where(head, jnp.concatenate([v, v], axis=0), jnp.zeros((), v.dtype))

    sp = lax.axis_index("sp")
    eye = jnp.where(iota((128, 128), 0) == iota((128, 128), 1), 1.0, 0.0).astype(BF16)
    below = jnp.zeros((128, 128), F32)
    entering = below
    groups = []
    for g in range(4):
        pair = None
        for r in range(4 * g, 4 * g + 4):
            move = jnp.where(r < sp, spread(states[r, 0]), eye)
            add = jnp.where(r < sp, spread(states[r, 1]).astype(F32), 0.0)
            if pair is None:
                pair = jnp.concatenate([add, move.astype(F32)], axis=0)
            else:
                pair = dot_wide(pair, move) + jnp.concatenate([add, below], axis=0)
        groups.append(pair)
    entering = groups[0][:128]
    for pair in groups[1:]:
        entering = fine(entering, pair[128:]) + pair[:128]
    read = free[...] + fine(along[...], entering, NT)
    mean = jnp.where(head, 1.0 / 64, 0.0).astype(BF16)
    read = read - dot_wide(read, mean)
    spread_of = dot_wide(read * read, mean)
    rec = read * lax.rsqrt(spread_of + GROUP_EPS) * branch[...] + bonus[...]
    both = jnp.concatenate([att[...].astype(F32), rec], axis=1).reshape(4, 2, 32, 256)
    core = lax.rem(lax.axis_index("tp"), 2)
    even, odd = both[:, 0].reshape(128, 256), both[:, 1].reshape(128, 256)
    kept = jnp.where(core == 0, even, odd).astype(BF16)
    sent = jnp.where(core == 0, odd, even).astype(BF16)
    for copy in copies:
        copy.wait()
    for k in range(4):
        send[:, columns(k)] = dot(sent, held[k]).astype(BF16)
    for k in range(4):
        keep[:, columns(k)] = dot(kept, held[k])


def merge(*args):
    outs = [jax.ShapeDtypeStruct((128, 2048), F32), jax.ShapeDtypeStruct((128, 2048), BF16)]
    scratch = [pltpu.VMEM((4, 256, 512), BF16), pltpu.SemaphoreType.DMA((4,))]
    return call(merge_body, outs, args, 4 << 30, scratch, [VMEM] * 6 + [HBM] * 4)


def exchanged(copies, axis, groups=None):
    return lax.all_to_all(copies, axis, 0, 0, axis_index_groups=groups, tiled=True)


def around(value):
    moves = [[(i, (i + by) % 4) for i in range(4)] for by in (1, 3, 2)]
    return [value] + [lax.ppermute(value, "fs", move) for move in moves]


def other_core(value):
    return lax.ppermute(value, "tp", [(i, i ^ 1) for i in range(8)])


def turn_table():
    half = ROPE // 2
    inverse = np.float32(10000.0) ** (-np.arange(half, dtype=np.float32) / np.float32(half))
    angle = np.arange(4096, dtype=np.float32)[:, None] * inverse.astype(np.float32)[None, :]
    both = np.concatenate([np.cos(angle), np.sin(angle)], axis=1).astype(np.float32)
    return both.reshape(16, ROWS, ROPE).transpose(0, 2, 1)


def shards(
    entering,
    entering_gain,
    wq,
    wc,
    wr,
    compact_gain,
    wk_up,
    wv_up,
    q_gain,
    k_gain,
    w_accept,
    w_key,
    w_value,
    fade1,
    fade2,
    fade_bias,
    fade_mult,
    fade_extra,
    adapt1,
    adapt2,
    adapt_bias,
    present,
    branch,
    wo_att,
    wo_rec,
):
    xs, small, big, late = prepare(
        entering[0],
        entering_gain.reshape(1, 2048),
        w_accept,
        w_key,
        w_value,
        wq.T,
        wc,
        wr.T,
        wo_att,
        wo_rec,
    )
    normed = exchanged(xs, "tp").reshape(ROWS, 2048)
    smalls = around(small)
    bigs = around(big)
    lates = around(late)

    table = jnp.asarray(turn_table())
    pay = latents(normed, *smalls)
    lat = exchanged(pay, "sp")

    free, along, bonus, state = recur(
        normed,
        *bigs,
        fade1,
        adapt1,
        fade2,
        fade_bias.reshape(1, 128),
        adapt2,
        adapt_bias.reshape(1, 128),
        fade_mult[0],
        fade_extra[0],
        present,
    )
    lat, state = lax.optimization_barrier((lat, state))
    states = exchanged(state, "sp")
    others = [lax.ppermute(lat, "tp", [(i, (i + by) % 8) for i in range(8)]) for by in (2, 6, 4)]
    lat_own = collect(lat, *others)
    lat_peer = other_core(lat_own)
    q, up, glat, key_gain = queries(
        normed,
        *lates,
        table,
        wk_up,
        wv_up,
        compact_gain.reshape(1, 256),
        k_gain.reshape(1, QK),
        q_gain.reshape(1, QK),
    )
    att, logs = attend(q, lat_own, lat_peer, up, glat, key_gain, table)
    keep, send = merge(att, free, along, bonus, states, branch.reshape(1, 128), *lates)
    pair = (keep + other_core(send).astype(F32)).astype(BF16)
    same_core = [[0, 2, 4, 6], [1, 3, 5, 7]]
    parts = exchanged(pair.reshape(4, 32, 2048), "tp", same_core)
    mixed = jnp.sum(parts.astype(F32), axis=0).astype(BF16)
    return mixed[None], logs[None]


def solution(mesh):
    placed = (
        P("fs", ("sp", "tp"), None),
        P(),
        P("fs", "tp"),
        P("fs", None),
        P("fs", None),
        P(),
        P(None, "tp"),
        P(None, "tp"),
        P(),
        P(),
        P("fs", "tp"),
        P("fs", "tp"),
        P("fs", "tp"),
        P(),
        P(None, "tp"),
        P("tp"),
        P("fs", "tp", "sp"),
        P("fs", "tp", "sp"),
        P(),
        P(None, "tp"),
        P("tp"),
        P("tp", None),
        P("tp"),
        P("tp", "fs"),
        P("tp", "fs"),
    )

    return jax.shard_map(
        shards,
        mesh=mesh,
        in_specs=placed,
        out_specs=(P("fs", ("sp", "tp"), None), P("fs", "tp", "sp")),
        check_vma=False,
    )
```

```python
import jax
import jax.numpy as jnp
import numpy as np
from jax import lax
from jax.experimental import pallas as pl
from jax.experimental.pallas import tpu as pltpu
from jax.sharding import PartitionSpec as P


F32 = jnp.float32
BF16 = jnp.bfloat16

ROWS = 256
NOPE = 64
ROPE = 32
QK = NOPE + ROPE
CHUNK = 64
RECUR_LIMIT = 63.9
CHUNKS = ROWS // CHUNK
EPS = 1e-6
GROUP_EPS = 0.00064
NN = (((1,), (0,)), ((), ()))
NT = (((1,), (1,)), ((), ()))
TN = (((0,), (0,)), ((), ()))

VMEM = pl.BlockSpec(memory_space=pltpu.VMEM)
HBM = pl.BlockSpec(memory_space=pltpu.HBM)


def dot(a, b, dims=NN):
    return lax.dot_general(a, b, dims, preferred_element_type=F32)


def halves(a):
    high = a.astype(BF16)
    return high, (a - high.astype(F32)).astype(BF16)


def fine(a, b, dims=NN):
    (i,), (j,) = dims[0]
    ah, al = halves(a)
    bh, bl = halves(b)
    wide = dot(jnp.concatenate([ah, al], axis=i), jnp.concatenate([bh, bh], axis=j), dims)
    return wide + dot(ah, bl, dims)


def dot_wide(a, b):
    high, low = halves(a)
    return dot(jnp.concatenate([high, low], axis=1), jnp.concatenate([b, b], axis=0))


def iota(shape, dim):
    return lax.broadcasted_iota(jnp.int32, shape, dim)


def call(body, outs, args, flops, scratch=(), specs=None, limit=24):
    return pl.pallas_call(
        body,
        out_shape=outs,
        in_specs=specs or [VMEM] * len(args),
        out_specs=jax.tree.map(lambda _: VMEM, outs),
        scratch_shapes=scratch,
        compiler_params=pltpu.CompilerParams(vmem_limit_bytes=int(limit * (1 << 20))),
        cost_estimate=pl.CostEstimate(flops=flops, bytes_accessed=4 << 20, transcendentals=0),
    )(*args)


def turned(n, table):
    half = ROPE // 2
    a, b = n[NOPE : NOPE + half], n[NOPE + half :]
    cosine, sine = table[:half], table[half:]
    return a * cosine - b * sine, b * cosine + a * sine


def prepare_body(
    x_in, gain_in, wa_in, wk_in, wv_in, wq_in, wc_in, wr_in, oa_in, or_in,
    xs, small, big, late, x, gain, wa, wk, wv, wq, wc, wr, oa, orr, turned_wc, arrived,
):
    pairs = [
        (x_in, x), (gain_in, gain), (wc_in, wc), (wr_in, wr), (wa_in, wa), (wk_in, wk),
        (wv_in, wv), (wq_in, wq), (oa_in, oa), (or_in, orr),
    ]
    copies = [pltpu.make_async_copy(a, b, arrived.at[i]) for i, (a, b) in enumerate(pairs)]
    for copy in copies:
        copy.start()
    copies[0].wait()
    copies[1].wait()
    v = x[...].astype(F32)
    v = v * lax.rsqrt(jnp.mean(v * v, axis=-1, keepdims=True) + EPS) * gain[...]
    v = v.astype(BF16)
    for i in range(8):
        xs[i] = v
    copies[2].wait()
    copies[3].wait()
    turned_wc[...] = wc[...].astype(F32).T
    start = pl.multiple_of(lax.axis_index("tp") * 32, 32)
    small[0:32] = turned_wc[pl.ds(start, 32), :].astype(BF16)
    small[32:64] = wr[...]
    for copy in copies[4:]:
        copy.wait()
    big[:, 0:128] = wa[...]
    big[:, 128:256] = wk[...]
    big[:, 256:384] = wv[...]
    late[0:192] = wq[...]
    late[192:320] = oa[...]
    late[320:448] = orr[...]


def prepare(*args):
    outs = [
        jax.ShapeDtypeStruct((8, 32, 2048), BF16),
        jax.ShapeDtypeStruct((64, 512), BF16),
        jax.ShapeDtypeStruct((512, 384), BF16),
        jax.ShapeDtypeStruct((448, 512), BF16),
    ]
    scratch = [pltpu.VMEM(a.shape, a.dtype) for a in args]
    scratch += [pltpu.VMEM((256, 512), F32), pltpu.SemaphoreType.DMA((10,))]
    return call(prepare_body, outs, args, 1 << 29, scratch, [HBM] * 10, 63.9)


def collect_body(own, left, right, far, out):
    chip = lax.axis_index("tp") // 2
    for by, part in ((0, own), (3, left), (1, right), (2, far)):
        out[lax.rem(chip + by, 4)] = part[...]


def collect(*parts):
    outs = jax.ShapeDtypeStruct((4, *parts[0].shape), BF16)
    return call(collect_body, outs, parts, 1 << 29)


def columns(k):
    shard = lax.rem(lax.axis_index("fs") + (0, 3, 1, 2)[k], 4)
    return pl.ds(pl.multiple_of(shard * 512, 512), 512)


def latents_body(x, w0, w1, w2, w3, pay):
    t = jnp.zeros((64, ROWS), F32)
    for k, w in enumerate((w0, w1, w2, w3)):
        t += dot(w[...], x[:, columns(k)], NT)
    tp = lax.axis_index("tp")
    group = jnp.zeros((8, ROWS), F32)
    for g in range(4):
        group += jnp.where(tp // 2 == g, t[32 + 8 * g : 40 + 8 * g], 0.0)
    group = jnp.where(iota((8, ROWS), 0) // 4 == lax.rem(tp, 2), group, 0.0)
    both = jnp.concatenate([t[0:32], group], axis=0).astype(BF16)
    for i in range(16):
        pay[i] = both


def latents(*args):
    outs = jax.ShapeDtypeStruct((16, 40, ROWS), BF16)
    return call(latents_body, outs, args, 1 << 29, limit=40)


def queries_body(
    x, w0, w1, w2, w3, table, wk_up, wv_up, compact_gain, kg, qg, q, up, glat, key_gain
):
    core = lax.rem(lax.axis_index("tp"), 2)

    def reordered(v):
        v = v.reshape(4, 2, 32, v.shape[-1])
        even, odd = v[:, 0].reshape(128, -1), v[:, 1].reshape(128, -1)
        first, second = jnp.where(core == 0, even, odd), jnp.where(core == 0, odd, even)
        return jnp.concatenate([first, second], axis=0)

    def column(source):
        wide = jnp.concatenate([source[...], jnp.zeros((1, 128 - QK), F32)], axis=1)
        return jnp.broadcast_to(wide, (128, 128)).T[0:QK]

    t = jnp.zeros((192, ROWS), F32)
    for k, w in enumerate((w0, w1, w2, w3)):
        t += dot(w[0:192], x[:, columns(k)], NT)
    t = t.astype(BF16).astype(F32)
    factor = np.float32(QK**-0.5 * np.log2(np.e))
    turn = table[lax.axis_index("sp")]
    gain = column(qg)[:, 0:1]
    for h in range(2):
        v = t[QK * h : QK * (h + 1)]
        n = v * (lax.rsqrt(jnp.mean(v * v, axis=0, keepdims=True) + EPS) * factor) * gain
        a, b = turned(n, turn)
        ready = jnp.concatenate([n[:NOPE], a, b, jnp.zeros((128 - QK, ROWS), F32)], axis=0)
        q[h] = ready.T.astype(BF16)
    both = jnp.concatenate([wk_up[...], wv_up[...]], axis=1).astype(F32)
    up[...] = reordered(both).T.astype(BF16)
    glat[...] = reordered(jnp.broadcast_to(compact_gain[...], (128, 256)).T)
    key_gain[...] = column(kg)


def queries(*args):
    outs = [
        jax.ShapeDtypeStruct((2, ROWS, 128), BF16),
        jax.ShapeDtypeStruct((256, 256), BF16),
        jax.ShapeDtypeStruct((256, 128), F32),
        jax.ShapeDtypeStruct((QK, 128), F32),
    ]
    return call(queries_body, outs, args, 1 << 29)


def recur_body(
    x, w0, w1, w2, w3, fd, fa, wd, bd, wa, ba, mult, extra, present,
    free, along, bonus, state,
):
    lane = iota((1, 128), 1)
    y = jnp.zeros((ROWS, 384), F32)
    for k, w in enumerate((w0, w1, w2, w3)):
        y += dot(x[:, columns(k)], w[...])
    y = y.astype(BF16).astype(F32)
    dlow = jnp.tanh(dot(x[...], fd[...]).astype(BF16).astype(F32)).astype(BF16)
    rlow = dot(x[...], fa[...]).astype(BF16)
    recept, key, value = (y[:, 128 * i : 128 * (i + 1)] for i in range(3))
    speed = jax.nn.sigmoid(bd[...] + dot(dlow, wd[...])) * np.float32(np.exp(-0.5))
    added = jnp.where(iota((128, ROWS), 0) < 64, extra[0:1], extra[1:2]).T
    ld = added - speed * jnp.where(lane < 64, mult[0:1, 0:1], mult[1:2, 0:1])
    here = jnp.concatenate([present[0:1], present[1:2]], axis=1)
    learn = jax.nn.sigmoid(ba[...] + dot(rlow, wa[...]))
    same = (iota((128, 128), 0) // 64 == iota((128, 128), 1) // 64).astype(BF16)
    unit = key * lax.rsqrt(dot_wide(key * key, same) + EPS)
    bonus[...] = dot_wide(recept * key * here, same) * value
    r, c = iota((ROWS, ROWS), 0), iota((ROWS, ROWS), 1)
    block = r // CHUNK == c // CHUNK
    sums = jnp.concatenate(
        [
            jnp.where(block & (c <= r), 1.0, 0.0),
            jnp.where(block & (lax.rem(c, CHUNK) < CHUNK // 2), 1.0, 0.0),
            jnp.where(block, 1.0, 0.0),
        ],
        axis=0,
    )
    sums = sums.astype(BF16)
    high, low = halves(ld)
    last = (ld - high.astype(F32) - low.astype(F32)).astype(BF16)
    sums = dot(
        jnp.concatenate([sums, sums, sums], axis=1), jnp.concatenate([high, low, last], axis=0)
    )
    cum, mid, end = sums[:ROWS], sums[ROWS : 2 * ROWS], sums[2 * ROWS :]
    prev = cum - ld
    toward = -unit
    remove = unit * learn
    grow, shrink = jnp.exp(cum - mid), jnp.exp(mid - cum)
    left1, left2 = toward * jnp.exp(prev - mid), recept * grow
    right1, right2 = remove * shrink, key * shrink
    start1, start2 = toward * jnp.exp(prev), recept * jnp.exp(cum)
    tail = jnp.exp(end - cum)
    tail1, tail2 = remove * tail, key * tail
    whole = jnp.exp(end)
    m0 = iota((CHUNK, 128), 1) < 64

    def stacked(v, k):
        v = v[CHUNK * k : CHUNK * (k + 1)]
        return jnp.concatenate([jnp.where(m0, v, 0.0), jnp.where(m0, 0.0, v)], axis=0)

    rr, cc = iota((128, 128), 0), iota((128, 128), 1)
    head = rr // 64 == cc // 64
    eye = jnp.where(rr == cc, 1.0, 0.0)
    in8, in16, in32 = (rr // n == cc // n for n in (8, 16, 32))
    strict, upto = head & (rr > cc), head & (rr >= cc)

    def square(top, mask):
        both = jnp.concatenate([top, top], axis=1)
        return jnp.where(mask, both, 0.0)

    stage = []
    for k in range(CHUNKS):
        rows = jnp.concatenate([stacked(left1, k), stacked(left2, k)], axis=0)
        part = slice(CHUNK * k, CHUNK * (k + 1))
        cols = jnp.concatenate([right1[part], right2[part]], axis=0)
        g = fine(rows, cols, NT)
        a = square(g[:128, :64], strict)
        kb = square(g[:128, 64:], strict)
        ru = square(g[128:, :64], upto)
        ku = square(g[128:, 64:], upto)
        stage.append([a, kb, ru, ku])
    inverse = []
    for k in range(CHUNKS):
        a = stage[k][0]
        small = jnp.where(in8, a, 0.0)
        power = small
        t = eye + small
        for _ in range(2):
            power = fine(power, power)
            t = t + fine(t, power)
        for wider, narrower in ((in16, in8), (in32, in16), (None, in32)):
            rest = jnp.where(narrower, 0.0, a)
            rest = rest if wider is None else jnp.where(wider, rest, 0.0)
            t = t + fine(fine(t, rest), t)
        inverse.append(t)
    pair = jnp.concatenate([jnp.zeros((128, 128), F32), eye], axis=0)
    for k in range(CHUNKS):
        _, kb, ru, ku = stage[k]
        v = stacked(value, k)
        xy = fine(inverse[k], jnp.concatenate([stacked(start1, k), fine(kb, v)], axis=1))
        read = fine(ru, xy)
        coef = stacked(start2, k) + read[:, :128]
        rest = read[:, 128:] + fine(ku, v)
        t1, t2 = stacked(tail1, k), stacked(tail2, k)
        moved = fine(xy, t1, TN)
        decay = whole[CHUNK * k : CHUNK * k + 1]
        step = moved[:128] + jnp.where(rr == cc, decay, 0.0)
        add = moved[128:] + fine(v, t2, TN)
        out = fine(coef, pair, NT)
        near = out[:, :128] + rest
        far = out[:, 128:]
        part = slice(CHUNK * k, CHUNK * (k + 1))
        free[part] = near[:64] + near[64:]
        along[part] = far[:64] + far[64:]
        pair = fine(pair, step) + jnp.concatenate([add, jnp.zeros((128, 128), F32)], axis=0)
    far = (pair[128:192] + pair[192:]).astype(BF16)
    near = (pair[:64] + pair[64:128]).astype(BF16)
    for i in range(16):
        state[i, 0] = far
        state[i, 1] = near


def recur(*args):
    wide = jax.ShapeDtypeStruct((ROWS, 128), F32)
    outs = [wide, wide, wide, jax.ShapeDtypeStruct((16, 2, 64, 128), BF16)]
    specs = [VMEM] * 14
    return call(recur_body, outs, args, 8 << 30, specs=specs, limit=RECUR_LIMIT)


def attend_body(q, own, peer, w, glat, gain, table, att, logs, acc, top):
    sp = lax.axis_index("sp")
    ones = jnp.where(iota((NOPE, ROWS), 0) == 0, 1.0, 0.0).astype(BF16)

    def twice(v):
        return jnp.concatenate([v, v], axis=1)

    def keys(j):
        lat = jnp.concatenate(
            [own[:, j, 0:32, :].reshape(128, ROWS), peer[:, j, 0:32, :].reshape(128, ROWS)], axis=0
        ).astype(F32)
        rope = (own[:, j, 32:40, :].astype(F32) + peer[:, j, 32:40, :].astype(F32)).reshape(
            ROPE, ROWS
        )
        lat = lat * lax.rsqrt(jnp.mean(lat * lat, axis=0, keepdims=True) + EPS) * twice(glat[...])
        kv = dot(w[...], lat.astype(BF16)).astype(BF16)
        rope_sum = jnp.sum(rope * rope, axis=0, keepdims=True)
        turn = table[j]
        cosine, sine = turn[:16], turn[16:]
        ra, rb = rope[:16] * twice(gain[64:80]), rope[16:] * twice(gain[80:96])
        ra, rb = ra * cosine - rb * sine, rb * cosine + ra * sine
        ready, values = [], []
        for h in range(2):
            k = kv[64 * h : 64 * (h + 1)].astype(F32)
            scale = lax.rsqrt(
                (jnp.sum(k * k, axis=0, keepdims=True) + rope_sum) * np.float32(1 / QK) + EPS
            )
            ready.append(
                jnp.concatenate([k * scale * twice(gain[0:64]), ra * scale, rb * scale], axis=0).astype(
                    BF16
                )
            )
            values.append(jnp.concatenate([kv[128 + 64 * h : 192 + 64 * h], ones], axis=0))
        return ready, values

    def block(places, first):
        made = [keys(j) for j in places]
        for h in range(2):
            ready = jnp.concatenate([m[0][h] for m in made], axis=1)
            v = jnp.concatenate([m[1][h] for m in made], axis=1)
            s = dot(q[h, :, 0:QK], ready)
            if first:
                s = jnp.where(iota((ROWS, ROWS), 1) <= iota((ROWS, ROWS), 0), s, -jnp.inf)
            peak = jnp.max(s, axis=1, keepdims=True)
            if first:
                top[h] = jnp.broadcast_to(peak, (ROWS, 128))
                acc[h] = dot(jnp.exp2(s - peak).astype(BF16), v, NT)
            else:
                old = top[h]
                new = jnp.maximum(old, peak)
                top[h] = new
                p = jnp.exp2(s - jnp.concatenate([new] * (2 * len(places)), axis=1)).astype(BF16)
                acc[h] = acc[h] * jnp.exp2(old - new) + dot(p, v, NT)

    block([sp], True)

    def loop(i, carry):
        block([5 * i + n for n in range(5)], False)
        return carry

    lax.fori_loop(0, sp // 5, loop, 0)
    left = lax.rem(sp, 5)
    for count in range(1, 5):

        @pl.when(left == count)
        def _():
            block([sp - count + n for n in range(count)], False)

    parts = []
    rows = []
    for h in range(2):
        total = acc[h][:, 64:65]
        parts.append(acc[h][:, 0:64] / total)
        full = top[h] * np.float32(np.log(2.0)) + jnp.log(jnp.broadcast_to(total, (ROWS, 128)))
        rows.append(full.T[0:1])
    att[...] = jnp.concatenate(parts, axis=1).astype(BF16)
    logs[...] = jnp.concatenate(rows, axis=0)


def attend(*args):
    outs = [jax.ShapeDtypeStruct((ROWS, 128), BF16), jax.ShapeDtypeStruct((2, ROWS), F32)]
    scratch = [pltpu.VMEM((2, ROWS, 128), F32), pltpu.VMEM((2, ROWS, 128), F32)]
    return call(attend_body, outs, args, 8 << 30, scratch, [VMEM] * 7)


def merge_body(att, free, along, bonus, states, branch, o0, o1, o2, o3, keep, send, held, arrived):
    copies = [
        pltpu.make_async_copy(o.at[pl.ds(192, 256)], held.at[k], arrived.at[k])
        for k, o in enumerate((o0, o1, o2, o3))
    ]
    for copy in copies:
        copy.start()
    head = iota((128, 128), 0) // 64 == iota((128, 128), 1) // 64

    def spread(v):
        return jnp.where(head, jnp.concatenate([v, v], axis=0), jnp.zeros((), v.dtype))

    sp = lax.axis_index("sp")
    eye = jnp.where(iota((128, 128), 0) == iota((128, 128), 1), 1.0, 0.0).astype(BF16)
    below = jnp.zeros((128, 128), F32)
    entering = below
    groups = []
    for g in range(4):
        pair = None
        for r in range(4 * g, 4 * g + 4):
            move = jnp.where(r < sp, spread(states[r, 0]), eye)
            add = jnp.where(r < sp, spread(states[r, 1]).astype(F32), 0.0)
            if pair is None:
                pair = jnp.concatenate([add, move.astype(F32)], axis=0)
            else:
                pair = dot_wide(pair, move) + jnp.concatenate([add, below], axis=0)
        groups.append(pair)
    entering = groups[0][:128]
    for pair in groups[1:]:
        entering = fine(entering, pair[128:]) + pair[:128]
    read = free[...] + fine(along[...], entering, NT)
    mean = jnp.where(head, 1.0 / 64, 0.0).astype(BF16)
    read = read - dot_wide(read, mean)
    spread_of = dot_wide(read * read, mean)
    rec = read * lax.rsqrt(spread_of + GROUP_EPS) * branch[...] + bonus[...]
    both = jnp.concatenate([att[...].astype(F32), rec], axis=1).reshape(4, 2, 32, 256)
    core = lax.rem(lax.axis_index("tp"), 2)
    even, odd = both[:, 0].reshape(128, 256), both[:, 1].reshape(128, 256)
    kept = jnp.where(core == 0, even, odd).astype(BF16)
    sent = jnp.where(core == 0, odd, even).astype(BF16)
    for copy in copies:
        copy.wait()
    for k in range(4):
        send[:, columns(k)] = dot(sent, held[k]).astype(BF16)
    for k in range(4):
        keep[:, columns(k)] = dot(kept, held[k])


def merge(*args):
    outs = [jax.ShapeDtypeStruct((128, 2048), F32), jax.ShapeDtypeStruct((128, 2048), BF16)]
    scratch = [pltpu.VMEM((4, 256, 512), BF16), pltpu.SemaphoreType.DMA((4,))]
    return call(merge_body, outs, args, 4 << 30, scratch, [VMEM] * 6 + [HBM] * 4)


def exchanged(copies, axis, groups=None):
    return lax.all_to_all(copies, axis, 0, 0, axis_index_groups=groups, tiled=True)


def around(value):
    moves = [[(i, (i + by) % 4) for i in range(4)] for by in (1, 3, 2)]
    return [value] + [lax.ppermute(value, "fs", move) for move in moves]


def other_core(value):
    return lax.ppermute(value, "tp", [(i, i ^ 1) for i in range(8)])


def turn_table():
    half = ROPE // 2
    inverse = np.float32(10000.0) ** (-np.arange(half, dtype=np.float32) / np.float32(half))
    angle = np.arange(4096, dtype=np.float32)[:, None] * inverse.astype(np.float32)[None, :]
    both = np.concatenate([np.cos(angle), np.sin(angle)], axis=1).astype(np.float32)
    return both.reshape(16, ROWS, ROPE).transpose(0, 2, 1)


def shards(
    entering,
    entering_gain,
    wq,
    wc,
    wr,
    compact_gain,
    wk_up,
    wv_up,
    q_gain,
    k_gain,
    w_accept,
    w_key,
    w_value,
    fade1,
    fade2,
    fade_bias,
    fade_mult,
    fade_extra,
    adapt1,
    adapt2,
    adapt_bias,
    present,
    branch,
    wo_att,
    wo_rec,
):
    xs, small, big, late = prepare(
        entering[0],
        entering_gain.reshape(1, 2048),
        w_accept,
        w_key,
        w_value,
        wq.T,
        wc,
        wr.T,
        wo_att,
        wo_rec,
    )
    normed = exchanged(xs, "tp").reshape(ROWS, 2048)
    smalls = around(small)
    bigs = around(big)
    lates = around(late)

    table = jnp.asarray(turn_table())
    pay = latents(normed, *smalls)
    lat = exchanged(pay, "sp")

    free, along, bonus, state = recur(
        normed,
        *bigs,
        fade1,
        adapt1,
        fade2,
        fade_bias.reshape(1, 128),
        adapt2,
        adapt_bias.reshape(1, 128),
        fade_mult[0],
        fade_extra[0],
        present,
    )
    lat, state = lax.optimization_barrier((lat, state))
    states = exchanged(state, "sp")
    others = [lax.ppermute(lat, "tp", [(i, (i + by) % 8) for i in range(8)]) for by in (2, 6, 4)]
    lat_own = collect(lat, *others)
    lat_peer = other_core(lat_own)
    q, up, glat, key_gain = queries(
        normed,
        *lates,
        table,
        wk_up,
        wv_up,
        compact_gain.reshape(1, 256),
        k_gain.reshape(1, QK),
        q_gain.reshape(1, QK),
    )
    att, logs = attend(q, lat_own, lat_peer, up, glat, key_gain, table)
    keep, send = merge(att, free, along, bonus, states, branch.reshape(1, 128), *lates)
    pair = (keep + other_core(send).astype(F32)).astype(BF16)
    same_core = [[0, 2, 4, 6], [1, 3, 5, 7]]
    parts = exchanged(pair.reshape(4, 32, 2048), "tp", same_core)
    mixed = jnp.sum(parts.astype(F32), axis=0).astype(BF16)
    return mixed[None], logs[None]


def solution(mesh):
    placed = (
        P("fs", ("sp", "tp"), None),
        P(),
        P("fs", "tp"),
        P("fs", None),
        P("fs", None),
        P(),
        P(None, "tp"),
        P(None, "tp"),
        P(),
        P(),
        P("fs", "tp"),
        P("fs", "tp"),
        P("fs", "tp"),
        P(),
        P(None, "tp"),
        P("tp"),
        P("fs", "tp", "sp"),
        P("fs", "tp", "sp"),
        P(),
        P(None, "tp"),
        P("tp"),
        P("tp", None),
        P("tp"),
        P("tp", "fs"),
        P("tp", "fs"),
    )

    return jax.shard_map(
        shards,
        mesh=mesh,
        in_specs=placed,
        out_specs=(P("fs", ("sp", "tp"), None), P("fs", "tp", "sp")),
        check_vma=False,
    )
```

```python
import jax
import jax.numpy as jnp
import numpy as np
from jax import lax
from jax.experimental import pallas as pl
from jax.experimental.pallas import tpu as pltpu
from jax.sharding import PartitionSpec as P


F32 = jnp.float32
BF16 = jnp.bfloat16

ROWS = 256
NOPE = 64
ROPE = 32
QK = NOPE + ROPE
CHUNK = 64
RECUR_LIMIT = 63.9
CHUNKS = ROWS // CHUNK
EPS = 1e-6
GROUP_EPS = 0.00064
NN = (((1,), (0,)), ((), ()))
NT = (((1,), (1,)), ((), ()))
TN = (((0,), (0,)), ((), ()))

VMEM = pl.BlockSpec(memory_space=pltpu.VMEM)
HBM = pl.BlockSpec(memory_space=pltpu.HBM)


def dot(a, b, dims=NN):
    return lax.dot_general(a, b, dims, preferred_element_type=F32)


def halves(a):
    high = a.astype(BF16)
    return high, (a - high.astype(F32)).astype(BF16)


def fine(a, b, dims=NN):
    (i,), (j,) = dims[0]
    ah, al = halves(a)
    bh, bl = halves(b)
    wide = dot(jnp.concatenate([ah, al], axis=i), jnp.concatenate([bh, bh], axis=j), dims)
    return wide + dot(ah, bl, dims)


def dot_wide(a, b):
    high, low = halves(a)
    return dot(jnp.concatenate([high, low], axis=1), jnp.concatenate([b, b], axis=0))


def iota(shape, dim):
    return lax.broadcasted_iota(jnp.int32, shape, dim)


def call(body, outs, args, flops, scratch=(), specs=None, limit=24):
    return pl.pallas_call(
        body,
        out_shape=outs,
        in_specs=specs or [VMEM] * len(args),
        out_specs=jax.tree.map(lambda _: VMEM, outs),
        scratch_shapes=scratch,
        compiler_params=pltpu.CompilerParams(vmem_limit_bytes=int(limit * (1 << 20))),
        cost_estimate=pl.CostEstimate(flops=flops, bytes_accessed=4 << 20, transcendentals=0),
    )(*args)


def turned(n, table):
    half = ROPE // 2
    a, b = n[NOPE : NOPE + half], n[NOPE + half :]
    cosine, sine = table[:half], table[half:]
    return a * cosine - b * sine, b * cosine + a * sine


def prepare_body(
    x_in, gain_in, wa_in, wk_in, wv_in, wq_in, wc_in, wr_in, oa_in, or_in,
    xs, big, late, x, gain, wa, wk, wv, wq, wc, wr, oa, orr, turned_wc, arrived,
):
    pairs = [
        (x_in, x), (gain_in, gain), (wc_in, wc), (wr_in, wr), (wa_in, wa), (wk_in, wk),
        (wv_in, wv), (wq_in, wq), (oa_in, oa), (or_in, orr),
    ]
    copies = [pltpu.make_async_copy(a, b, arrived.at[i]) for i, (a, b) in enumerate(pairs)]
    for copy in copies:
        copy.start()
    copies[0].wait()
    copies[1].wait()
    v = x[...].astype(F32)
    v = v * lax.rsqrt(jnp.mean(v * v, axis=-1, keepdims=True) + EPS) * gain[...]
    v = v.astype(BF16)
    for i in range(8):
        xs[i] = v
    copies[2].wait()
    copies[3].wait()
    turned_wc[...] = wc[...].astype(F32).T
    start = pl.multiple_of(lax.axis_index("tp") * 32, 32)
    small = jnp.concatenate([turned_wc[pl.ds(start, 32), :], wr[...].astype(F32)], axis=0)
    big[512:576] = small[:, 0:384].astype(BF16)
    last = jnp.concatenate([small[:, 384:512], jnp.zeros((8, 128), F32)], axis=0)
    big[576:600] = jnp.concatenate([last[24 * i : 24 * i + 24] for i in range(3)], axis=1).astype(
        BF16
    )
    for copy in copies[4:]:
        copy.wait()
    big[0:512, 0:128] = wa[...]
    big[0:512, 128:256] = wk[...]
    big[0:512, 256:384] = wv[...]
    late[0:192] = wq[...]
    late[192:320] = oa[...]
    late[320:448] = orr[...]


def prepare(*args):
    outs = [
        jax.ShapeDtypeStruct((8, 32, 2048), BF16),
        jax.ShapeDtypeStruct((600, 384), BF16),
        jax.ShapeDtypeStruct((448, 512), BF16),
    ]
    scratch = [pltpu.VMEM(a.shape, a.dtype) for a in args]
    scratch += [pltpu.VMEM((256, 512), F32), pltpu.SemaphoreType.DMA((10,))]
    return call(prepare_body, outs, args, 1 << 29, scratch, [HBM] * 10, 63.9)


def collect_body(own, left, right, far, out):
    chip = lax.axis_index("tp") // 2
    for by, part in ((0, own), (3, left), (1, right), (2, far)):
        out[lax.rem(chip + by, 4)] = part[...]


def collect(*parts):
    outs = jax.ShapeDtypeStruct((4, *parts[0].shape), BF16)
    return call(collect_body, outs, parts, 1 << 29)


def columns(k):
    shard = lax.rem(lax.axis_index("fs") + (0, 3, 1, 2)[k], 4)
    return pl.ds(pl.multiple_of(shard * 512, 512), 512)


def latents_body(x, w0, w1, w2, w3, pay, held, arrived):
    copies = [
        pltpu.make_async_copy(w.at[pl.ds(512, 88)], held.at[k], arrived.at[k])
        for k, w in enumerate((w0, w1, w2, w3))
    ]
    for copy in copies:
        copy.start()
    for copy in copies:
        copy.wait()
    t = jnp.zeros((64, ROWS), F32)
    for k in range(4):
        w = held[k].astype(F32)
        last = jnp.concatenate([w[64:88, 128 * i : 128 * i + 128] for i in range(3)], axis=0)
        w = jnp.concatenate([w[0:64], last[0:64]], axis=1).astype(BF16)
        t += dot(w, x[:, columns(k)], NT)
    tp = lax.axis_index("tp")
    group = jnp.zeros((8, ROWS), F32)
    for g in range(4):
        group += jnp.where(tp // 2 == g, t[32 + 8 * g : 40 + 8 * g], 0.0)
    group = jnp.where(iota((8, ROWS), 0) // 4 == lax.rem(tp, 2), group, 0.0)
    both = jnp.concatenate([t[0:32], group], axis=0).astype(BF16)
    for i in range(16):
        pay[i] = both


def latents(*args):
    outs = jax.ShapeDtypeStruct((16, 40, ROWS), BF16)
    scratch = [pltpu.VMEM((4, 88, 384), BF16), pltpu.SemaphoreType.DMA((4,))]
    return call(latents_body, outs, args, 1 << 29, scratch, [VMEM] + [HBM] * 4, 40)


def queries_body(
    x, w0, w1, w2, w3, table, wk_up, wv_up, compact_gain, kg, qg, q, up, glat, key_gain
):
    core = lax.rem(lax.axis_index("tp"), 2)

    def reordered(v):
        v = v.reshape(4, 2, 32, v.shape[-1])
        even, odd = v[:, 0].reshape(128, -1), v[:, 1].reshape(128, -1)
        first, second = jnp.where(core == 0, even, odd), jnp.where(core == 0, odd, even)
        return jnp.concatenate([first, second], axis=0)

    def column(source):
        wide = jnp.concatenate([source[...], jnp.zeros((1, 128 - QK), F32)], axis=1)
        return jnp.broadcast_to(wide, (128, 128)).T[0:QK]

    t = jnp.zeros((192, ROWS), F32)
    for k, w in enumerate((w0, w1, w2, w3)):
        t += dot(w[0:192], x[:, columns(k)], NT)
    t = t.astype(BF16).astype(F32)
    factor = np.float32(QK**-0.5 * np.log2(np.e))
    turn = table[lax.axis_index("sp")]
    gain = column(qg)[:, 0:1]
    for h in range(2):
        v = t[QK * h : QK * (h + 1)]
        n = v * (lax.rsqrt(jnp.mean(v * v, axis=0, keepdims=True) + EPS) * factor) * gain
        a, b = turned(n, turn)
        ready = jnp.concatenate([n[:NOPE], a, b, jnp.zeros((128 - QK, ROWS), F32)], axis=0)
        q[h] = ready.T.astype(BF16)
    both = jnp.concatenate([wk_up[...], wv_up[...]], axis=1).astype(F32)
    up[...] = reordered(both).T.astype(BF16)
    glat[...] = reordered(jnp.broadcast_to(compact_gain[...], (128, 256)).T)
    key_gain[...] = column(kg)


def queries(*args):
    outs = [
        jax.ShapeDtypeStruct((2, ROWS, 128), BF16),
        jax.ShapeDtypeStruct((256, 256), BF16),
        jax.ShapeDtypeStruct((256, 128), F32),
        jax.ShapeDtypeStruct((QK, 128), F32),
    ]
    return call(queries_body, outs, args, 1 << 29)


def recur_body(
    x, w0, w1, w2, w3, fd, fa, wd, bd, wa, ba, mult, extra, present,
    free, along, bonus, state,
):
    lane = iota((1, 128), 1)
    y = jnp.zeros((ROWS, 384), F32)
    for k, w in enumerate((w0, w1, w2, w3)):
        y += dot(x[:, columns(k)], w[0:512])
    y = y.astype(BF16).astype(F32)
    dlow = jnp.tanh(dot(x[...], fd[...]).astype(BF16).astype(F32)).astype(BF16)
    rlow = dot(x[...], fa[...]).astype(BF16)
    recept, key, value = (y[:, 128 * i : 128 * (i + 1)] for i in range(3))
    speed = jax.nn.sigmoid(bd[...] + dot(dlow, wd[...])) * np.float32(np.exp(-0.5))
    added = jnp.where(iota((128, ROWS), 0) < 64, extra[0:1], extra[1:2]).T
    ld = added - speed * jnp.where(lane < 64, mult[0:1, 0:1], mult[1:2, 0:1])
    here = jnp.concatenate([present[0:1], present[1:2]], axis=1)
    learn = jax.nn.sigmoid(ba[...] + dot(rlow, wa[...]))
    same = (iota((128, 128), 0) // 64 == iota((128, 128), 1) // 64).astype(BF16)
    unit = key * lax.rsqrt(dot_wide(key * key, same) + EPS)
    bonus[...] = dot_wide(recept * key * here, same) * value
    r, c = iota((ROWS, ROWS), 0), iota((ROWS, ROWS), 1)
    block = r // CHUNK == c // CHUNK
    sums = jnp.concatenate(
        [
            jnp.where(block & (c <= r), 1.0, 0.0),
            jnp.where(block & (lax.rem(c, CHUNK) < CHUNK // 2), 1.0, 0.0),
            jnp.where(block, 1.0, 0.0),
        ],
        axis=0,
    )
    sums = sums.astype(BF16)
    high, low = halves(ld)
    last = (ld - high.astype(F32) - low.astype(F32)).astype(BF16)
    sums = dot(
        jnp.concatenate([sums, sums, sums], axis=1), jnp.concatenate([high, low, last], axis=0)
    )
    cum, mid, end = sums[:ROWS], sums[ROWS : 2 * ROWS], sums[2 * ROWS :]
    prev = cum - ld
    toward = -unit
    remove = unit * learn
    grow, shrink = jnp.exp(cum - mid), jnp.exp(mid - cum)
    left1, left2 = toward * jnp.exp(prev - mid), recept * grow
    right1, right2 = remove * shrink, key * shrink
    start1, start2 = toward * jnp.exp(prev), recept * jnp.exp(cum)
    tail = jnp.exp(end - cum)
    tail1, tail2 = remove * tail, key * tail
    whole = jnp.exp(end)
    m0 = iota((CHUNK, 128), 1) < 64

    def stacked(v, k):
        v = v[CHUNK * k : CHUNK * (k + 1)]
        return jnp.concatenate([jnp.where(m0, v, 0.0), jnp.where(m0, 0.0, v)], axis=0)

    rr, cc = iota((128, 128), 0), iota((128, 128), 1)
    head = rr // 64 == cc // 64
    eye = jnp.where(rr == cc, 1.0, 0.0)
    in8, in16, in32 = (rr // n == cc // n for n in (8, 16, 32))
    strict, upto = head & (rr > cc), head & (rr >= cc)

    def square(top, mask):
        both = jnp.concatenate([top, top], axis=1)
        return jnp.where(mask, both, 0.0)

    stage = []
    for k in range(CHUNKS):
        rows = jnp.concatenate([stacked(left1, k), stacked(left2, k)], axis=0)
        part = slice(CHUNK * k, CHUNK * (k + 1))
        cols = jnp.concatenate([right1[part], right2[part]], axis=0)
        g = fine(rows, cols, NT)
        a = square(g[:128, :64], strict)
        kb = square(g[:128, 64:], strict)
        ru = square(g[128:, :64], upto)
        ku = square(g[128:, 64:], upto)
        stage.append([a, kb, ru, ku])
    inverse = []
    for k in range(CHUNKS):
        a = stage[k][0]
        small = jnp.where(in8, a, 0.0)
        power = small
        t = eye + small
        for _ in range(2):
            power = fine(power, power)
            t = t + fine(t, power)
        for wider, narrower in ((in16, in8), (in32, in16), (None, in32)):
            rest = jnp.where(narrower, 0.0, a)
            rest = rest if wider is None else jnp.where(wider, rest, 0.0)
            t = t + fine(fine(t, rest), t)
        inverse.append(t)
    pair = jnp.concatenate([jnp.zeros((128, 128), F32), eye], axis=0)
    for k in range(CHUNKS):
        _, kb, ru, ku = stage[k]
        v = stacked(value, k)
        xy = fine(inverse[k], jnp.concatenate([stacked(start1, k), fine(kb, v)], axis=1))
        read = fine(ru, xy)
        coef = stacked(start2, k) + read[:, :128]
        rest = read[:, 128:] + fine(ku, v)
        t1, t2 = stacked(tail1, k), stacked(tail2, k)
        moved = fine(xy, t1, TN)
        decay = whole[CHUNK * k : CHUNK * k + 1]
        step = moved[:128] + jnp.where(rr == cc, decay, 0.0)
        add = moved[128:] + fine(v, t2, TN)
        out = fine(coef, pair, NT)
        near = out[:, :128] + rest
        far = out[:, 128:]
        part = slice(CHUNK * k, CHUNK * (k + 1))
        free[part] = near[:64] + near[64:]
        along[part] = far[:64] + far[64:]
        pair = fine(pair, step) + jnp.concatenate([add, jnp.zeros((128, 128), F32)], axis=0)
    far = (pair[128:192] + pair[192:]).astype(BF16)
    near = (pair[:64] + pair[64:128]).astype(BF16)
    for i in range(16):
        state[i, 0] = far
        state[i, 1] = near


def recur(*args):
    wide = jax.ShapeDtypeStruct((ROWS, 128), F32)
    outs = [wide, wide, wide, jax.ShapeDtypeStruct((16, 2, 64, 128), BF16)]
    specs = [VMEM] * 14
    return call(recur_body, outs, args, 8 << 30, specs=specs, limit=RECUR_LIMIT)


def attend_body(q, own, peer, w, glat, gain, table, att, logs, acc, top):
    sp = lax.axis_index("sp")
    ones = jnp.where(iota((NOPE, ROWS), 0) == 0, 1.0, 0.0).astype(BF16)

    def twice(v):
        return jnp.concatenate([v, v], axis=1)

    def keys(j):
        lat = jnp.concatenate(
            [own[:, j, 0:32, :].reshape(128, ROWS), peer[:, j, 0:32, :].reshape(128, ROWS)], axis=0
        ).astype(F32)
        rope = (own[:, j, 32:40, :].astype(F32) + peer[:, j, 32:40, :].astype(F32)).reshape(
            ROPE, ROWS
        )
        lat = lat * lax.rsqrt(jnp.mean(lat * lat, axis=0, keepdims=True) + EPS) * twice(glat[...])
        kv = dot(w[...], lat.astype(BF16)).astype(BF16)
        rope_sum = jnp.sum(rope * rope, axis=0, keepdims=True)
        turn = table[j]
        cosine, sine = turn[:16], turn[16:]
        ra, rb = rope[:16] * twice(gain[64:80]), rope[16:] * twice(gain[80:96])
        ra, rb = ra * cosine - rb * sine, rb * cosine + ra * sine
        ready, values = [], []
        for h in range(2):
            k = kv[64 * h : 64 * (h + 1)].astype(F32)
            scale = lax.rsqrt(
                (jnp.sum(k * k, axis=0, keepdims=True) + rope_sum) * np.float32(1 / QK) + EPS
            )
            ready.append(
                jnp.concatenate([k * scale * twice(gain[0:64]), ra * scale, rb * scale], axis=0).astype(
                    BF16
                )
            )
            values.append(jnp.concatenate([kv[128 + 64 * h : 192 + 64 * h], ones], axis=0))
        return ready, values

    def block(places, first):
        made = [keys(j) for j in places]
        for h in range(2):
            ready = jnp.concatenate([m[0][h] for m in made], axis=1)
            v = jnp.concatenate([m[1][h] for m in made], axis=1)
            s = dot(q[h, :, 0:QK], ready)
            if first:
                s = jnp.where(iota((ROWS, ROWS), 1) <= iota((ROWS, ROWS), 0), s, -jnp.inf)
            peak = jnp.max(s, axis=1, keepdims=True)
            if first:
                top[h] = jnp.broadcast_to(peak, (ROWS, 128))
                acc[h] = dot(jnp.exp2(s - peak).astype(BF16), v, NT)
            else:
                old = top[h]
                new = jnp.maximum(old, peak)
                top[h] = new
                p = jnp.exp2(s - jnp.concatenate([new] * (2 * len(places)), axis=1)).astype(BF16)
                acc[h] = acc[h] * jnp.exp2(old - new) + dot(p, v, NT)

    block([sp], True)

    def loop(i, carry):
        block([5 * i + n for n in range(5)], False)
        return carry

    lax.fori_loop(0, sp // 5, loop, 0)
    left = lax.rem(sp, 5)
    for count in range(1, 5):

        @pl.when(left == count)
        def _():
            block([sp - count + n for n in range(count)], False)

    parts = []
    rows = []
    for h in range(2):
        total = acc[h][:, 64:65]
        parts.append(acc[h][:, 0:64] / total)
        full = top[h] * np.float32(np.log(2.0)) + jnp.log(jnp.broadcast_to(total, (ROWS, 128)))
        rows.append(full.T[0:1])
    att[...] = jnp.concatenate(parts, axis=1).astype(BF16)
    logs[...] = jnp.concatenate(rows, axis=0)


def attend(*args):
    outs = [jax.ShapeDtypeStruct((ROWS, 128), BF16), jax.ShapeDtypeStruct((2, ROWS), F32)]
    scratch = [pltpu.VMEM((2, ROWS, 128), F32), pltpu.VMEM((2, ROWS, 128), F32)]
    return call(attend_body, outs, args, 8 << 30, scratch, [VMEM] * 7)


def merge_body(att, free, along, bonus, states, branch, o0, o1, o2, o3, keep, send, held, arrived):
    copies = [
        pltpu.make_async_copy(o.at[pl.ds(192, 256)], held.at[k], arrived.at[k])
        for k, o in enumerate((o0, o1, o2, o3))
    ]
    for copy in copies:
        copy.start()
    head = iota((128, 128), 0) // 64 == iota((128, 128), 1) // 64

    def spread(v):
        return jnp.where(head, jnp.concatenate([v, v], axis=0), jnp.zeros((), v.dtype))

    sp = lax.axis_index("sp")
    eye = jnp.where(iota((128, 128), 0) == iota((128, 128), 1), 1.0, 0.0).astype(BF16)
    below = jnp.zeros((128, 128), F32)
    entering = below
    groups = []
    for g in range(4):
        pair = None
        for r in range(4 * g, 4 * g + 4):
            move = jnp.where(r < sp, spread(states[r, 0]), eye)
            add = jnp.where(r < sp, spread(states[r, 1]).astype(F32), 0.0)
            if pair is None:
                pair = jnp.concatenate([add, move.astype(F32)], axis=0)
            else:
                pair = dot_wide(pair, move) + jnp.concatenate([add, below], axis=0)
        groups.append(pair)
    entering = groups[0][:128]
    for pair in groups[1:]:
        entering = fine(entering, pair[128:]) + pair[:128]
    read = free[...] + fine(along[...], entering, NT)
    mean = jnp.where(head, 1.0 / 64, 0.0).astype(BF16)
    read = read - dot_wide(read, mean)
    spread_of = dot_wide(read * read, mean)
    rec = read * lax.rsqrt(spread_of + GROUP_EPS) * branch[...] + bonus[...]
    both = jnp.concatenate([att[...].astype(F32), rec], axis=1).reshape(4, 2, 32, 256)
    core = lax.rem(lax.axis_index("tp"), 2)
    even, odd = both[:, 0].reshape(128, 256), both[:, 1].reshape(128, 256)
    kept = jnp.where(core == 0, even, odd).astype(BF16)
    sent = jnp.where(core == 0, odd, even).astype(BF16)
    for copy in copies:
        copy.wait()
    for k in range(4):
        send[:, columns(k)] = dot(sent, held[k]).astype(BF16)
    for k in range(4):
        keep[:, columns(k)] = dot(kept, held[k])


def merge(*args):
    outs = [jax.ShapeDtypeStruct((128, 2048), F32), jax.ShapeDtypeStruct((128, 2048), BF16)]
    scratch = [pltpu.VMEM((4, 256, 512), BF16), pltpu.SemaphoreType.DMA((4,))]
    return call(merge_body, outs, args, 4 << 30, scratch, [VMEM] * 6 + [HBM] * 4)


def exchanged(copies, axis, groups=None):
    return lax.all_to_all(copies, axis, 0, 0, axis_index_groups=groups, tiled=True)


def around(value):
    moves = [[(i, (i + by) % 4) for i in range(4)] for by in (1, 3, 2)]
    return [value] + [lax.ppermute(value, "fs", move) for move in moves]


def other_core(value):
    return lax.ppermute(value, "tp", [(i, i ^ 1) for i in range(8)])


def turn_table():
    half = ROPE // 2
    inverse = np.float32(10000.0) ** (-np.arange(half, dtype=np.float32) / np.float32(half))
    angle = np.arange(4096, dtype=np.float32)[:, None] * inverse.astype(np.float32)[None, :]
    both = np.concatenate([np.cos(angle), np.sin(angle)], axis=1).astype(np.float32)
    return both.reshape(16, ROWS, ROPE).transpose(0, 2, 1)


def shards(
    entering,
    entering_gain,
    wq,
    wc,
    wr,
    compact_gain,
    wk_up,
    wv_up,
    q_gain,
    k_gain,
    w_accept,
    w_key,
    w_value,
    fade1,
    fade2,
    fade_bias,
    fade_mult,
    fade_extra,
    adapt1,
    adapt2,
    adapt_bias,
    present,
    branch,
    wo_att,
    wo_rec,
):
    xs, big, late = prepare(
        entering[0],
        entering_gain.reshape(1, 2048),
        w_accept,
        w_key,
        w_value,
        wq.T,
        wc,
        wr.T,
        wo_att,
        wo_rec,
    )
    normed = exchanged(xs, "tp").reshape(ROWS, 2048)
    bigs = around(big)
    lates = around(late)

    table = jnp.asarray(turn_table())
    pay = latents(normed, *bigs)
    lat = exchanged(pay, "sp")

    free, along, bonus, state = recur(
        normed,
        *bigs,
        fade1,
        adapt1,
        fade2,
        fade_bias.reshape(1, 128),
        adapt2,
        adapt_bias.reshape(1, 128),
        fade_mult[0],
        fade_extra[0],
        present,
    )
    lat, state = lax.optimization_barrier((lat, state))
    states = exchanged(state, "sp")
    others = [lax.ppermute(lat, "tp", [(i, (i + by) % 8) for i in range(8)]) for by in (2, 6, 4)]
    lat_own = collect(lat, *others)
    lat_peer = other_core(lat_own)
    q, up, glat, key_gain = queries(
        normed,
        *lates,
        table,
        wk_up,
        wv_up,
        compact_gain.reshape(1, 256),
        k_gain.reshape(1, QK),
        q_gain.reshape(1, QK),
    )
    att, logs = attend(q, lat_own, lat_peer, up, glat, key_gain, table)
    keep, send = merge(att, free, along, bonus, states, branch.reshape(1, 128), *lates)
    pair = (keep + other_core(send).astype(F32)).astype(BF16)
    same_core = [[0, 2, 4, 6], [1, 3, 5, 7]]
    parts = exchanged(pair.reshape(4, 32, 2048), "tp", same_core)
    mixed = jnp.sum(parts.astype(F32), axis=0).astype(BF16)
    return mixed[None], logs[None]


def solution(mesh):
    placed = (
        P("fs", ("sp", "tp"), None),
        P(),
        P("fs", "tp"),
        P("fs", None),
        P("fs", None),
        P(),
        P(None, "tp"),
        P(None, "tp"),
        P(),
        P(),
        P("fs", "tp"),
        P("fs", "tp"),
        P("fs", "tp"),
        P(),
        P(None, "tp"),
        P("tp"),
        P("fs", "tp", "sp"),
        P("fs", "tp", "sp"),
        P(),
        P(None, "tp"),
        P("tp"),
        P("tp", None),
        P("tp"),
        P("tp", "fs"),
        P("tp", "fs"),
    )

    return jax.shard_map(
        shards,
        mesh=mesh,
        in_specs=placed,
        out_specs=(P("fs", ("sp", "tp"), None), P("fs", "tp", "sp")),
        check_vma=False,
    )
```
